32 devices in a mesh: ep: 8 (over z, y), tp: 4 (over x, core).
Axes of the slice: x: 2, y: 2, z: 4, core: 2. Of those that a mesh axis runs over, the one named last changes fastest.
Arguments:
- mixer_in: bfloat16 [4096, 2048], P('ep'), may hold values from -6 to 6
- mixer_gain: float32 [2048], replicated, may hold values from 0.1 to 1.9
- query_weight: bfloat16 [2048, 1024], P(None, 'tp'), may hold values from -0.125 to 0.125
- key_weight: bfloat16 [2048, 1024], P(None, 'tp'), may hold values from -0.125 to 0.125
- value_weight: bfloat16 [2048, 1024], P(None, 'tp'), may hold values from -0.125 to 0.125
- input_gate: float32 [8, 4096], P('tp', 'ep'), may hold values from -4 to 240
- forget_gate: float32 [8, 4096], P('tp', 'ep'), may hold values from 0 to 25
- head_gain: float32 [1024], replicated, may hold values from 0.1 to 1.9
- mixer_out_weight: bfloat16 [1024, 2048], P('tp'), may hold values from -0.1875 to 0.1875
- expert_in: bfloat16 [2048, 2048], P('ep'), may hold values from -6 to 6
- expert_gain: float32 [2048], replicated, may hold values from 0.1 to 1.9
- group_router: bfloat16 [2048, 2], replicated, may hold values from -0.125 to 0.125
- expert_router: bfloat16 [2048, 8], replicated, may hold values from -0.125 to 0.125
- routes: int32 [2048, 2], P('ep'), may hold values from 0 to 7, all different within a row; in each aligned block of 256 rows (0 to 255, 256 to 511, ...) at most 128 rows name the same one
- gate_experts: bfloat16 [8, 2048, 1024], P('ep', None, 'tp'), may hold values from -0.125 to 0.125
- up_experts: bfloat16 [8, 2048, 1024], P('ep', None, 'tp'), may hold values from -0.125 to 0.125
- down_experts: bfloat16 [8, 1024, 2048], P('ep', 'tp'), may hold values from -0.1875 to 0.1875
Outputs:
- mixer_out: bfloat16 [4096, 2048], P(('ep', 'tp'))
- expert_out: bfloat16 [2048, 2048], P('ep', 'tp')
The draws below stay inside these ranges and needn't reach their ends.
Inputs may be any that keep to these rules, and one draw needn't show every extreme that they name: `routes`: each row names 2 different experts. In each aligned block of 256 rows (the rows of one index of ep) no expert is named by more than 128 rows, a bound that some block reaches.
All inputs are finite; a program needn't handle non-finite values.
Results may differ from the reference program's by a relative error of at most 0.014.
The reference program's roundings to bfloat16 on the way count: a program that leaves them out, or rounds other values in their place, can miss the bound.
Values may be sent and summed in bfloat16 or wider, within the bound.
A program may use at most 128 MiB of HBM per device.

```python
import math
import jax
import jax.numpy as jnp
import numpy as np
from jax import lax

D = 2048
HEADS = 8
W = 1024
FF = 1024
BLOCK = 128
TOPK = 2
TA_DEV = 512
TB_DEV = 256
SEQUENCE_SPAN = 4096
TB = 2048
EXPERTS = 8
GROUPS = 2
CAP = 128
N_EP = 8
N_TP = 4


def draw_input_gate(key, part):
    value_rows = jnp.clip(jax.random.normal(jax.random.fold_in(key, 11), (HEADS, SEQUENCE_SPAN), jnp.float32), -4.0, 4.0)
    return value_rows


def draw_forget_gate(key, part):
    sequence_place = jnp.arange(SEQUENCE_SPAN)
    fast_cut = 5
    is_fast = jax.random.randint(jax.random.fold_in(key, 21), (HEADS,), 0, 10) < fast_cut
    factors = jnp.exp(jax.random.uniform(jax.random.fold_in(key, 22), (SEQUENCE_SPAN // TA_DEV,), jnp.float32, math.log(0.4), math.log(2.5)))
    noise = jnp.exp(0.7 * jnp.clip(jax.random.normal(jax.random.fold_in(key, 23), (HEADS, SEQUENCE_SPAN), jnp.float32), -4.0, 4.0))
    slow_rate = 0.3 / SEQUENCE_SPAN * factors[sequence_place // TA_DEV]
    rate = jnp.where(is_fast[:, None], 1.0 / 40.0, slow_rate[None, :]) * noise
    value_rows = -jnp.log(rate)
    spike_location = jax.random.randint(jax.random.fold_in(key, 25), (3,), 0, SEQUENCE_SPAN)
    retain_flag = jax.random.uniform(jax.random.fold_in(key, 26), (HEADS, 3), jnp.float32, 0.5, 0.8)
    spike_magnitude = jnp.log(retain_flag / (1.0 - retain_flag))
    for column_slot in range(3):
        value_rows = jnp.where(sequence_place[None, :] == spike_location[column_slot], spike_magnitude[:, column_slot:column_slot + 1], value_rows)
    return value_rows


def steps_of(rng, extent, shards, smallest, largest):
    level, own = 1.0, jax.random.fold_in(rng, 6)
    for dim, parts in shards:
        heights = jnp.exp(jax.random.uniform(jax.random.fold_in(own, dim), (parts,), jnp.float32, smallest / len(shards), largest / len(shards)))
        level = level * jnp.repeat(heights, extent[dim] // parts).reshape([-1 if axis == dim else 1 for axis in range(len(extent))])
    return level


def routed_block(key, own, number, rows, count, top, limit, skew):
    ranking = jax.random.permutation(key, count)
    crowded, common = shares(count, rows * top, limit, skew, True), shares(count, rows * top, limit, skew, False)
    places = jnp.arange(count)

    def named(lengths, offset_by):
        used = int((lengths > 0).sum())
        fixed = max(1, used // 4)
        shifted = fixed + (places - fixed + offset_by * (used - fixed)) % max(1, count - fixed)
        return jnp.zeros((count,), jnp.int32).at[ranking[jnp.where(places < fixed, places, shifted)]].set(jnp.asarray(lengths, jnp.int32))

    lengths = jnp.where(number % 4 == 0, named(crowded, number // 4), named(common, number - number // 4 - 1))
    mixed = jax.random.permutation(jax.random.fold_in(own, 3), count)
    source_of, sink = mixed[0:count // 2 * 2:2], mixed[1:count // 2 * 2:2]
    margin = jnp.minimum(lengths[source_of] - 1, limit - lengths[sink]) // 2
    margin = jnp.where((source_of == ranking[0]) | (sink == ranking[0]) | (lengths[sink] == 0), 0, jnp.maximum(margin, 0))
    shifted = jax.random.randint(jax.random.fold_in(own, 4), (count // 2,), 0, 1 << 20) % (margin + 1)
    lengths = lengths.at[source_of].add(-shifted).at[sink].add(shifted)
    labels = jnp.searchsorted(jnp.cumsum(lengths), jnp.arange(rows * top), side="right").astype(jnp.int32)
    table = labels.reshape(top, rows).T
    table = table[jax.random.permutation(jax.random.fold_in(own, 1), rows)]
    offset_by = jax.random.randint(jax.random.fold_in(own, 2), (rows, 1), 0, top)
    return jnp.take_along_axis(table, (jnp.arange(top)[None, :] + offset_by) % top, axis=1)


def shares(count, total, limit, slope, full):
    weights = [(1 << 20) // math.isqrt(standing ** slope) + 1 for standing in range(1, count + 1)]
    largest = limit if full else min(limit, max(-(-total // count), total * weights[0] // sum(weights)))
    least = 1 if total - largest >= count - 1 else 0
    holding, surplus = [largest] + [least] * (count - 1), total - largest - least * (count - 1)
    while surplus > 0:
        candidates = [i for i in range(1, count) if holding[i] < largest] or [i for i in range(1, count) if holding[i] < limit]
        whole, budget = sum([weights[i] for i in candidates]), surplus
        for i in candidates:
            addition = min(limit - holding[i], max(1, budget * weights[i] // whole), surplus)
            holding[i] = holding[i] + addition
            surplus = surplus - addition
    return np.array(holding)


def normal_values(key, dims, scale, bound, pieces=(), kind=jnp.bfloat16):
    entries = jax.random.normal(key, dims, jnp.float32) * scale
    if len(pieces) > 0:
        entries = steps_of(key, dims, pieces, -0.22, 0.18) * entries
    return jnp.clip(entries, min=-bound, max=bound).astype(kind)


def setup_inputs(seed: int = 0) -> dict:
    key_list = jax.random.split(jax.random.key(seed), 18)
    mixer_in = normal_values(key_list[0], (SEQUENCE_SPAN, D), 1.0, 6.0, ((0, 8),))
    mixer_gain = jnp.clip(1.0 + 0.18 * jax.random.normal(key_list[1], (D,), jnp.float32), 0.1, 1.9)
    query_weight = normal_values(key_list[2], (D, W), D ** -0.5, 0.125, ((1, 4),))
    key_weight = normal_values(key_list[3], (D, W), D ** -0.5, 0.125, ((1, 4),))
    value_weight = normal_values(key_list[4], (D, W), D ** -0.5, 0.125, ((1, 4),))
    input_gate = draw_input_gate(jax.random.fold_in(key_list[17], 71), 0)
    forget_gate = draw_forget_gate(jax.random.fold_in(key_list[17], 71), 0)
    head_gain = jnp.clip(1.0 + 0.18 * jax.random.normal(key_list[7], (W,), jnp.float32), 0.1, 1.9)
    mixer_out_weight = normal_values(key_list[8], (W, D), W ** -0.5, 0.1875, ((0, 4),))
    expert_in = normal_values(key_list[9], (TB, D), 1.0, 6.0, ((0, 8),))
    expert_gain = jnp.clip(1.0 + 0.18 * jax.random.normal(key_list[10], (D,), jnp.float32), 0.1, 1.9)
    group_router = normal_values(key_list[11], (D, GROUPS), D ** -0.5, 0.125)
    expert_router = normal_values(key_list[12], (D, EXPERTS), D ** -0.5, 0.125)
    routes_keys = jax.random.split(jax.random.fold_in(key_list[13], 1), TB // TB_DEV)
    routes_turns = jax.random.permutation(jax.random.fold_in(key_list[13], 3), TB // TB_DEV)
    routes = jax.vmap(lambda own, number: routed_block(jax.random.fold_in(key_list[13], 2), own, number, TB_DEV, EXPERTS, TOPK, CAP, 1))(routes_keys, routes_turns).reshape((TB, TOPK))
    gate_experts = normal_values(key_list[14], (EXPERTS, D, FF), D ** -0.5, 0.125, ((0, 8), (2, 4)))
    up_experts = normal_values(key_list[15], (EXPERTS, D, FF), D ** -0.5, 0.125, ((0, 8), (2, 4)))
    down_experts = normal_values(key_list[16], (EXPERTS, FF, D), FF ** -0.5, 0.1875, ((0, 8), (1, 4)))
    return dict(mixer_in=mixer_in, mixer_gain=mixer_gain, query_weight=query_weight, key_weight=key_weight, value_weight=value_weight, input_gate=input_gate, forget_gate=forget_gate, head_gain=head_gain, mixer_out_weight=mixer_out_weight, expert_in=expert_in, expert_gain=expert_gain, group_router=group_router, expert_router=expert_router, routes=routes, gate_experts=gate_experts, up_experts=up_experts, down_experts=down_experts)


epsilon = 1e-06
highest = lax.Precision.HIGHEST
floor_log = -1e+30

def rms_rows(matrix, gain):
    widened = matrix.astype(jnp.float32)
    scaled = widened * lax.rsqrt(lax.optimization_barrier(jnp.mean(widened * widened, axis=-1, keepdims=True)) + epsilon)
    return scaled * gain

def block_state(keys, value_rows, input_block, forget_block, scale):
    cumulative = jnp.cumsum(forget_block, axis=-1)
    total_log = cumulative[..., -1]
    log_weight = total_log[..., None] - cumulative + input_block
    peak_log = lax.optimization_barrier(jnp.max(log_weight, axis=-1))
    weights = jnp.exp(log_weight - peak_log[..., None])
    key_float = keys.astype(jnp.float32) * scale
    value_weighted = value_rows.astype(jnp.float32) * weights[..., None]
    memory = jnp.einsum('...sv,...sk->...vk', value_weighted, key_float, precision=highest)
    return (memory, peak_log, total_log)

def merge_state(earlier, later):
    peak_log = jnp.maximum(later[2] + earlier[1], later[1])
    fade_earlier = jnp.exp(later[2] + earlier[1] - peak_log)
    fade_later = jnp.exp(later[1] - peak_log)
    memory = fade_earlier[..., None, None] * earlier[0] + fade_later[..., None, None] * later[0]
    return (memory, peak_log, earlier[2] + later[2])

def block_out(queries, keys, value_rows, input_block, forget_block, state, scale):
    cumulative = jnp.cumsum(forget_block, axis=-1)
    length = cumulative.shape[-1]
    causal = jnp.tril(jnp.ones((length, length), dtype=bool))
    within = jnp.where(causal, cumulative[..., :, None] - cumulative[..., None, :] + input_block[..., None, :], -jnp.inf)
    carried = cumulative + state[1][..., None]
    highest_log = jnp.maximum(lax.optimization_barrier(jnp.max(within, axis=-1)), carried)
    weight_within = jnp.exp(within - highest_log[..., None])
    weight_carried = jnp.exp(carried - highest_log)
    raw_scores = jnp.einsum('...td,...sd->...ts', queries.astype(jnp.float32), keys.astype(jnp.float32)) * scale
    block_scores = raw_scores * weight_within
    rounded = lax.optimization_barrier(block_scores.astype(jnp.bfloat16)).astype(jnp.float32)
    numerator = jnp.einsum('...ts,...sd->...td', rounded, value_rows.astype(jnp.float32))
    query_float = queries.astype(jnp.float32)
    return numerator + weight_carried[..., None] * jnp.einsum('...vk,...tk->...tv', state[0], query_float, precision=highest)

def route_weights(group_logits, expert_logits, routes):
    members = expert_logits.shape[1] // group_logits.shape[1]
    chosen = jnp.take_along_axis(expert_logits, routes, axis=1)
    group_pick = jnp.take_along_axis(group_logits, routes // members, axis=1)
    return jax.nn.sigmoid(group_pick) * jax.nn.sigmoid(chosen - chosen[:, ::-1])

def reference(mixer_in, mixer_gain, query_weight, key_weight, value_weight, input_gate, forget_gate, head_gain, mixer_out_weight, expert_in, expert_gain, group_router, expert_router, routes, gate_experts, up_experts, down_experts):
    normed_a = rms_rows(mixer_in, mixer_gain).astype(jnp.bfloat16)
    queries = jnp.dot(normed_a, query_weight, preferred_element_type=jnp.float32).astype(jnp.bfloat16)
    keys = jnp.dot(normed_a, key_weight, preferred_element_type=jnp.float32).astype(jnp.bfloat16)
    value_rows = jnp.dot(normed_a, value_weight, preferred_element_type=jnp.float32).astype(jnp.bfloat16)
    sequence = normed_a.shape[0]
    head_count = input_gate.shape[0]
    width = queries.shape[1]
    head_size = width // head_count
    block_count = sequence // BLOCK
    scale = head_size ** (-0.5)

    def split_heads(matrix):
        return matrix.reshape(block_count, BLOCK, head_count, head_size).transpose(0, 2, 1, 3)

    def split_gates(gates):
        return gates.reshape(head_count, block_count, BLOCK).transpose(1, 0, 2)
    initial = (jnp.zeros((head_count, head_size, head_size), jnp.float32), jnp.full((head_count,), floor_log, jnp.float32), jnp.zeros((head_count,), jnp.float32))

    def block_step(state, block_data):
        query_block, key_block, value_block, input_block, forget_block = block_data
        output = block_out(query_block, key_block, value_block, input_block, forget_block, state, scale)
        updated = merge_state(state, block_state(key_block, value_block, input_block, forget_block, scale))
        return (updated, output)
    outcome = lax.scan(block_step, initial, (split_heads(queries), split_heads(keys), split_heads(value_rows), split_gates(input_gate), split_gates(jax.nn.log_sigmoid(forget_gate))))
    cells = outcome[1].transpose(0, 2, 1, 3).reshape(sequence, head_count, head_size)
    cell_rows = rms_rows(cells, head_gain.reshape(head_count, head_size)).reshape(sequence, width).astype(jnp.bfloat16)
    group_width = width // N_TP
    mixed = jnp.zeros((sequence, mixer_out_weight.shape[1]), jnp.float32)
    for group in range(N_TP):
        partial_value = jnp.dot(cell_rows[:, group * group_width:(group + 1) * group_width], mixer_out_weight[group * group_width:(group + 1) * group_width], preferred_element_type=jnp.float32).astype(jnp.bfloat16)
        mixed = mixed + lax.optimization_barrier(partial_value).astype(jnp.float32)
    mixer_out = mixed.astype(jnp.bfloat16)
    normed_b = rms_rows(expert_in, expert_gain).astype(jnp.bfloat16)
    group_logits = jnp.dot(normed_b, group_router, preferred_element_type=jnp.float32)
    expert_logits = jnp.dot(normed_b, expert_router, preferred_element_type=jnp.float32)
    combine = route_weights(group_logits, expert_logits, routes)
    token_count = normed_b.shape[0]
    expert_total = expert_logits.shape[1]
    token_device = token_count // N_EP
    capacity = 4 * token_device // expert_total
    flat_routes = routes.reshape(-1)
    pair_total = flat_routes.shape[0]
    matches = (flat_routes.reshape(N_EP, 2 * token_device)[:, :, None] == jnp.arange(expert_total, dtype=jnp.int32)[None, None, :]).astype(jnp.int32)
    sequence_place = (lax.optimization_barrier(jnp.sum(jnp.cumsum(matches, axis=1) * matches, axis=2)) - 1).reshape(-1)
    source = jnp.arange(pair_total, dtype=jnp.int32) // (2 * token_device)
    slot_index = source * capacity + sequence_place
    owner = jnp.full((expert_total, N_EP * capacity), pair_total, jnp.int32).at[flat_routes, slot_index].set(jnp.arange(pair_total, dtype=jnp.int32))
    padded = jnp.concatenate([normed_b, jnp.zeros((1, normed_b.shape[1]), jnp.bfloat16)], axis=0)
    weights_flat = jnp.concatenate([combine.reshape(-1), jnp.zeros((1,), jnp.float32)])
    hidden_group = gate_experts.shape[2] // N_TP

    def expert_step(total_out, expert_data):
        owners, gate_weight, up_weight, down_weight = expert_data
        rows_in = padded[owners // 2]
        gate_act = jnp.dot(rows_in, gate_weight, preferred_element_type=jnp.float32)
        up_act = jnp.dot(rows_in, up_weight, preferred_element_type=jnp.float32)
        hidden = (jax.nn.silu(gate_act) * up_act).astype(jnp.bfloat16)
        summed = jnp.zeros((rows_in.shape[0], down_weight.shape[1]), jnp.float32)
        for group in range(N_TP):
            partial_value = jnp.dot(hidden[:, group * hidden_group:(group + 1) * hidden_group], down_weight[group * hidden_group:(group + 1) * hidden_group], preferred_element_type=jnp.float32).astype(jnp.bfloat16)
            summed = summed + lax.optimization_barrier(partial_value).astype(jnp.float32)
        result = lax.optimization_barrier(summed.astype(jnp.bfloat16)).astype(jnp.float32)
        total_out = total_out.at[owners // 2].add(weights_flat[owners][:, None] * result)
        return (total_out, None)
    finished = lax.scan(expert_step, jnp.zeros((token_count + 1, normed_b.shape[1]), jnp.float32), (owner, gate_experts, up_experts, down_experts))
    expert_out = finished[0][:token_count].astype(jnp.bfloat16)
    return (mixer_out, expert_out)
```

```python
import functools

import jax
import jax.numpy as jnp
from jax import lax
from jax.experimental import pallas as pl
from jax.experimental.pallas import tpu as pltpu
from jax.sharding import PartitionSpec as P

MESH = pl.DeviceIdType.MESH


epsilon = 1e-06
highest = lax.Precision.HIGHEST
floor_log = -1e30


def is_power(count):
    return count & (count - 1) == 0


def rms_rows(matrix, gain):
    widened = matrix.astype(jnp.float32)
    scaled = widened * lax.rsqrt(jnp.mean(widened * widened, axis=-1, keepdims=True) + epsilon)
    return scaled * gain


def merged(earlier_memory, earlier_peak, later_memory, later_peak, later_total):
    moved = later_total + earlier_peak
    peak = jnp.maximum(moved, later_peak)
    return jnp.exp(moved - peak) * earlier_memory + jnp.exp(later_peak - peak) * later_memory, peak


def expert_kernel(
    sizes, own_ref, gate_ref, up_ref, down_ref, mix_ref,
    packed_ref, query_ref, key_ref, value_ref, cum_ref, cum_col_ref, in_ref, gain_ref, project_ref,
    out_ref, mixed_ref,
    rows, part, pin, csum, xin, fin, ret,
    peer, plane, mem, pre, pre_in, state, state_peak, state_parts, mpart, mpin, msum, mxin,
    own_sem, send_a, recv_a, send_x, recv_x, send_p, recv_p,
    send_q, recv_q, send_c, recv_c, send_r, recv_r,
    send_m, recv_m, send_k, recv_k, send_h, recv_h, send_y, recv_y,
):
    n, share, cap, width, quarter = sizes
    near = n // 2
    planes = n // 2
    me, tp = lax.axis_index("ep"), lax.axis_index("tp")
    core, column = lax.rem(tp, 2), lax.div(tp, 2)
    pair = tp + 1 - 2 * core
    cross = lax.rem(tp + 2, 4)
    pair_cross = lax.rem(pair + 2, 4)
    side, level = lax.rem(me, 2), lax.div(me, 2)
    mate = me + 1 - 2 * side

    def other(i):
        total, bit = 0, 1
        while bit < n:
            total = total + bit * lax.rem(lax.div(me, bit) + lax.div(i, bit), 2)
            bit *= 2
        return total

    high = lax.rem(lax.div(me, near), 2)
    inner = lax.rem(high + lax.div(lax.rem(me, near), near // 2), 2)

    def turn(t):
        half = near // 2
        swapped = near + lax.rem(t - near + inner * half, near)
        return jnp.where(t < near, t, swapped)

    def remote(src, dst, send, recv, to):
        return pltpu.make_async_remote_copy(
            src_ref=src, dst_ref=dst, send_sem=send, recv_sem=recv, device_id=to, device_id_type=MESH
        )

    barrier = pltpu.get_barrier_semaphore()
    for i in range(1, n):
        pl.semaphore_signal(
            barrier, inc=1, device_id=(lax.rem(me + i, n), tp), device_id_type=MESH
        )
    pl.semaphore_signal(barrier, inc=1, device_id=(me, pair), device_id_type=MESH)
    pl.semaphore_signal(barrier, inc=1, device_id=(me, cross), device_id_type=MESH)
    own = pltpu.make_async_copy(own_ref.at[me], rows.at[me, core], own_sem)
    own.start()
    pl.semaphore_wait(barrier, n + 1)

    def scatter_near(i, place):
        to = other(i)
        return remote(own_ref.at[to], rows.at[place, core], send_a.at[i], recv_a.at[i], (to, tp))

    def scatter_far(i, place):
        to = other(i)
        mine = pl.ds(pl.multiple_of(column * share, share), share)
        return remote(
            own_ref.at[to, mine], rows.at[place, core, mine], send_a.at[i], recv_a.at[i], (to, tp)
        )

    def across(s, which):
        mine = pl.ds(pl.multiple_of(which * share, share), share)
        return remote(
            rows.at[s, core, mine], rows.at[s, core, mine], send_x.at[s], recv_x.at[s], (me, cross)
        )

    def beside(s, which):
        return remote(
            rows.at[s, which], rows.at[s, which], send_p.at[s], recv_p.at[s], (me, pair)
        )

    def halves(s, k, who):
        return remote(part.at[s, who], pin.at[s, k], send_q.at[s, k], recv_q.at[s, k], (me, pair))

    def summed(s):
        return remote(csum.at[s], xin.at[s], send_c.at[s], recv_c.at[s], (me, cross))

    def back(i):
        to = other(i)
        return remote(fin.at[to], ret.at[me], send_r.at[i], recv_r.at[i], (to, tp))

    def to_mate():
        return remote(packed_ref, peer, send_k.at[0], recv_k.at[0], (mate, tp))

    def to_level(d):
        return remote(
            plane, mem.at[level], send_m.at[d], recv_m.at[d], (lax.rem(me + 2 * d, n), tp)
        )

    def from_level(d):
        return remote(
            plane, mem.at[level - d], send_m.at[d], recv_m.at[d], (lax.rem(me + 2 * d, n), tp)
        )

    def prefix_mate():
        return remote(pre, pre_in, send_k.at[1], recv_k.at[1], (mate, tp))

    def mixed_half(k, who):
        return remote(mpart.at[who], mpin.at[k], send_h.at[k], recv_h.at[k], (me, pair))

    def mixed_sum():
        return remote(msum, mxin, send_y, recv_y, (me, cross))

    heads = packed_ref.shape[0]
    size = packed_ref.shape[2]
    length = query_ref.shape[0]
    chunk = length // 4
    scale = size ** (-0.5)
    body, top_row, sum_row = slice(0, size), slice(size, size + 1), slice(size + 1, size + 2)

    def combine_plane():
        to_mate().wait_recv()

        def joined(first, second):
            memory, peak = merged(
                first[side, body], first[side, top_row],
                second[side, body], second[side, top_row], second[side, sum_row],
            )
            plane[size : size + 8] = jnp.zeros((8, size), jnp.float32)
            plane[body] = memory
            plane[top_row] = peak
            plane[sum_row] = first[side, sum_row] + second[side, sum_row]

        @pl.when(side == 0)
        def _():
            joined(packed_ref, peer)

        @pl.when(side == 1)
        def _():
            joined(peer, packed_ref)

        for d in range(1, planes):
            @pl.when(level + d < planes)
            def _():
                to_level(d).start()

    def combine_levels():
        pre[...] = jnp.zeros_like(pre)
        pre[top_row] = jnp.full((1, size), floor_log, jnp.float32)
        for k in range(planes - 1):
            d = planes - 1 - k

            @pl.when(d <= level)
            def _():
                from_level(d).wait_recv()
                z = level - d
                memory, peak = merged(
                    pre[body], pre[top_row], mem[z, body], mem[z, top_row], mem[z, sum_row]
                )
                pre[body] = memory
                pre[top_row] = peak

        prefix_mate().start()

    def combine_last():
        prefix_mate().wait_recv()
        state[side] = pre[body]
        state_peak[side, 0:1, :] = pre[top_row]
        state[1 - side] = pre_in[body]
        state_peak[1 - side, 0:1, :] = pre_in[top_row]

        @pl.when(side == 1)
        def _():
            for h in range(heads):
                memory, peak = merged(
                    state[h], state_peak[h, 0:1, :],
                    peer[h, body], peer[h, top_row], peer[h, sum_row],
                )
                state[h] = memory
                state_peak[h, 0:1, :] = peak

        for h in range(heads):
            rest = state[h]
            for piece in range(3):
                top_part = rest.astype(jnp.bfloat16)
                state_parts[h, piece] = top_part
                rest = rest - top_part.astype(jnp.float32)

    def attend(j):
        start = pl.multiple_of(j * chunk, chunk)
        row = start + lax.broadcasted_iota(jnp.int32, (chunk, length), 0)
        causal = row >= lax.broadcasted_iota(jnp.int32, (chunk, length), 1)
        nt = (((1,), (1,)), ((), ()))
        cell_list = []
        for h in range(heads):
            cols = slice(h * size, (h + 1) * size)
            q = query_ref[pl.ds(start, chunk), cols]
            c = cum_col_ref[pl.ds(start, chunk), h : h + 1]
            within = jnp.where(causal, c - cum_ref[h : h + 1, :] + in_ref[h : h + 1, :], -jnp.inf)
            carried = c + state_peak[h, 0:1, 0:1]
            top = jnp.maximum(jnp.max(within, axis=1, keepdims=True), carried)
            raw = lax.dot_general(q, key_ref[:, cols], nt, preferred_element_type=jnp.float32)
            scores = (raw * scale * jnp.exp(within - top)).astype(jnp.bfloat16)
            cells = jnp.dot(scores, value_ref[:, cols], preferred_element_type=jnp.float32)
            held = jnp.zeros((chunk, size), jnp.float32)
            for piece in (2, 1, 0):
                held = held + lax.dot_general(
                    q, state_parts[h, piece], nt, preferred_element_type=jnp.float32
                )
            cells = cells + jnp.exp(carried - top) * held
            mean = jnp.mean(cells * cells, axis=1, keepdims=True)
            cell_list.append(
                (cells * lax.rsqrt(mean + epsilon) * gain_ref[h : h + 1, :]).astype(jnp.bfloat16)
            )
        cell_rows = jnp.concatenate(cell_list, axis=1)
        for q in range(4):
            cols = slice(q * quarter, (q + 1) * quarter)
            mpart[j, :, cols] = jnp.dot(
                cell_rows, project_ref[:, cols], preferred_element_type=jnp.float32
            ).astype(jnp.bfloat16)

    begin = 4

    def mixer_step(t):
        @pl.when(t == 2)
        def _():
            combine_levels()

        @pl.when(t == begin)
        def _():
            combine_last()

        @pl.when((t >= begin) & (t < begin + 4))
        def _():
            k = t - begin
            attend(jnp.where(k == 0, pair_cross, jnp.where(k == 1, pair, jnp.where(k == 2, cross, tp))))

        @pl.when(t == begin)
        def _():
            mixed_half(1, pair_cross).start()

        @pl.when(t == begin + 1)
        def _():
            mixed_half(0, pair).start()

        @pl.when(t == begin + 2)
        def _():
            mixed_half(1, pair_cross).wait_recv()
            msum[...] = (
                mpart[cross].astype(jnp.float32) + mpin[1].astype(jnp.float32)
            ).astype(jnp.bfloat16)
            mixed_sum().start()

    def first_near(i, carry):
        scatter_near(i, me).start()
        return carry

    def first_far(t, carry):
        scatter_far(turn(t), me).start()
        return carry

    to_mate().start()
    lax.fori_loop(1, near - 1, first_near, 0)
    own.wait()
    beside(me, core).start()
    combine_plane()
    lax.fori_loop(near - 1, near, first_near, 0)
    lax.fori_loop(near, n, first_far, 0)

    def step(t, carry):
        @pl.when(t >= 4)
        def _():
            i = turn(t - 4)
            s = other(i)
            halves(s, 0, pair).wait_recv()
            summed(s).wait_recv()
            total = (
                part[s, tp].astype(jnp.float32)
                + pin[s, 0].astype(jnp.float32)
                + xin[s].astype(jnp.float32)
            ).astype(jnp.bfloat16)

            @pl.when(i > 0)
            def _():
                fin[s] = total
                back(i).start()

            @pl.when(i == 0)
            def _():
                ret[s] = total

        @pl.when((t >= 3) & (t < n + 3))
        def _():
            s = other(turn(t - 3))
            halves(s, 1, pair_cross).wait_recv()
            csum[s] = (
                part[s, cross].astype(jnp.float32) + pin[s, 1].astype(jnp.float32)
            ).astype(jnp.bfloat16)
            summed(s).start()

        @pl.when((t >= 1) & (t < near))
        def _():
            s = other(t)
            scatter_near(t, s).wait_recv()
            beside(s, core).start()

        @pl.when((t >= near) & (t < n))
        def _():
            i = turn(t)
            s = other(i)
            scatter_far(i, s).wait_recv()
            across(s, column).start()

        @pl.when((t >= near + 1) & (t < n + 1))
        def _():
            s = other(turn(t - 1))
            across(s, 1 - column).wait_recv()
            beside(s, core).start()

        @pl.when((t >= 2) & (t < n + 2))
        def _():
            s = other(turn(t - 2))
            beside(s, 1 - core).wait_recv()
            x = rows[s].reshape(cap, width)
            gate_act = jnp.dot(x, gate_ref[...], preferred_element_type=jnp.float32)
            up_act = jnp.dot(x, up_ref[...], preferred_element_type=jnp.float32)
            hidden = (gate_act * jax.nn.sigmoid(gate_act) * up_act).astype(jnp.bfloat16)
            for q in range(4):
                part[s, q] = jnp.dot(
                    hidden,
                    down_ref[:, q * quarter : (q + 1) * quarter],
                    preferred_element_type=jnp.float32,
                ).astype(jnp.bfloat16)
            halves(s, 1, pair_cross).start()
            halves(s, 0, pair).start()

        mixer_step(t)
        return carry

    lax.fori_loop(0, n + 4, step, 0)

    mixed_half(0, pair).wait_recv()
    mixed_sum().wait_recv()
    mixed_ref[...] = (
        mpart[tp].astype(jnp.float32) + mpin[0].astype(jnp.float32) + mxin[...].astype(jnp.float32)
    ).astype(mixed_ref.dtype)

    def finish(i, carry):
        back(i).wait_recv()
        return carry

    lax.fori_loop(1, n, finish, 0)
    mix = mix_ref[...]
    high_mix = mix.astype(jnp.bfloat16)
    low_mix = (mix - high_mix.astype(jnp.float32)).astype(jnp.bfloat16)
    table = ret[...].reshape(n * cap, quarter)
    out_ref[...] = (
        jnp.dot(high_mix, table, preferred_element_type=jnp.float32)
        + jnp.dot(low_mix, table, preferred_element_type=jnp.float32)
    ).astype(out_ref.dtype)

    def drain(i, carry):
        s = other(i)
        beside(s, core).wait_send()
        halves(s, 0, pair).wait_send()
        halves(s, 1, pair_cross).wait_send()
        summed(s).wait_send()

        @pl.when(i > 0)
        def _():
            back(i).wait_send()

        @pl.when((i > 0) & (i < near))
        def _():
            scatter_near(i, me).wait_send()

        @pl.when(i >= near)
        def _():
            scatter_far(i, me).wait_send()
            across(s, column).wait_send()

        return carry

    lax.fori_loop(0, n, drain, 0)
    to_mate().wait_send()
    prefix_mate().wait_send()
    for d in range(1, planes):
        @pl.when(level + d < planes)
        def _():
            to_level(d).wait_send()
    mixed_half(0, pair).wait_send()
    mixed_half(1, pair_cross).wait_send()
    mixed_sum().wait_send()


def all_fused(own_share, gate_weight, up_weight, down_weight, mix, prepared, gain, project):
    n, pieces, width = own_share.shape
    share = pieces // 2
    cap = share * 4
    quarter = width // 4
    tokens = mix.shape[0]
    packed, queries, keys, values, cumulative, input_gate = prepared
    heads, size = packed.shape[0], packed.shape[2]
    chunk = queries.shape[0] // 4
    vmem = pl.BlockSpec(memory_space=pltpu.VMEM)
    dma = pltpu.SemaphoreType.DMA
    bf = jnp.bfloat16
    f32 = jnp.float32
    return pl.pallas_call(
        functools.partial(expert_kernel, (n, share, cap, width, quarter)),
        out_shape=(
            jax.ShapeDtypeStruct((tokens, quarter), bf),
            jax.ShapeDtypeStruct((chunk, width), bf),
        ),
        in_specs=[vmem] * 14,
        out_specs=(vmem, vmem),
        scratch_shapes=[
            pltpu.VMEM((n, 2, 2 * share, width), bf),
            pltpu.VMEM((n, 4, cap, quarter), bf),
            pltpu.VMEM((n, 2, cap, quarter), bf),
            pltpu.VMEM((n, cap, quarter), bf),
            pltpu.VMEM((n, cap, quarter), bf),
            pltpu.VMEM((n, cap, quarter), bf),
            pltpu.VMEM((n, cap, quarter), bf),
            pltpu.VMEM((heads, size + 8, size), f32),
            pltpu.VMEM((size + 8, size), f32),
            pltpu.VMEM((n // 2, size + 8, size), f32),
            pltpu.VMEM((size + 8, size), f32),
            pltpu.VMEM((size + 8, size), f32),
            pltpu.VMEM((heads, size, size), f32),
            pltpu.VMEM((heads, 8, size), f32),
            pltpu.VMEM((heads, 3, size, size), bf),
            pltpu.VMEM((4, chunk, width), bf),
            pltpu.VMEM((2, chunk, width), bf),
            pltpu.VMEM((chunk, width), bf),
            pltpu.VMEM((chunk, width), bf),
            dma,
            dma((n,)), dma((n,)), dma((n,)), dma((n,)), dma((n,)), dma((n,)),
            dma((n, 2)), dma((n, 2)), dma((n,)), dma((n,)), dma((n,)), dma((n,)),
            dma((n // 2,)), dma((n // 2,)), dma((2,)), dma((2,)), dma((2,)), dma((2,)), dma, dma,
        ],
        compiler_params=pltpu.CompilerParams(collective_id=0, has_side_effects=True),
        cost_estimate=pl.CostEstimate(
            flops=60_000_000_000, bytes_accessed=8_000_000, transcendentals=0
        ),
    )(
        own_share, gate_weight, up_weight, down_weight, mix,
        packed, queries, keys, values, cumulative, cumulative.T, input_gate, gain, project,
    )


def experts_plain(own_share, gate_weight, up_weight, down_weight, mix):
    arrived = lax.all_to_all(own_share, "ep", split_axis=0, concat_axis=0, tiled=True)
    piece_rows = lax.all_gather(arrived, "tp", axis=1, tiled=True)
    gate_act = jnp.einsum(
        "scd,df->scf", piece_rows, gate_weight, preferred_element_type=jnp.float32
    )
    up_act = jnp.einsum("scd,df->scf", piece_rows, up_weight, preferred_element_type=jnp.float32)
    hidden = (jax.nn.silu(gate_act) * up_act).astype(jnp.bfloat16)
    partial_rows = jnp.einsum(
        "scf,fo->sco", hidden, down_weight, preferred_element_type=jnp.float32
    )
    summed = lax.psum_scatter(
        partial_rows.astype(jnp.bfloat16), "tp", scatter_dimension=2, tiled=True
    )
    returned = lax.all_to_all(summed, "ep", split_axis=0, concat_axis=0, tiled=True)
    return jnp.dot(
        mix, returned.reshape(-1, returned.shape[2]).astype(jnp.float32), precision=highest
    ).astype(jnp.bfloat16)


def mixer_prepare(normed_a, query_weight, key_weight, value_weight, input_gate, forget_gate):
    def project(weight):
        return jnp.dot(normed_a, weight, preferred_element_type=jnp.float32).astype(jnp.bfloat16)

    rows = normed_a.shape[0]
    heads = input_gate.shape[0]
    width_local = query_weight.shape[1]
    head_size = width_local // heads
    scale = head_size ** (-0.5)
    causal = jnp.tril(jnp.ones((rows, rows), dtype=bool))
    log_forget = jax.nn.log_sigmoid(forget_gate)
    cumulative = jnp.einsum(
        "hs,ts->ht", log_forget, causal.astype(jnp.float32), precision=highest
    )
    total = cumulative[:, -1]
    log_weight = total[:, None] - cumulative + input_gate
    peak = jnp.max(log_weight, axis=-1)
    weights = jnp.exp(log_weight - peak[:, None])
    keys = project(key_weight)
    values = project(value_weight)

    def by_head(matrix):
        return [matrix[:, h * head_size : (h + 1) * head_size] for h in range(heads)]

    key_heads, value_heads = by_head(keys), by_head(values)
    memory = jnp.stack(
        [
            lax.dot_general(
                value_heads[h].astype(jnp.float32) * weights[h][:, None],
                key_heads[h].astype(jnp.float32) * scale,
                (((0,), (0,)), ((), ())),
                precision=highest,
            )
            for h in range(heads)
        ]
    )
    stats = jnp.stack([peak, total], axis=1)
    stats = jnp.concatenate([stats, jnp.zeros((heads, 6), jnp.float32)], axis=1)
    packed = jnp.concatenate(
        [memory, jnp.broadcast_to(stats[:, :, None], (heads, 8, head_size))], axis=1
    )
    return (packed, project(query_weight), keys, values, cumulative, input_gate)


def mixer_partial(prepared, gain_local, mixer_out_weight):
    packed, queries, keys, values, cumulative, input_gate = prepared
    rows = queries.shape[0]
    heads, head_size = gain_local.shape
    scale = head_size ** (-0.5)
    causal = jnp.tril(jnp.ones((rows, rows), dtype=bool))

    def by_head(matrix):
        return [matrix[:, h * head_size : (h + 1) * head_size] for h in range(heads)]

    query_heads, key_heads, value_heads = by_head(queries), by_head(keys), by_head(values)
    everything = lax.all_gather(packed, "ep")
    n, place = lax.axis_size("ep"), lax.axis_index("ep")
    peaks = everything[:, :, head_size, 0]
    totals = everything[:, :, head_size + 1, 0]
    order = jnp.arange(n)
    later = (order[None, :] > order[:, None]) & (order[None, :] < place)
    suffix = jnp.sum(jnp.where(later[:, :, None], totals[None], 0.0), axis=1)
    before = (order < place)[:, None]
    candidate = jnp.where(before, peaks + suffix, floor_log)
    state_peak = jnp.max(candidate, axis=0)
    fade = jnp.where(before, jnp.exp(candidate - state_peak[None]), 0.0)
    state = jnp.sum(everything[:, :, :head_size] * fade[:, :, None, None], axis=0)
    cell_list = []
    for h in range(heads):
        c, gate = cumulative[h], input_gate[h]
        within = jnp.where(causal, c[:, None] - c[None, :] + gate[None, :], -jnp.inf)
        carried = c + state_peak[h]
        top = jnp.maximum(jnp.max(within, axis=-1), carried)
        raw = lax.dot_general(
            query_heads[h], key_heads[h], (((1,), (1,)), ((), ())), preferred_element_type=jnp.float32
        )
        scores = raw * scale * jnp.exp(within - top[:, None])
        cells = jnp.dot(
            scores.astype(jnp.bfloat16), value_heads[h], preferred_element_type=jnp.float32
        )
        carried_cells = lax.dot_general(
            query_heads[h].astype(jnp.float32),
            state[h],
            (((1,), (1,)), ((), ())),
            precision=highest,
        )
        cells = cells + jnp.exp(carried - top)[:, None] * carried_cells
        cell_list.append(rms_rows(cells, gain_local[h]).astype(jnp.bfloat16))
    cell_rows = jnp.concatenate(cell_list, axis=1)
    return jnp.dot(cell_rows, mixer_out_weight, preferred_element_type=jnp.float32).astype(
        jnp.bfloat16
    )


def shards(
    mixer_in,
    mixer_gain,
    query_weight,
    key_weight,
    value_weight,
    input_gate,
    forget_gate,
    head_gain,
    mixer_out_weight,
    expert_in,
    expert_gain,
    group_router,
    expert_router,
    routes,
    gate_experts,
    up_experts,
    down_experts,
):
    normed_b = rms_rows(expert_in, expert_gain).astype(jnp.bfloat16)
    tokens = normed_b.shape[0]
    expert_total = expert_router.shape[1]
    members = expert_total // group_router.shape[1]
    capacity = 4 * tokens // expert_total
    share = capacity // lax.axis_size("tp")
    group_logits = jnp.dot(normed_b, group_router, preferred_element_type=jnp.float32)
    expert_logits = jnp.dot(normed_b, expert_router, preferred_element_type=jnp.float32)
    expert_ids = jnp.arange(expert_total, dtype=jnp.int32)
    group_ids = jnp.arange(group_router.shape[1], dtype=jnp.int32)
    named = [routes[:, k : k + 1] == expert_ids[None, :] for k in range(2)]
    chosen = [jnp.sum(jnp.where(m, expert_logits, 0.0), axis=1, keepdims=True) for m in named]
    combine = jnp.zeros((tokens, expert_total), jnp.float32)
    for k in range(2):
        in_group = routes[:, k : k + 1] // members == group_ids[None, :]
        group_pick = jnp.sum(jnp.where(in_group, group_logits, 0.0), axis=1, keepdims=True)
        weight = jax.nn.sigmoid(group_pick) * jax.nn.sigmoid(chosen[k] - chosen[1 - k])
        combine = combine + jnp.where(named[k], weight, 0.0)
    matches = named[0] | named[1]
    earlier = jnp.tril(jnp.ones((tokens, tokens), jnp.bfloat16), -1)
    rank = jnp.dot(
        earlier, matches.astype(jnp.bfloat16), preferred_element_type=jnp.float32
    ).astype(jnp.int32)
    rank = jnp.where(matches, rank, -1)
    slots = jnp.arange(capacity, dtype=jnp.int32)
    mix = jnp.where(
        rank[:, :, None] == slots[None, None, :], combine[:, :, None], 0.0
    ).reshape(tokens, expert_total * capacity)
    tp_place = lax.axis_index("tp")
    fused = lax.axis_size("tp") == 4 and share % 16 == 0 and lax.axis_size("ep") >= 4
    fused = fused and mixer_in.shape[0] % 512 == 0 and input_gate.shape[0] == 2
    fused = fused and gate_experts.shape[0] == 1 and is_power(lax.axis_size("ep"))
    pieces = 2 if fused else 1
    place = lax.rem(tp_place, 2) * 2 if fused else tp_place
    own_slots = place * share + jnp.arange(pieces * share, dtype=jnp.int32)
    select = (rank.T[:, None, :] == own_slots[None, :, None]).astype(jnp.bfloat16)
    own_share = (
        jnp.dot(
            select.reshape(expert_total * pieces * share, tokens),
            normed_b,
            preferred_element_type=jnp.float32,
        )
        .astype(jnp.bfloat16)
        .reshape(expert_total, pieces * share, normed_b.shape[1])
    )
    normed_a = rms_rows(mixer_in, mixer_gain).astype(jnp.bfloat16)
    prepared = mixer_prepare(
        normed_a, query_weight, key_weight, value_weight, input_gate, forget_gate
    )
    width_local = query_weight.shape[1]
    gain_local = lax.dynamic_slice_in_dim(
        head_gain, lax.axis_index("tp") * width_local, width_local
    ).reshape(input_gate.shape[0], -1)
    experts = (own_share, gate_experts[0], up_experts[0], down_experts[0], mix)
    if fused:
        expert_out, mixer_out = all_fused(*experts, prepared, gain_local, mixer_out_weight)
    else:
        partial = mixer_partial(prepared, gain_local, mixer_out_weight)
        mixer_out = lax.psum_scatter(partial, "tp", scatter_dimension=0, tiled=True)
        expert_out = experts_plain(*experts)
    return (mixer_out, expert_out)


def solution(mesh):
    in_specs = (
        P("ep", None),
        P(),
        P(None, "tp"),
        P(None, "tp"),
        P(None, "tp"),
        P("tp", "ep"),
        P("tp", "ep"),
        P(),
        P("tp", None),
        P("ep", None),
        P(),
        P(),
        P(),
        P("ep", None),
        P("ep", None, "tp"),
        P("ep", None, "tp"),
        P("ep", "tp", None),
    )
    out_specs = (P(("ep", "tp"), None), P("ep", "tp"))
    return jax.shard_map(shards, mesh=mesh, in_specs=in_specs, out_specs=out_specs, check_vma=False)
```

```python
import functools

import jax
import jax.numpy as jnp
from jax import lax
from jax.experimental import pallas as pl
from jax.experimental.pallas import tpu as pltpu
from jax.sharding import PartitionSpec as P

MESH = pl.DeviceIdType.MESH


epsilon = 1e-06
highest = lax.Precision.HIGHEST
floor_log = -1e30


def is_power(count):
    return count & (count - 1) == 0


def rms_rows(matrix, gain):
    widened = matrix.astype(jnp.float32)
    scaled = widened * lax.rsqrt(jnp.mean(widened * widened, axis=-1, keepdims=True) + epsilon)
    return scaled * gain


def merged(earlier_memory, earlier_peak, later_memory, later_peak, later_total):
    moved = later_total + earlier_peak
    peak = jnp.maximum(moved, later_peak)
    return jnp.exp(moved - peak) * earlier_memory + jnp.exp(later_peak - peak) * later_memory, peak


def three_parts(matrix):
    parts = []
    for _ in range(3):
        top_part = matrix.astype(jnp.bfloat16)
        parts.append(top_part)
        matrix = matrix - top_part.astype(jnp.float32)
    return parts


nn = (((1,), (0,)), ((), ()))
nt = (((1,), (1,)), ((), ()))
tn = (((0,), (0,)), ((), ()))


def product(left, right, numbers):
    return lax.dot_general(left, right, numbers, preferred_element_type=jnp.float32)


def normalize(source, gain_ref, target):
    block = 64

    def body(b, carry):
        place = pl.ds(pl.multiple_of(b * block, block), block)
        widened = source[place, :].astype(jnp.float32)
        mean = jnp.mean(widened * widened, axis=-1, keepdims=True)
        factor = lax.rsqrt(mean + epsilon)
        target[place, :] = (source[place, :].astype(jnp.float32) * factor * gain_ref[...]).astype(
            target.dtype
        )
        return carry

    lax.fori_loop(0, source.shape[0] // block, body, 0)


def whole_kernel(
    sizes, mixer_hbm, expert_hbm, query_hbm, key_hbm, value_hbm, project_hbm, gate_hbm, up_hbm, down_hbm,
    mixer_gain_ref, expert_gain_ref, head_gain_ref, in_ref, forget_ref,
    group_router_ref, expert_router_ref, routes_ref,
    out_ref, mixed_ref,
    mixer_in, expert_in, query_w, key_w, value_w, project_ref, gate_ref, up_ref, down_ref,
    normed_a, normed_b, rank, combine, near_rows, far_rows,
    query_ref, key_ref, value_ref, cum_ref, cum_col_ref, packed_ref, acc,
    rows, part, pin, csum, xin, fin, ret,
    peer, plane, mem, pre, pre_in, state, state_peak, state_parts, mpart, mpin, msum, mxin,
    own_sem, send_a, recv_a, send_x, recv_x, send_p, recv_p,
    send_q, recv_q, send_c, recv_c, send_r, recv_r,
    send_m, recv_m, send_k, recv_k, send_h, recv_h, send_y, recv_y,
):
    n, share, cap, width, quarter, heads, size = sizes
    near = n // 2
    planes = n // 2
    me, tp = lax.axis_index("ep"), lax.axis_index("tp")
    core, column = lax.rem(tp, 2), lax.div(tp, 2)
    pair = tp + 1 - 2 * core
    cross = lax.rem(tp + 2, 4)
    pair_cross = lax.rem(pair + 2, 4)
    side, level = lax.rem(me, 2), lax.div(me, 2)
    mate = me + 1 - 2 * side
    tokens = expert_in.shape[0]
    length = mixer_in.shape[0]
    chunk = length // 4
    scale = size ** (-0.5)

    def other(i):
        total, bit = 0, 1
        while bit < n:
            total = total + bit * lax.rem(lax.div(me, bit) + lax.div(i, bit), 2)
            bit *= 2
        return total

    high = lax.rem(lax.div(me, near), 2)
    inner = lax.rem(high + lax.div(lax.rem(me, near), near // 2), 2)

    def turn(t):
        half = near // 2
        swapped = near + lax.rem(t - near + inner * half, near)
        return jnp.where(t < near, t, swapped)

    def remote(src, dst, send, recv, to):
        return pltpu.make_async_remote_copy(
            src_ref=src, dst_ref=dst, send_sem=send, recv_sem=recv, device_id=to, device_id_type=MESH
        )

    barrier = pltpu.get_barrier_semaphore()
    for i in range(1, n):
        pl.semaphore_signal(
            barrier, inc=1, device_id=(lax.rem(me + i, n), tp), device_id_type=MESH
        )
    pl.semaphore_signal(barrier, inc=1, device_id=(me, pair), device_id_type=MESH)
    pl.semaphore_signal(barrier, inc=1, device_id=(me, cross), device_id_type=MESH)

    loads = [
        pltpu.make_async_copy(src, dst, own_sem.at[k])
        for k, (src, dst) in enumerate(
            [
                (expert_hbm, expert_in), (gate_hbm, gate_ref), (up_hbm, up_ref),
                (down_hbm, down_ref), (mixer_hbm, mixer_in), (key_hbm, key_w),
                (value_hbm, value_w), (query_hbm, query_w), (project_hbm, project_ref),
            ]
        )
    ]
    for load in loads:
        load.start()

    def scatter_near(i, place):
        slot = jnp.maximum(i - 1, 0)
        return remote(
            near_rows.at[slot], rows.at[place, core], send_a.at[i], recv_a.at[i], (other(i), tp)
        )

    def scatter_far(i, place):
        slot = jnp.maximum(i - near, 0)
        mine = pl.ds(pl.multiple_of(column * share, share), share)
        return remote(
            far_rows.at[slot], rows.at[place, core, mine], send_a.at[i], recv_a.at[i], (other(i), tp)
        )

    def across(s, which):
        mine = pl.ds(pl.multiple_of(which * share, share), share)
        return remote(
            rows.at[s, core, mine], rows.at[s, core, mine], send_x.at[s], recv_x.at[s], (me, cross)
        )

    def beside(s, which):
        return remote(
            rows.at[s, which], rows.at[s, which], send_p.at[s], recv_p.at[s], (me, pair)
        )

    def halves(s, k, who):
        return remote(part.at[s, who], pin.at[s, k], send_q.at[s, k], recv_q.at[s, k], (me, pair))

    def summed(s):
        return remote(csum.at[s], xin.at[s], send_c.at[s], recv_c.at[s], (me, cross))

    def back(i):
        to = other(i)
        return remote(fin.at[to], ret.at[me], send_r.at[i], recv_r.at[i], (to, tp))

    def to_mate():
        return remote(packed_ref, peer, send_k.at[0], recv_k.at[0], (mate, tp))

    def to_level(d):
        return remote(
            plane, mem.at[level], send_m.at[d], recv_m.at[d], (lax.rem(me + 2 * d, n), tp)
        )

    def from_level(d):
        return remote(
            plane, mem.at[level - d], send_m.at[d], recv_m.at[d], (lax.rem(me + 2 * d, n), tp)
        )

    def prefix_mate():
        return remote(pre, pre_in, send_k.at[1], recv_k.at[1], (mate, tp))

    def mixed_half(k, who):
        return remote(mpart.at[who], mpin.at[k], send_h.at[k], recv_h.at[k], (me, pair))

    def mixed_sum(q):
        return remote(msum.at[q], mxin.at[q], send_y.at[q], recv_y.at[q], (me, cross))

    body, top_row, sum_row = slice(0, size), slice(size, size + 1), slice(size + 1, size + 2)

    def picks(e, first, count):
        slots = lax.broadcasted_iota(jnp.int32, (count, tokens), 0) + first
        return rank[pl.ds(e, 1), :] == slots.astype(jnp.float32)

    def gathered(parts):
        select = jnp.concatenate([jnp.where(p, 1.0, 0.0).astype(jnp.bfloat16) for p in parts], axis=0)
        return product(select, normed_b[...], nn).astype(jnp.bfloat16)

    def prepare_rank():
        experts = lax.broadcasted_iota(jnp.int32, (n, tokens), 0)
        matches = (routes_ref[0:1, :] == experts) | (routes_ref[1:2, :] == experts)
        earlier = lax.broadcasted_iota(jnp.int32, (tokens, tokens), 0)
        earlier = earlier < lax.broadcasted_iota(jnp.int32, (tokens, tokens), 1)
        count = product(
            jnp.where(matches, 1.0, 0.0).astype(jnp.bfloat16),
            jnp.where(earlier, 1.0, 0.0).astype(jnp.bfloat16),
            nn,
        )
        rank[...] = jnp.where(matches, count, -1.0)

    def prepare_combine():
        experts = lax.broadcasted_iota(jnp.int32, (n, tokens), 0)
        groups = group_router_ref.shape[0]
        expert_logits = product(expert_router_ref[...], normed_b[...], nt)
        group_logits = product(group_router_ref[...], normed_b[...], nt)
        group_full = jnp.zeros((n, tokens), jnp.float32)
        for g in range(groups):
            inside = (experts >= g * (n // groups)) & (experts < (g + 1) * (n // groups))
            group_full = group_full + jnp.where(inside, group_logits[g : g + 1, :], 0.0)
        named = [routes_ref[k : k + 1, :] == experts for k in range(2)]
        chosen = [jnp.sum(jnp.where(m, expert_logits, 0.0), axis=0, keepdims=True) for m in named]
        total = jnp.zeros((n, tokens), jnp.float32)
        for k in range(2):
            group_pick = jnp.sum(jnp.where(named[k], group_full, 0.0), axis=0, keepdims=True)
            weight = jax.nn.sigmoid(group_pick) * jax.nn.sigmoid(chosen[k] - chosen[1 - k])
            total = total + jnp.where(named[k], weight, 0.0)
        combine[...] = total

    def prepare_near():
        step_rows = 2 * share
        moved = gathered([picks(other(i), core * step_rows, step_rows) for i in range(1, near)])
        for i in range(1, near):
            near_rows[i - 1] = moved[(i - 1) * step_rows : i * step_rows]

    def prepare_far():
        first = core * (2 * share) + column * share
        moved = gathered([picks(other(i), first, share) for i in range(near, n)])
        for i in range(near, n):
            far_rows[i - near] = moved[(i - near) * share : (i - near + 1) * share]

    def prepare_own():
        rows[me] = gathered([picks(me, 0, cap)]).reshape(2, 2 * share, width)

    def ffn(s):
        x = rows[s].reshape(cap, width)
        gate_act = jnp.dot(x, gate_ref[...], preferred_element_type=jnp.float32)
        up_act = jnp.dot(x, up_ref[...], preferred_element_type=jnp.float32)
        hidden = (gate_act * jax.nn.sigmoid(gate_act) * up_act).astype(jnp.bfloat16)
        for q in range(4):
            part[s, q] = jnp.dot(
                hidden,
                down_ref[:, q * quarter : (q + 1) * quarter],
                preferred_element_type=jnp.float32,
            ).astype(jnp.bfloat16)

    def prepare_gates():
        log_forget = jnp.minimum(forget_ref[...], 0.0) - jnp.log1p(jnp.exp(-jnp.abs(forget_ref[...])))
        pieces = jnp.concatenate(
            [p.astype(jnp.float32) for p in three_parts(log_forget)]
            + [jnp.zeros((16 - 3 * heads, length), jnp.float32)],
            axis=0,
        ).astype(jnp.bfloat16)
        first = lax.broadcasted_iota(jnp.int32, (length, length), 0)
        upto = first <= lax.broadcasted_iota(jnp.int32, (length, length), 1)
        sums = product(pieces, jnp.where(upto, 1.0, 0.0).astype(jnp.bfloat16), nn)
        cum_ref[...] = sums[2 * heads : 3 * heads] + sums[heads : 2 * heads] + sums[0:heads]
        back_to = first >= lax.broadcasted_iota(jnp.int32, (length, length), 1)
        sums = product(jnp.where(back_to, 1.0, 0.0).astype(jnp.bfloat16), pieces, nt)
        cum_col_ref[...] = (
            sums[:, 2 * heads : 3 * heads] + sums[:, heads : 2 * heads] + sums[:, 0:heads]
        )

    def prepare_memory():
        key_ref[...] = jnp.dot(
            normed_a[...], key_w[...], preferred_element_type=jnp.float32
        ).astype(jnp.bfloat16)
        value_ref[...] = jnp.dot(
            normed_a[...], value_w[...], preferred_element_type=jnp.float32
        ).astype(jnp.bfloat16)
        for h in range(heads):
            cols = slice(h * size, (h + 1) * size)
            cum = cum_ref[h : h + 1, :]
            total = cum_ref[h : h + 1, length - 1 : length]
            log_weight = total - cum + in_ref[h : h + 1, :]
            peak = jnp.max(log_weight, axis=1, keepdims=True)
            weighted = value_ref[:, cols].astype(jnp.float32).T * jnp.exp(log_weight - peak)
            memory = jnp.zeros((size, size), jnp.float32)
            for piece in three_parts(weighted)[::-1]:
                memory = memory + product(piece, key_ref[:, cols], nn)
            packed_ref[h, body] = memory * scale
            packed_ref[h, size : size + 8] = jnp.zeros((8, size), jnp.float32)
            packed_ref[h, top_row] = jnp.broadcast_to(peak, (1, size))
            packed_ref[h, sum_row] = jnp.broadcast_to(total, (1, size))

    def prepare_query():
        query_ref[...] = jnp.dot(
            normed_a[...], query_w[...], preferred_element_type=jnp.float32
        ).astype(jnp.bfloat16)

    def combine_plane():
        to_mate().wait_recv()

        def joined(first, second):
            memory, peak = merged(
                first[side, body], first[side, top_row],
                second[side, body], second[side, top_row], second[side, sum_row],
            )
            plane[size : size + 8] = jnp.zeros((8, size), jnp.float32)
            plane[body] = memory
            plane[top_row] = peak
            plane[sum_row] = first[side, sum_row] + second[side, sum_row]

        @pl.when(side == 0)
        def _():
            joined(packed_ref, peer)

        @pl.when(side == 1)
        def _():
            joined(peer, packed_ref)

        for d in range(1, planes):
            @pl.when(level + d < planes)
            def _():
                to_level(d).start()

    def combine_levels():
        pre[...] = jnp.zeros_like(pre)
        pre[top_row] = jnp.full((1, size), floor_log, jnp.float32)
        for k in range(planes - 1):
            d = planes - 1 - k

            @pl.when(d <= level)
            def _():
                from_level(d).wait_recv()
                z = level - d
                memory, peak = merged(
                    pre[body], pre[top_row], mem[z, body], mem[z, top_row], mem[z, sum_row]
                )
                pre[body] = memory
                pre[top_row] = peak

        prefix_mate().start()

    def combine_last():
        prefix_mate().wait_recv()
        state[side] = pre[body]
        state_peak[side, 0:1, :] = pre[top_row]
        state[1 - side] = pre_in[body]
        state_peak[1 - side, 0:1, :] = pre_in[top_row]

        @pl.when(side == 1)
        def _():
            for h in range(heads):
                memory, peak = merged(
                    state[h], state_peak[h, 0:1, :],
                    peer[h, body], peer[h, top_row], peer[h, sum_row],
                )
                state[h] = memory
                state_peak[h, 0:1, :] = peak

        for h in range(heads):
            for piece, value in enumerate(three_parts(state[h])):
                state_parts[h, piece] = value

    def attend(j):
        start = pl.multiple_of(j * chunk, chunk)
        row = start + lax.broadcasted_iota(jnp.int32, (chunk, length), 0)
        causal = row >= lax.broadcasted_iota(jnp.int32, (chunk, length), 1)
        cell_list = []
        for h in range(heads):
            cols = slice(h * size, (h + 1) * size)
            q = query_ref[pl.ds(start, chunk), cols]
            c = cum_col_ref[pl.ds(start, chunk), h : h + 1]
            within = jnp.where(causal, c - cum_ref[h : h + 1, :] + in_ref[h : h + 1, :], -jnp.inf)
            carried = c + state_peak[h, 0:1, 0:1]
            top = jnp.maximum(jnp.max(within, axis=1, keepdims=True), carried)
            raw = product(q, key_ref[:, cols], nt)
            scores = (raw * scale * jnp.exp(within - top)).astype(jnp.bfloat16)
            cells = jnp.dot(scores, value_ref[:, cols], preferred_element_type=jnp.float32)
            held = jnp.zeros((chunk, size), jnp.float32)
            for piece in (2, 1, 0):
                held = held + product(q, state_parts[h, piece], nt)
            cells = cells + jnp.exp(carried - top) * held
            mean = jnp.mean(cells * cells, axis=1, keepdims=True)
            gain = head_gain_ref[pl.ds(tp * heads + h, 1), :]
            cell_list.append((cells * lax.rsqrt(mean + epsilon) * gain).astype(jnp.bfloat16))
        cell_rows = jnp.concatenate(cell_list, axis=1)
        for q in range(4):
            cols = slice(q * quarter, (q + 1) * quarter)
            mpart[j, q] = jnp.dot(
                cell_rows, project_ref[:, cols], preferred_element_type=jnp.float32
            ).astype(jnp.bfloat16)

    begin = 4

    def mixer_step(t):
        @pl.when(t == 1)
        def _():
            combine_plane()

            @pl.when(inner == 0)
            def _():
                send_far()

        @pl.when(t == 3)
        def _():
            combine_levels()

        @pl.when(t == begin)
        def _():
            combine_last()

        @pl.when((t >= begin) & (t < begin + 4))
        def _():
            k = t - begin
            attend(jnp.where(k == 0, pair_cross, jnp.where(k == 1, pair, jnp.where(k == 2, cross, tp))))

        @pl.when(t == begin)
        def _():
            mixed_half(1, pair_cross).start()

        @pl.when(t == begin + 1)
        def _():
            mixed_half(0, pair).start()

        @pl.when(t == begin + 2)
        def _():
            mixed_half(1, pair_cross).wait_recv()
            msum[...] = (
                mpart[cross].astype(jnp.float32) + mpin[1].astype(jnp.float32)
            ).astype(jnp.bfloat16)

        @pl.when((t >= begin + 2) & (t < begin + 6))
        def _():
            mixed_sum(t - begin - 2).start()

    def send_far():
        def one(t, carry):
            scatter_far(turn(t), me).start()
            return carry

        lax.fori_loop(near, n, one, 0)

    def collect(s):
        halves(s, 1, pair_cross).wait_recv()
        csum[s] = (
            part[s, cross].astype(jnp.float32) + pin[s, 1].astype(jnp.float32)
        ).astype(jnp.bfloat16)
        summed(s).start()

    def send_halves(s):
        halves(s, 1, pair_cross).start()
        halves(s, 0, pair).start()

    prepare_rank()
    loads[0].wait()
    normalize(expert_in, expert_gain_ref, normed_b)
    prepare_near()
    prepare_far()
    pl.semaphore_wait(barrier, n + 1)
    for i in range(1, near):
        scatter_near(i, me).start()

    @pl.when(inner == 1)
    def _():
        send_far()

    prepare_own()
    for k in (1, 2, 3):
        loads[k].wait()
    ffn(me)
    send_halves(me)
    loads[4].wait()
    normalize(mixer_in, mixer_gain_ref, normed_a)
    collect(me)
    prepare_gates()
    loads[5].wait()
    loads[6].wait()
    prepare_memory()
    to_mate().start()
    loads[7].wait()
    prepare_query()
    prepare_combine()
    loads[8].wait()

    def step(t, carry):
        @pl.when((t >= near + 1) & (t < n + 1))
        def _():
            s = other(turn(t - 1))
            across(s, 1 - column).wait_recv()
            beside(s, core).start()

        @pl.when(t >= 2)
        def _():
            mixer_step(t)

        @pl.when((t >= 2) & (t < n + 1))
        def _():
            s = other(turn(t - 1))
            beside(s, 1 - core).wait_recv()
            ffn(s)
            send_halves(s)

        @pl.when(t < near)
        def _():
            s = other(t)
            scatter_near(t, s).wait_recv()
            beside(s, core).start()

        @pl.when((t >= near) & (t < n))
        def _():
            i = turn(t)
            s = other(i)
            scatter_far(i, s).wait_recv()
            across(s, column).start()

        @pl.when(t == 1)
        def _():
            mixer_step(t)

        @pl.when((t >= 2) & (t < n + 1))
        def _():
            collect(other(turn(t - 1)))

        @pl.when(t >= 2)
        def _():
            i = turn(t - 2)
            s = other(i)
            halves(s, 0, pair).wait_recv()
            summed(s).wait_recv()
            total = (
                part[s, tp].astype(jnp.float32)
                + pin[s, 0].astype(jnp.float32)
                + xin[s].astype(jnp.float32)
            ).astype(jnp.bfloat16)

            @pl.when(i > 0)
            def _():
                fin[s] = total
                back(i).start()

            @pl.when(i == 0)
            def _():
                ret[s] = total

        return carry

    lax.fori_loop(1, n + 2, step, 0)

    mixed_half(0, pair).wait_recv()
    for q in range(4):
        mixed_sum(q).wait_recv()
        cols = slice(q * quarter, (q + 1) * quarter)
        mixed_ref[:, cols] = (
            mpart[tp, q].astype(jnp.float32)
            + mpin[0, q].astype(jnp.float32)
            + mxin[q].astype(jnp.float32)
        ).astype(mixed_ref.dtype)

    acc[...] = jnp.zeros_like(acc)

    def finish(t, carry):
        i = turn(t)
        s = other(i)

        @pl.when(t > 0)
        def _():
            back(i).wait_recv()

        chosen = picks(s, 0, cap)
        weight = combine[pl.ds(s, 1), :]
        high_weight = weight.astype(jnp.bfloat16).astype(jnp.float32)
        table = ret[s]
        acc[...] += product(
            jnp.where(chosen, high_weight, 0.0).astype(jnp.bfloat16), table, tn
        ) + product(jnp.where(chosen, weight - high_weight, 0.0).astype(jnp.bfloat16), table, tn)
        return carry

    lax.fori_loop(0, n, finish, 0)
    out_ref[...] = acc[...].astype(out_ref.dtype)

    def drain(i, carry):
        s = other(i)
        halves(s, 0, pair).wait_send()
        halves(s, 1, pair_cross).wait_send()
        summed(s).wait_send()

        @pl.when(i > 0)
        def _():
            beside(s, core).wait_send()
            back(i).wait_send()

        @pl.when((i > 0) & (i < near))
        def _():
            scatter_near(i, me).wait_send()

        @pl.when(i >= near)
        def _():
            scatter_far(i, me).wait_send()
            across(s, column).wait_send()

        return carry

    lax.fori_loop(0, n, drain, 0)
    to_mate().wait_send()
    prefix_mate().wait_send()
    for d in range(1, planes):
        @pl.when(level + d < planes)
        def _():
            to_level(d).wait_send()
    mixed_half(0, pair).wait_send()
    mixed_half(1, pair_cross).wait_send()
    for q in range(4):
        mixed_sum(q).wait_send()


def all_fused(
    mixer_in, mixer_gain, query_weight, key_weight, value_weight, input_gate, forget_gate,
    head_gain, mixer_out_weight, expert_in, expert_gain, group_router, expert_router, routes,
    gate_weight, up_weight, down_weight,
):
    n = expert_router.shape[1]
    tokens, width = expert_in.shape
    cap = 4 * tokens // n
    share = cap // 4
    quarter = width // 4
    length = mixer_in.shape[0]
    heads = input_gate.shape[0]
    inner_width = query_weight.shape[1]
    size = inner_width // heads
    hidden = gate_weight.shape[1]
    chunk = length // 4
    vmem = pl.BlockSpec(memory_space=pltpu.VMEM)
    whole = pl.BlockSpec(memory_space=pl.ANY)
    dma = pltpu.SemaphoreType.DMA
    bf = jnp.bfloat16
    f32 = jnp.float32
    return pl.pallas_call(
        functools.partial(whole_kernel, (n, share, cap, width, quarter, heads, size)),
        out_shape=(
            jax.ShapeDtypeStruct((tokens, quarter), bf),
            jax.ShapeDtypeStruct((chunk, width), bf),
        ),
        in_specs=[whole] * 9 + [vmem] * 8,
        out_specs=(vmem, vmem),
        scratch_shapes=[
            pltpu.VMEM((length, width), bf),
            pltpu.VMEM((tokens, width), bf),
            pltpu.VMEM((width, inner_width), bf),
            pltpu.VMEM((width, inner_width), bf),
            pltpu.VMEM((width, inner_width), bf),
            pltpu.VMEM((inner_width, width), bf),
            pltpu.VMEM((width, hidden), bf),
            pltpu.VMEM((width, hidden), bf),
            pltpu.VMEM((hidden, width), bf),
            pltpu.VMEM((length, width), bf),
            pltpu.VMEM((tokens, width), bf),
            pltpu.VMEM((n, tokens), f32),
            pltpu.VMEM((n, tokens), f32),
            pltpu.VMEM((n // 2 - 1, 2 * share, width), bf),
            pltpu.VMEM((n // 2, share, width), bf),
            pltpu.VMEM((length, inner_width), bf),
            pltpu.VMEM((length, inner_width), bf),
            pltpu.VMEM((length, inner_width), bf),
            pltpu.VMEM((heads, length), f32),
            pltpu.VMEM((length, heads), f32),
            pltpu.VMEM((heads, size + 8, size), f32),
            pltpu.VMEM((tokens, quarter), f32),
            pltpu.VMEM((n, 2, 2 * share, width), bf),
            pltpu.VMEM((n, 4, cap, quarter), bf),
            pltpu.VMEM((n, 2, cap, quarter), bf),
            pltpu.VMEM((n, cap, quarter), bf),
            pltpu.VMEM((n, cap, quarter), bf),
            pltpu.VMEM((n, cap, quarter), bf),
            pltpu.VMEM((n, cap, quarter), bf),
            pltpu.VMEM((heads, size + 8, size), f32),
            pltpu.VMEM((size + 8, size), f32),
            pltpu.VMEM((n // 2, size + 8, size), f32),
            pltpu.VMEM((size + 8, size), f32),
            pltpu.VMEM((size + 8, size), f32),
            pltpu.VMEM((heads, size, size), f32),
            pltpu.VMEM((heads, 8, size), f32),
            pltpu.VMEM((heads, 3, size, size), bf),
            pltpu.VMEM((4, 4, chunk, quarter), bf),
            pltpu.VMEM((2, 4, chunk, quarter), bf),
            pltpu.VMEM((4, chunk, quarter), bf),
            pltpu.VMEM((4, chunk, quarter), bf),
            dma((9,)),
            dma((n,)), dma((n,)), dma((n,)), dma((n,)), dma((n,)), dma((n,)),
            dma((n, 2)), dma((n, 2)), dma((n,)), dma((n,)), dma((n,)), dma((n,)),
            dma((n // 2,)), dma((n // 2,)), dma((2,)), dma((2,)), dma((2,)), dma((2,)),
            dma((4,)), dma((4,)),
        ],
        compiler_params=pltpu.CompilerParams(
            collective_id=0, has_side_effects=True, vmem_limit_bytes=60 * 1024 * 1024
        ),
        cost_estimate=pl.CostEstimate(
            flops=60_000_000_000, bytes_accessed=8_000_000, transcendentals=0
        ),
    )(
        mixer_in, expert_in, query_weight, key_weight, value_weight, mixer_out_weight,
        gate_weight, up_weight, down_weight,
        mixer_gain.reshape(1, width), expert_gain.reshape(1, width),
        head_gain.reshape(-1, size), input_gate, forget_gate,
        group_router.T, expert_router.T, routes.T,
    )


def experts_plain(own_share, gate_weight, up_weight, down_weight, mix):
    arrived = lax.all_to_all(own_share, "ep", split_axis=0, concat_axis=0, tiled=True)
    piece_rows = lax.all_gather(arrived, "tp", axis=1, tiled=True)
    gate_act = jnp.einsum(
        "scd,df->scf", piece_rows, gate_weight, preferred_element_type=jnp.float32
    )
    up_act = jnp.einsum("scd,df->scf", piece_rows, up_weight, preferred_element_type=jnp.float32)
    hidden = (jax.nn.silu(gate_act) * up_act).astype(jnp.bfloat16)
    partial_rows = jnp.einsum(
        "scf,fo->sco", hidden, down_weight, preferred_element_type=jnp.float32
    )
    summed = lax.psum_scatter(
        partial_rows.astype(jnp.bfloat16), "tp", scatter_dimension=2, tiled=True
    )
    returned = lax.all_to_all(summed, "ep", split_axis=0, concat_axis=0, tiled=True)
    return jnp.dot(
        mix, returned.reshape(-1, returned.shape[2]).astype(jnp.float32), precision=highest
    ).astype(jnp.bfloat16)


def mixer_prepare(normed_a, query_weight, key_weight, value_weight, input_gate, forget_gate):
    def project(weight):
        return jnp.dot(normed_a, weight, preferred_element_type=jnp.float32).astype(jnp.bfloat16)

    rows = normed_a.shape[0]
    heads = input_gate.shape[0]
    width_local = query_weight.shape[1]
    head_size = width_local // heads
    scale = head_size ** (-0.5)
    causal = jnp.tril(jnp.ones((rows, rows), dtype=bool))
    log_forget = jax.nn.log_sigmoid(forget_gate)
    cumulative = jnp.einsum(
        "hs,ts->ht", log_forget, causal.astype(jnp.float32), precision=highest
    )
    total = cumulative[:, -1]
    log_weight = total[:, None] - cumulative + input_gate
    peak = jnp.max(log_weight, axis=-1)
    weights = jnp.exp(log_weight - peak[:, None])
    keys = project(key_weight)
    values = project(value_weight)

    def by_head(matrix):
        return [matrix[:, h * head_size : (h + 1) * head_size] for h in range(heads)]

    key_heads, value_heads = by_head(keys), by_head(values)
    memory = jnp.stack(
        [
            lax.dot_general(
                value_heads[h].astype(jnp.float32) * weights[h][:, None],
                key_heads[h].astype(jnp.float32) * scale,
                (((0,), (0,)), ((), ())),
                precision=highest,
            )
            for h in range(heads)
        ]
    )
    stats = jnp.stack([peak, total], axis=1)
    stats = jnp.concatenate([stats, jnp.zeros((heads, 6), jnp.float32)], axis=1)
    packed = jnp.concatenate(
        [memory, jnp.broadcast_to(stats[:, :, None], (heads, 8, head_size))], axis=1
    )
    return (packed, project(query_weight), keys, values, cumulative, input_gate)


def mixer_partial(prepared, gain_local, mixer_out_weight):
    packed, queries, keys, values, cumulative, input_gate = prepared
    rows = queries.shape[0]
    heads, head_size = gain_local.shape
    scale = head_size ** (-0.5)
    causal = jnp.tril(jnp.ones((rows, rows), dtype=bool))

    def by_head(matrix):
        return [matrix[:, h * head_size : (h + 1) * head_size] for h in range(heads)]

    query_heads, key_heads, value_heads = by_head(queries), by_head(keys), by_head(values)
    everything = lax.all_gather(packed, "ep")
    n, place = lax.axis_size("ep"), lax.axis_index("ep")
    peaks = everything[:, :, head_size, 0]
    totals = everything[:, :, head_size + 1, 0]
    order = jnp.arange(n)
    later = (order[None, :] > order[:, None]) & (order[None, :] < place)
    suffix = jnp.sum(jnp.where(later[:, :, None], totals[None], 0.0), axis=1)
    before = (order < place)[:, None]
    candidate = jnp.where(before, peaks + suffix, floor_log)
    state_peak = jnp.max(candidate, axis=0)
    fade = jnp.where(before, jnp.exp(candidate - state_peak[None]), 0.0)
    state = jnp.sum(everything[:, :, :head_size] * fade[:, :, None, None], axis=0)
    cell_list = []
    for h in range(heads):
        c, gate = cumulative[h], input_gate[h]
        within = jnp.where(causal, c[:, None] - c[None, :] + gate[None, :], -jnp.inf)
        carried = c + state_peak[h]
        top = jnp.maximum(jnp.max(within, axis=-1), carried)
        raw = lax.dot_general(
            query_heads[h], key_heads[h], (((1,), (1,)), ((), ())), preferred_element_type=jnp.float32
        )
        scores = raw * scale * jnp.exp(within - top[:, None])
        cells = jnp.dot(
            scores.astype(jnp.bfloat16), value_heads[h], preferred_element_type=jnp.float32
        )
        carried_cells = lax.dot_general(
            query_heads[h].astype(jnp.float32),
            state[h],
            (((1,), (1,)), ((), ())),
            precision=highest,
        )
        cells = cells + jnp.exp(carried - top)[:, None] * carried_cells
        cell_list.append(rms_rows(cells, gain_local[h]).astype(jnp.bfloat16))
    cell_rows = jnp.concatenate(cell_list, axis=1)
    return jnp.dot(cell_rows, mixer_out_weight, preferred_element_type=jnp.float32).astype(
        jnp.bfloat16
    )


def shards(
    mixer_in,
    mixer_gain,
    query_weight,
    key_weight,
    value_weight,
    input_gate,
    forget_gate,
    head_gain,
    mixer_out_weight,
    expert_in,
    expert_gain,
    group_router,
    expert_router,
    routes,
    gate_experts,
    up_experts,
    down_experts,
):
    ranks = lax.axis_size("ep")
    share = expert_in.shape[0] // expert_router.shape[1]
    fused = lax.axis_size("tp") == 4 and ranks >= 4 and is_power(ranks) and share % 16 == 0
    fused = fused and mixer_in.shape[0] % 512 == 0 and input_gate.shape[0] == 2
    fused = fused and gate_experts.shape[0] == 1
    if fused:
        expert_out, mixer_out = all_fused(
            mixer_in, mixer_gain, query_weight, key_weight, value_weight, input_gate, forget_gate,
            head_gain, mixer_out_weight, expert_in, expert_gain, group_router, expert_router,
            routes, gate_experts[0], up_experts[0], down_experts[0],
        )
        return (mixer_out, expert_out)
    normed_b = rms_rows(expert_in, expert_gain).astype(jnp.bfloat16)
    tokens = normed_b.shape[0]
    expert_total = expert_router.shape[1]
    members = expert_total // group_router.shape[1]
    capacity = 4 * tokens // expert_total
    share = capacity // lax.axis_size("tp")
    group_logits = jnp.dot(normed_b, group_router, preferred_element_type=jnp.float32)
    expert_logits = jnp.dot(normed_b, expert_router, preferred_element_type=jnp.float32)
    expert_ids = jnp.arange(expert_total, dtype=jnp.int32)
    group_ids = jnp.arange(group_router.shape[1], dtype=jnp.int32)
    named = [routes[:, k : k + 1] == expert_ids[None, :] for k in range(2)]
    chosen = [jnp.sum(jnp.where(m, expert_logits, 0.0), axis=1, keepdims=True) for m in named]
    combine = jnp.zeros((tokens, expert_total), jnp.float32)
    for k in range(2):
        in_group = routes[:, k : k + 1] // members == group_ids[None, :]
        group_pick = jnp.sum(jnp.where(in_group, group_logits, 0.0), axis=1, keepdims=True)
        weight = jax.nn.sigmoid(group_pick) * jax.nn.sigmoid(chosen[k] - chosen[1 - k])
        combine = combine + jnp.where(named[k], weight, 0.0)
    matches = named[0] | named[1]
    earlier = jnp.tril(jnp.ones((tokens, tokens), jnp.bfloat16), -1)
    rank = jnp.dot(
        earlier, matches.astype(jnp.bfloat16), preferred_element_type=jnp.float32
    ).astype(jnp.int32)
    rank = jnp.where(matches, rank, -1)
    slots = jnp.arange(capacity, dtype=jnp.int32)
    mix = jnp.where(
        rank[:, :, None] == slots[None, None, :], combine[:, :, None], 0.0
    ).reshape(tokens, expert_total * capacity)
    own_slots = lax.axis_index("tp") * share + jnp.arange(share, dtype=jnp.int32)
    select = (rank.T[:, None, :] == own_slots[None, :, None]).astype(jnp.bfloat16)
    own_share = (
        jnp.dot(
            select.reshape(expert_total * share, tokens),
            normed_b,
            preferred_element_type=jnp.float32,
        )
        .astype(jnp.bfloat16)
        .reshape(expert_total, share, normed_b.shape[1])
    )
    normed_a = rms_rows(mixer_in, mixer_gain).astype(jnp.bfloat16)
    prepared = mixer_prepare(
        normed_a, query_weight, key_weight, value_weight, input_gate, forget_gate
    )
    width_local = query_weight.shape[1]
    gain_local = lax.dynamic_slice_in_dim(
        head_gain, lax.axis_index("tp") * width_local, width_local
    ).reshape(input_gate.shape[0], -1)
    experts = (own_share, gate_experts[0], up_experts[0], down_experts[0], mix)
    partial = mixer_partial(prepared, gain_local, mixer_out_weight)
    mixer_out = lax.psum_scatter(partial, "tp", scatter_dimension=0, tiled=True)
    expert_out = experts_plain(*experts)
    return (mixer_out, expert_out)


def solution(mesh):
    in_specs = (
        P("ep", None),
        P(),
        P(None, "tp"),
        P(None, "tp"),
        P(None, "tp"),
        P("tp", "ep"),
        P("tp", "ep"),
        P(),
        P("tp", None),
        P("ep", None),
        P(),
        P(),
        P(),
        P("ep", None),
        P("ep", None, "tp"),
        P("ep", None, "tp"),
        P("ep", "tp", None),
    )
    out_specs = (P(("ep", "tp"), None), P("ep", "tp"))
    return jax.shard_map(shards, mesh=mesh, in_specs=in_specs, out_specs=out_specs, check_vma=False)
```

```python
import functools

import jax
import jax.numpy as jnp
from jax import lax
from jax.experimental import pallas as pl
from jax.experimental.pallas import tpu as pltpu
from jax.sharding import PartitionSpec as P

MESH = pl.DeviceIdType.MESH


epsilon = 1e-06
highest = lax.Precision.HIGHEST
floor_log = -1e30


def is_power(count):
    return count & (count - 1) == 0


def rms_rows(matrix, gain):
    widened = matrix.astype(jnp.float32)
    scaled = widened * lax.rsqrt(jnp.mean(widened * widened, axis=-1, keepdims=True) + epsilon)
    return scaled * gain


def merged(earlier_memory, earlier_peak, later_memory, later_peak, later_total):
    moved = later_total + earlier_peak
    peak = jnp.maximum(moved, later_peak)
    return jnp.exp(moved - peak) * earlier_memory + jnp.exp(later_peak - peak) * later_memory, peak


def three_parts(matrix):
    parts = []
    for _ in range(3):
        top_part = matrix.astype(jnp.bfloat16)
        parts.append(top_part)
        matrix = matrix - top_part.astype(jnp.float32)
    return parts


nn = (((1,), (0,)), ((), ()))
nt = (((1,), (1,)), ((), ()))
tn = (((0,), (0,)), ((), ()))


def product(left, right, numbers):
    return lax.dot_general(left, right, numbers, preferred_element_type=jnp.float32)


def normalize(source, gain_ref, target):
    block = 64

    def body(b, carry):
        place = pl.ds(pl.multiple_of(b * block, block), block)
        widened = source[place, :].astype(jnp.float32)
        mean = jnp.mean(widened * widened, axis=-1, keepdims=True)
        factor = lax.rsqrt(mean + epsilon)
        target[place, :] = (source[place, :].astype(jnp.float32) * factor * gain_ref[...]).astype(
            target.dtype
        )
        return carry

    lax.fori_loop(0, source.shape[0] // block, body, 0)


def whole_kernel(
    sizes, mixer_hbm, expert_hbm, query_hbm, key_hbm, value_hbm, project_hbm, gate_hbm, up_hbm, down_hbm,
    mixer_gain_ref, expert_gain_ref, head_gain_ref, in_ref, forget_ref,
    group_router_ref, expert_router_ref, routes_ref,
    out_ref, mixed_ref,
    mixer_in, expert_in, query_w, key_w, value_w, project_ref, gate_ref, up_ref, down_ref,
    normed_a, normed_b, rank, combine, near_rows, far_rows,
    query_ref, key_ref, value_ref, cum_ref, cum_col_ref, packed_ref, acc,
    rows, part, pin, csum, xin, fin, ret,
    peer, plane, mem, pre, pre_in, state, state_peak, state_parts, mpart, mpin, msum, mxin,
    own_sem, send_a, recv_a, send_x, recv_x, send_p, recv_p,
    send_q, recv_q, send_c, recv_c, send_r, recv_r,
    send_m, recv_m, send_k, recv_k, send_h, recv_h, send_y, recv_y,
):
    n, share, cap, width, quarter, heads, size = sizes
    near = n // 2
    planes = n // 2
    me, tp = lax.axis_index("ep"), lax.axis_index("tp")
    core, column = lax.rem(tp, 2), lax.div(tp, 2)
    pair = tp + 1 - 2 * core
    cross = lax.rem(tp + 2, 4)
    pair_cross = lax.rem(pair + 2, 4)
    side, level = lax.rem(me, 2), lax.div(me, 2)
    mate = me + 1 - 2 * side
    tokens = expert_in.shape[0]
    length = mixer_in.shape[0]
    chunk = length // 4
    scale = size ** (-0.5)

    def other(i):
        total, bit = 0, 1
        while bit < n:
            total = total + bit * lax.rem(lax.div(me, bit) + lax.div(i, bit), 2)
            bit *= 2
        return total

    high = lax.rem(lax.div(me, near), 2)
    inner = lax.rem(high + lax.div(lax.rem(me, near), near // 2), 2)

    def far_turn(k):
        half = near // 2
        return near + half * lax.rem(lax.rem(k, 2) + 1 - inner, 2) + lax.div(k, 2)

    order = [(False, 0), (False, 1), (True, 0), (True, 1)]
    order += [(False, k) for k in range(2, near - 1)] + [(True, k) for k in range(2, near)]
    order += [(False, near - 1)] * (near > 2)

    def turn(t):
        total = 0
        for place, (far, k) in enumerate(order):
            total = total + jnp.where(t == place, far_turn(k) if far else k, 0)
        return total

    def is_far(t):
        total = t < 0
        for place, (far, k) in enumerate(order):
            total = total | (t == place) if far else total
        return total

    def remote(src, dst, send, recv, to):
        return pltpu.make_async_remote_copy(
            src_ref=src, dst_ref=dst, send_sem=send, recv_sem=recv, device_id=to, device_id_type=MESH
        )

    barrier = pltpu.get_barrier_semaphore()
    for i in range(1, n):
        pl.semaphore_signal(
            barrier, inc=1, device_id=(lax.rem(me + i, n), tp), device_id_type=MESH
        )
    pl.semaphore_signal(barrier, inc=1, device_id=(me, pair), device_id_type=MESH)
    pl.semaphore_signal(barrier, inc=1, device_id=(me, cross), device_id_type=MESH)

    loads = [
        pltpu.make_async_copy(src, dst, own_sem.at[k])
        for k, (src, dst) in enumerate(
            [
                (expert_hbm, expert_in), (gate_hbm, gate_ref), (up_hbm, up_ref),
                (down_hbm, down_ref), (mixer_hbm, mixer_in), (key_hbm, key_w),
                (value_hbm, value_w), (query_hbm, query_w), (project_hbm, project_ref),
            ]
        )
    ]
    for load in loads:
        load.start()

    def scatter_near(i, place):
        slot = jnp.maximum(i - 1, 0)
        return remote(
            near_rows.at[slot], rows.at[place, core], send_a.at[i], recv_a.at[i], (other(i), tp)
        )

    def scatter_far(i, place):
        slot = jnp.maximum(i - near, 0)
        mine = pl.ds(pl.multiple_of(column * share, share), share)
        return remote(
            far_rows.at[slot], rows.at[place, core, mine], send_a.at[i], recv_a.at[i], (other(i), tp)
        )

    def across(s, which):
        mine = pl.ds(pl.multiple_of(which * share, share), share)
        return remote(
            rows.at[s, core, mine], rows.at[s, core, mine], send_x.at[s], recv_x.at[s], (me, cross)
        )

    def beside(s, which):
        return remote(
            rows.at[s, which], rows.at[s, which], send_p.at[s], recv_p.at[s], (me, pair)
        )

    def halves(s, k, who):
        return remote(part.at[s, who], pin.at[s, k], send_q.at[s, k], recv_q.at[s, k], (me, pair))

    def summed(s):
        return remote(csum.at[s], xin.at[s], send_c.at[s], recv_c.at[s], (me, cross))

    def back(i):
        to = other(i)
        return remote(fin.at[to], ret.at[me], send_r.at[i], recv_r.at[i], (to, tp))

    def to_mate():
        return remote(
            packed_ref.at[1 - side], peer.at[1 - side], send_k.at[0], recv_k.at[0], (mate, tp)
        )

    def from_mate():
        return remote(packed_ref.at[side], peer.at[side], send_k.at[0], recv_k.at[0], (mate, tp))

    def rest_to_mate():
        return remote(packed_ref.at[0], peer.at[0], send_k.at[2], recv_k.at[2], (mate, tp))

    def to_level(d):
        return remote(
            plane, mem.at[level], send_m.at[d], recv_m.at[d], (lax.rem(me + 2 * d, n), tp)
        )

    def from_level(d):
        return remote(
            plane, mem.at[level - d], send_m.at[d], recv_m.at[d], (lax.rem(me + 2 * d, n), tp)
        )

    def prefix_mate():
        return remote(pre, pre_in, send_k.at[1], recv_k.at[1], (mate, tp))

    def mixed_half(k, who):
        return remote(mpart.at[who], mpin.at[k], send_h.at[k], recv_h.at[k], (me, pair))

    def mixed_sum(q):
        return remote(msum.at[q], mxin.at[q], send_y.at[q], recv_y.at[q], (me, cross))

    body, top_row, sum_row = slice(0, size), slice(size, size + 1), slice(size + 1, size + 2)

    def picks(e, first, count):
        slots = lax.broadcasted_iota(jnp.int32, (count, tokens), 0) + first
        return rank[pl.ds(e, 1), :] == slots.astype(jnp.float32)

    def gathered(parts):
        select = jnp.concatenate([jnp.where(p, 1.0, 0.0).astype(jnp.bfloat16) for p in parts], axis=0)
        return product(select, normed_b[...], nn).astype(jnp.bfloat16)

    def prepare_rank():
        experts = lax.broadcasted_iota(jnp.int32, (n, tokens), 0)
        matches = (routes_ref[0:1, :] == experts) | (routes_ref[1:2, :] == experts)
        earlier = lax.broadcasted_iota(jnp.int32, (tokens, tokens), 0)
        earlier = earlier < lax.broadcasted_iota(jnp.int32, (tokens, tokens), 1)
        count = product(
            jnp.where(matches, 1.0, 0.0).astype(jnp.bfloat16),
            jnp.where(earlier, 1.0, 0.0).astype(jnp.bfloat16),
            nn,
        )
        rank[...] = jnp.where(matches, count, -1.0)

    def prepare_combine():
        experts = lax.broadcasted_iota(jnp.int32, (n, tokens), 0)
        groups = group_router_ref.shape[0]
        expert_logits = product(expert_router_ref[...], normed_b[...], nt)
        group_logits = product(group_router_ref[...], normed_b[...], nt)
        group_full = jnp.zeros((n, tokens), jnp.float32)
        for g in range(groups):
            inside = (experts >= g * (n // groups)) & (experts < (g + 1) * (n // groups))
            group_full = group_full + jnp.where(inside, group_logits[g : g + 1, :], 0.0)
        named = [routes_ref[k : k + 1, :] == experts for k in range(2)]
        chosen = [jnp.sum(jnp.where(m, expert_logits, 0.0), axis=0, keepdims=True) for m in named]
        total = jnp.zeros((n, tokens), jnp.float32)
        for k in range(2):
            group_pick = jnp.sum(jnp.where(named[k], group_full, 0.0), axis=0, keepdims=True)
            weight = jax.nn.sigmoid(group_pick) * jax.nn.sigmoid(chosen[k] - chosen[1 - k])
            total = total + jnp.where(named[k], weight, 0.0)
        combine[...] = total

    def prepare_near():
        step_rows = 2 * share
        moved = gathered([picks(other(i), core * step_rows, step_rows) for i in range(1, near)])
        for i in range(1, near):
            near_rows[i - 1] = moved[(i - 1) * step_rows : i * step_rows]

    def prepare_far():
        first = core * (2 * share) + column * share
        moved = gathered([picks(other(i), first, share) for i in range(near, n)])
        for i in range(near, n):
            far_rows[i - near] = moved[(i - near) * share : (i - near + 1) * share]

    def prepare_own():
        rows[me] = gathered([picks(me, 0, cap)]).reshape(2, 2 * share, width)

    def ffn(s):
        x = rows[s].reshape(cap, width)
        gate_act = jnp.dot(x, gate_ref[...], preferred_element_type=jnp.float32)
        up_act = jnp.dot(x, up_ref[...], preferred_element_type=jnp.float32)
        hidden = (gate_act * jax.nn.sigmoid(gate_act) * up_act).astype(jnp.bfloat16)
        for q in range(4):
            part[s, q] = jnp.dot(
                hidden,
                down_ref[:, q * quarter : (q + 1) * quarter],
                preferred_element_type=jnp.float32,
            ).astype(jnp.bfloat16)

    def prepare_gates():
        log_forget = jnp.minimum(forget_ref[...], 0.0) - jnp.log1p(jnp.exp(-jnp.abs(forget_ref[...])))
        pieces = jnp.concatenate(
            [p.astype(jnp.float32) for p in three_parts(log_forget)]
            + [jnp.zeros((16 - 3 * heads, length), jnp.float32)],
            axis=0,
        ).astype(jnp.bfloat16)
        first = lax.broadcasted_iota(jnp.int32, (length, length), 0)
        upto = first <= lax.broadcasted_iota(jnp.int32, (length, length), 1)
        sums = product(pieces, jnp.where(upto, 1.0, 0.0).astype(jnp.bfloat16), nn)
        cum_ref[...] = sums[2 * heads : 3 * heads] + sums[heads : 2 * heads] + sums[0:heads]
        back_to = first >= lax.broadcasted_iota(jnp.int32, (length, length), 1)
        sums = product(jnp.where(back_to, 1.0, 0.0).astype(jnp.bfloat16), pieces, nt)
        cum_col_ref[...] = (
            sums[:, 2 * heads : 3 * heads] + sums[:, heads : 2 * heads] + sums[:, 0:heads]
        )

    def prepare_memory():
        key_ref[...] = jnp.dot(
            normed_a[...], key_w[...], preferred_element_type=jnp.float32
        ).astype(jnp.bfloat16)
        value_ref[...] = jnp.dot(
            normed_a[...], value_w[...], preferred_element_type=jnp.float32
        ).astype(jnp.bfloat16)
        for h in range(heads):
            cols = slice(h * size, (h + 1) * size)
            cum = cum_ref[h : h + 1, :]
            total = cum_ref[h : h + 1, length - 1 : length]
            log_weight = total - cum + in_ref[h : h + 1, :]
            peak = jnp.max(log_weight, axis=1, keepdims=True)
            weighted = value_ref[:, cols].astype(jnp.float32).T * jnp.exp(log_weight - peak)
            memory = jnp.zeros((size, size), jnp.float32)
            for piece in three_parts(weighted)[::-1]:
                memory = memory + product(piece, key_ref[:, cols], nn)
            packed_ref[h, body] = memory * scale
            packed_ref[h, size : size + 8] = jnp.zeros((8, size), jnp.float32)
            packed_ref[h, top_row] = jnp.broadcast_to(peak, (1, size))
            packed_ref[h, sum_row] = jnp.broadcast_to(total, (1, size))

    def prepare_query():
        query_ref[...] = jnp.dot(
            normed_a[...], query_w[...], preferred_element_type=jnp.float32
        ).astype(jnp.bfloat16)

    def combine_plane():
        from_mate().wait_recv()

        def joined(first, second):
            memory, peak = merged(
                first[side, body], first[side, top_row],
                second[side, body], second[side, top_row], second[side, sum_row],
            )
            plane[size : size + 8] = jnp.zeros((8, size), jnp.float32)
            plane[body] = memory
            plane[top_row] = peak
            plane[sum_row] = first[side, sum_row] + second[side, sum_row]

        @pl.when(side == 0)
        def _():
            joined(packed_ref, peer)

        @pl.when(side == 1)
        def _():
            joined(peer, packed_ref)

        for d in range(1, planes):
            @pl.when(level + d < planes)
            def _():
                to_level(d).start()

    def combine_levels():
        pre[...] = jnp.zeros_like(pre)
        pre[top_row] = jnp.full((1, size), floor_log, jnp.float32)
        for k in range(planes - 1):
            d = planes - 1 - k

            @pl.when(d <= level)
            def _():
                from_level(d).wait_recv()
                z = level - d
                memory, peak = merged(
                    pre[body], pre[top_row], mem[z, body], mem[z, top_row], mem[z, sum_row]
                )
                pre[body] = memory
                pre[top_row] = peak

        prefix_mate().start()

    def combine_last():
        prefix_mate().wait_recv()
        state[side] = pre[body]
        state_peak[side, 0:1, :] = pre[top_row]
        state[1 - side] = pre_in[body]
        state_peak[1 - side, 0:1, :] = pre_in[top_row]

        @pl.when(side == 1)
        def _():
            rest_to_mate().wait_recv()
            for h in range(heads):
                memory, peak = merged(
                    state[h], state_peak[h, 0:1, :],
                    peer[h, body], peer[h, top_row], peer[h, sum_row],
                )
                state[h] = memory
                state_peak[h, 0:1, :] = peak

        for h in range(heads):
            for piece, value in enumerate(three_parts(state[h])):
                state_parts[h, piece] = value

    def attend(j):
        start = pl.multiple_of(j * chunk, chunk)
        row = start + lax.broadcasted_iota(jnp.int32, (chunk, length), 0)
        causal = row >= lax.broadcasted_iota(jnp.int32, (chunk, length), 1)
        cell_list = []
        for h in range(heads):
            cols = slice(h * size, (h + 1) * size)
            q = query_ref[pl.ds(start, chunk), cols]
            c = cum_col_ref[pl.ds(start, chunk), h : h + 1]
            within = jnp.where(causal, c - cum_ref[h : h + 1, :] + in_ref[h : h + 1, :], -jnp.inf)
            carried = c + state_peak[h, 0:1, 0:1]
            top = jnp.maximum(jnp.max(within, axis=1, keepdims=True), carried)
            raw = product(q, key_ref[:, cols], nt)
            scores = (raw * scale * jnp.exp(within - top)).astype(jnp.bfloat16)
            cells = jnp.dot(scores, value_ref[:, cols], preferred_element_type=jnp.float32)
            held = jnp.zeros((chunk, size), jnp.float32)
            for piece in (2, 1, 0):
                held = held + product(q, state_parts[h, piece], nt)
            cells = cells + jnp.exp(carried - top) * held
            mean = jnp.mean(cells * cells, axis=1, keepdims=True)
            gain = head_gain_ref[pl.ds(tp * heads + h, 1), :]
            cell_list.append((cells * lax.rsqrt(mean + epsilon) * gain).astype(jnp.bfloat16))
        cell_rows = jnp.concatenate(cell_list, axis=1)
        for q in range(4):
            cols = slice(q * quarter, (q + 1) * quarter)
            mpart[j, q] = jnp.dot(
                cell_rows, project_ref[:, cols], preferred_element_type=jnp.float32
            ).astype(jnp.bfloat16)

    begin = n - 1

    def send_far(first):
        for k in range(first, first + 2):
            scatter_far(far_turn(k), me).start()

    def mixer_step(t):
        @pl.when(t == begin - 1)
        def _():
            combine_levels()

        @pl.when(t == begin)
        def _():
            combine_last()

            def one(k, carry):
                later = jnp.where(k == 2, cross, tp)
                attend(jnp.where(k == 0, pair_cross, jnp.where(k == 1, pair, later)))

                @pl.when(k == 1)
                def _():
                    mixed_half(1, pair_cross).start()
                    mixed_half(0, pair).start()

                return carry

            lax.fori_loop(0, 4, one, 0)

    def mixer_send(t):
        @pl.when(t == begin)
        def _():
            mixed_half(1, pair_cross).wait_recv()
            msum[...] = (
                mpart[cross].astype(jnp.float32) + mpin[1].astype(jnp.float32)
            ).astype(jnp.bfloat16)
            mixed_sum(0).start()

        @pl.when(t == begin + 1)
        def _():
            mixed_sum(1).start()

        @pl.when(t == begin + 2)
        def _():
            mixed_sum(2).start()
            mixed_sum(3).start()

    def collect(s):
        halves(s, 1, pair_cross).wait_recv()
        csum[s] = (
            part[s, cross].astype(jnp.float32) + pin[s, 1].astype(jnp.float32)
        ).astype(jnp.bfloat16)
        summed(s).start()

    def send_halves(s):
        halves(s, 1, pair_cross).start()
        halves(s, 0, pair).start()

    prepare_rank()
    loads[0].wait()
    normalize(expert_in, expert_gain_ref, normed_b)
    prepare_near()
    prepare_far()
    pl.semaphore_wait(barrier, n + 1)
    scatter_near(1, me).start()

    @pl.when(inner == 0)
    def _():
        send_far(0)

    @pl.when(inner == 1)
    def _():
        for i in range(2, near - 1):
            scatter_near(i, me).start()

    prepare_own()
    for k in (1, 2, 3):
        loads[k].wait()
    ffn(me)
    send_halves(me)
    loads[4].wait()
    normalize(mixer_in, mixer_gain_ref, normed_a)
    collect(me)
    prepare_gates()
    loads[5].wait()
    loads[6].wait()
    prepare_memory()
    to_mate().start()

    @pl.when(inner == 0)
    def _():
        for i in range(2, near - 1):
            scatter_near(i, me).start()

    @pl.when(inner == 1)
    def _():
        send_far(0)
        if near > 2:
            scatter_near(near - 1, me).start()

    loads[7].wait()
    prepare_query()
    prepare_combine()
    loads[8].wait()

    def step(t, carry):
        @pl.when((t >= 3) & (t < n + 2))
        def _():
            @pl.when(is_far(t - 2))
            def _():
                s = other(turn(t - 2))
                across(s, 1 - column).wait_recv()
                beside(s, core).start()

        mixer_step(t)

        @pl.when((t >= 3) & (t < n + 2))
        def _():
            s = other(turn(t - 2))
            beside(s, 1 - core).wait_recv()
            ffn(s)
            send_halves(s)

        @pl.when((t >= 3) & (t < n + 2))
        def _():
            collect(other(turn(t - 2)))

        mixer_send(t)

        @pl.when(t < n)
        def _():
            i = turn(t)
            s = other(i)

            @pl.when(is_far(t))
            def _():
                scatter_far(i, s).wait_recv()
                across(s, column).start()

            @pl.when(jnp.logical_not(is_far(t)))
            def _():
                scatter_near(i, s).wait_recv()
                beside(s, core).start()

        @pl.when(t == 1)
        def _():
            combine_plane()
            for first in range(2, near, 2):
                send_far(first)

            @pl.when(inner == 0)
            def _():
                if near > 2:
                    scatter_near(near - 1, me).start()

            @pl.when(side == 0)
            def _():
                rest_to_mate().start()

        @pl.when(t >= 3)
        def _():
            i = turn(t - 3)
            s = other(i)
            halves(s, 0, pair).wait_recv()
            summed(s).wait_recv()
            total = (
                part[s, tp].astype(jnp.float32)
                + pin[s, 0].astype(jnp.float32)
                + xin[s].astype(jnp.float32)
            ).astype(jnp.bfloat16)

            @pl.when(i > 0)
            def _():
                fin[s] = total
                back(i).start()

            @pl.when(i == 0)
            def _():
                ret[s] = total

        return carry

    lax.fori_loop(1, n + 3, step, 0)

    mixed_half(0, pair).wait_recv()
    for q in range(4):
        mixed_sum(q).wait_recv()
        cols = slice(q * quarter, (q + 1) * quarter)
        mixed_ref[:, cols] = (
            mpart[tp, q].astype(jnp.float32)
            + mpin[0, q].astype(jnp.float32)
            + mxin[q].astype(jnp.float32)
        ).astype(mixed_ref.dtype)

    acc[...] = jnp.zeros_like(acc)

    def finish(t, carry):
        i = turn(t)
        s = other(i)

        @pl.when(t > 0)
        def _():
            back(i).wait_recv()

        chosen = picks(s, 0, cap)
        weight = combine[pl.ds(s, 1), :]
        high_weight = weight.astype(jnp.bfloat16).astype(jnp.float32)
        table = ret[s]
        acc[...] += product(
            jnp.where(chosen, high_weight, 0.0).astype(jnp.bfloat16), table, tn
        ) + product(jnp.where(chosen, weight - high_weight, 0.0).astype(jnp.bfloat16), table, tn)
        return carry

    lax.fori_loop(0, n, finish, 0)
    out_ref[...] = acc[...].astype(out_ref.dtype)

    def drain(i, carry):
        s = other(i)
        halves(s, 0, pair).wait_send()
        halves(s, 1, pair_cross).wait_send()
        summed(s).wait_send()

        @pl.when(i > 0)
        def _():
            beside(s, core).wait_send()
            back(i).wait_send()

        @pl.when((i > 0) & (i < near))
        def _():
            scatter_near(i, me).wait_send()

        @pl.when(i >= near)
        def _():
            scatter_far(i, me).wait_send()
            across(s, column).wait_send()

        return carry

    lax.fori_loop(0, n, drain, 0)
    to_mate().wait_send()

    @pl.when(side == 0)
    def _():
        rest_to_mate().wait_send()

    prefix_mate().wait_send()
    for d in range(1, planes):
        @pl.when(level + d < planes)
        def _():
            to_level(d).wait_send()
    mixed_half(0, pair).wait_send()
    mixed_half(1, pair_cross).wait_send()
    for q in range(4):
        mixed_sum(q).wait_send()


def all_fused(
    mixer_in, mixer_gain, query_weight, key_weight, value_weight, input_gate, forget_gate,
    head_gain, mixer_out_weight, expert_in, expert_gain, group_router, expert_router, routes,
    gate_weight, up_weight, down_weight,
):
    n = expert_router.shape[1]
    tokens, width = expert_in.shape
    cap = 4 * tokens // n
    share = cap // 4
    quarter = width // 4
    length = mixer_in.shape[0]
    heads = input_gate.shape[0]
    inner_width = query_weight.shape[1]
    size = inner_width // heads
    hidden = gate_weight.shape[1]
    chunk = length // 4
    vmem = pl.BlockSpec(memory_space=pltpu.VMEM)
    whole = pl.BlockSpec(memory_space=pl.ANY)
    dma = pltpu.SemaphoreType.DMA
    bf = jnp.bfloat16
    f32 = jnp.float32
    return pl.pallas_call(
        functools.partial(whole_kernel, (n, share, cap, width, quarter, heads, size)),
        out_shape=(
            jax.ShapeDtypeStruct((tokens, quarter), bf),
            jax.ShapeDtypeStruct((chunk, width), bf),
        ),
        in_specs=[whole] * 9 + [vmem] * 8,
        out_specs=(vmem, vmem),
        scratch_shapes=[
            pltpu.VMEM((length, width), bf),
            pltpu.VMEM((tokens, width), bf),
            pltpu.VMEM((width, inner_width), bf),
            pltpu.VMEM((width, inner_width), bf),
            pltpu.VMEM((width, inner_width), bf),
            pltpu.VMEM((inner_width, width), bf),
            pltpu.VMEM((width, hidden), bf),
            pltpu.VMEM((width, hidden), bf),
            pltpu.VMEM((hidden, width), bf),
            pltpu.VMEM((length, width), bf),
            pltpu.VMEM((tokens, width), bf),
            pltpu.VMEM((n, tokens), f32),
            pltpu.VMEM((n, tokens), f32),
            pltpu.VMEM((n // 2 - 1, 2 * share, width), bf),
            pltpu.VMEM((n // 2, share, width), bf),
            pltpu.VMEM((length, inner_width), bf),
            pltpu.VMEM((length, inner_width), bf),
            pltpu.VMEM((length, inner_width), bf),
            pltpu.VMEM((heads, length), f32),
            pltpu.VMEM((length, heads), f32),
            pltpu.VMEM((heads, size + 8, size), f32),
            pltpu.VMEM((tokens, quarter), f32),
            pltpu.VMEM((n, 2, 2 * share, width), bf),
            pltpu.VMEM((n, 4, cap, quarter), bf),
            pltpu.VMEM((n, 2, cap, quarter), bf),
            pltpu.VMEM((n, cap, quarter), bf),
            pltpu.VMEM((n, cap, quarter), bf),
            pltpu.VMEM((n, cap, quarter), bf),
            pltpu.VMEM((n, cap, quarter), bf),
            pltpu.VMEM((heads, size + 8, size), f32),
            pltpu.VMEM((size + 8, size), f32),
            pltpu.VMEM((n // 2, size + 8, size), f32),
            pltpu.VMEM((size + 8, size), f32),
            pltpu.VMEM((size + 8, size), f32),
            pltpu.VMEM((heads, size, size), f32),
            pltpu.VMEM((heads, 8, size), f32),
            pltpu.VMEM((heads, 3, size, size), bf),
            pltpu.VMEM((4, 4, chunk, quarter), bf),
            pltpu.VMEM((2, 4, chunk, quarter), bf),
            pltpu.VMEM((4, chunk, quarter), bf),
            pltpu.VMEM((4, chunk, quarter), bf),
            dma((9,)),
            dma((n,)), dma((n,)), dma((n,)), dma((n,)), dma((n,)), dma((n,)),
            dma((n, 2)), dma((n, 2)), dma((n,)), dma((n,)), dma((n,)), dma((n,)),
            dma((n // 2,)), dma((n // 2,)), dma((3,)), dma((3,)), dma((2,)), dma((2,)),
            dma((4,)), dma((4,)),
        ],
        compiler_params=pltpu.CompilerParams(
            collective_id=0, has_side_effects=True, vmem_limit_bytes=60 * 1024 * 1024
        ),
        cost_estimate=pl.CostEstimate(
            flops=60_000_000_000, bytes_accessed=8_000_000, transcendentals=0
        ),
    )(
        mixer_in, expert_in, query_weight, key_weight, value_weight, mixer_out_weight,
        gate_weight, up_weight, down_weight,
        mixer_gain.reshape(1, width), expert_gain.reshape(1, width),
        head_gain.reshape(-1, size), input_gate, forget_gate,
        group_router.T, expert_router.T, routes.T,
    )


def experts_plain(own_share, gate_weight, up_weight, down_weight, mix):
    arrived = lax.all_to_all(own_share, "ep", split_axis=0, concat_axis=0, tiled=True)
    piece_rows = lax.all_gather(arrived, "tp", axis=1, tiled=True)
    gate_act = jnp.einsum(
        "scd,df->scf", piece_rows, gate_weight, preferred_element_type=jnp.float32
    )
    up_act = jnp.einsum("scd,df->scf", piece_rows, up_weight, preferred_element_type=jnp.float32)
    hidden = (jax.nn.silu(gate_act) * up_act).astype(jnp.bfloat16)
    partial_rows = jnp.einsum(
        "scf,fo->sco", hidden, down_weight, preferred_element_type=jnp.float32
    )
    summed = lax.psum_scatter(
        partial_rows.astype(jnp.bfloat16), "tp", scatter_dimension=2, tiled=True
    )
    returned = lax.all_to_all(summed, "ep", split_axis=0, concat_axis=0, tiled=True)
    return jnp.dot(
        mix, returned.reshape(-1, returned.shape[2]).astype(jnp.float32), precision=highest
    ).astype(jnp.bfloat16)


def mixer_prepare(normed_a, query_weight, key_weight, value_weight, input_gate, forget_gate):
    def project(weight):
        return jnp.dot(normed_a, weight, preferred_element_type=jnp.float32).astype(jnp.bfloat16)

    rows = normed_a.shape[0]
    heads = input_gate.shape[0]
    width_local = query_weight.shape[1]
    head_size = width_local // heads
    scale = head_size ** (-0.5)
    causal = jnp.tril(jnp.ones((rows, rows), dtype=bool))
    log_forget = jax.nn.log_sigmoid(forget_gate)
    cumulative = jnp.einsum(
        "hs,ts->ht", log_forget, causal.astype(jnp.float32), precision=highest
    )
    total = cumulative[:, -1]
    log_weight = total[:, None] - cumulative + input_gate
    peak = jnp.max(log_weight, axis=-1)
    weights = jnp.exp(log_weight - peak[:, None])
    keys = project(key_weight)
    values = project(value_weight)

    def by_head(matrix):
        return [matrix[:, h * head_size : (h + 1) * head_size] for h in range(heads)]

    key_heads, value_heads = by_head(keys), by_head(values)
    memory = jnp.stack(
        [
            lax.dot_general(
                value_heads[h].astype(jnp.float32) * weights[h][:, None],
                key_heads[h].astype(jnp.float32) * scale,
                (((0,), (0,)), ((), ())),
                precision=highest,
            )
            for h in range(heads)
        ]
    )
    stats = jnp.stack([peak, total], axis=1)
    stats = jnp.concatenate([stats, jnp.zeros((heads, 6), jnp.float32)], axis=1)
    packed = jnp.concatenate(
        [memory, jnp.broadcast_to(stats[:, :, None], (heads, 8, head_size))], axis=1
    )
    return (packed, project(query_weight), keys, values, cumulative, input_gate)


def mixer_partial(prepared, gain_local, mixer_out_weight):
    packed, queries, keys, values, cumulative, input_gate = prepared
    rows = queries.shape[0]
    heads, head_size = gain_local.shape
    scale = head_size ** (-0.5)
    causal = jnp.tril(jnp.ones((rows, rows), dtype=bool))

    def by_head(matrix):
        return [matrix[:, h * head_size : (h + 1) * head_size] for h in range(heads)]

    query_heads, key_heads, value_heads = by_head(queries), by_head(keys), by_head(values)
    everything = lax.all_gather(packed, "ep")
    n, place = lax.axis_size("ep"), lax.axis_index("ep")
    peaks = everything[:, :, head_size, 0]
    totals = everything[:, :, head_size + 1, 0]
    order = jnp.arange(n)
    later = (order[None, :] > order[:, None]) & (order[None, :] < place)
    suffix = jnp.sum(jnp.where(later[:, :, None], totals[None], 0.0), axis=1)
    before = (order < place)[:, None]
    candidate = jnp.where(before, peaks + suffix, floor_log)
    state_peak = jnp.max(candidate, axis=0)
    fade = jnp.where(before, jnp.exp(candidate - state_peak[None]), 0.0)
    state = jnp.sum(everything[:, :, :head_size] * fade[:, :, None, None], axis=0)
    cell_list = []
    for h in range(heads):
        c, gate = cumulative[h], input_gate[h]
        within = jnp.where(causal, c[:, None] - c[None, :] + gate[None, :], -jnp.inf)
        carried = c + state_peak[h]
        top = jnp.maximum(jnp.max(within, axis=-1), carried)
        raw = lax.dot_general(
            query_heads[h], key_heads[h], (((1,), (1,)), ((), ())), preferred_element_type=jnp.float32
        )
        scores = raw * scale * jnp.exp(within - top[:, None])
        cells = jnp.dot(
            scores.astype(jnp.bfloat16), value_heads[h], preferred_element_type=jnp.float32
        )
        carried_cells = lax.dot_general(
            query_heads[h].astype(jnp.float32),
            state[h],
            (((1,), (1,)), ((), ())),
            precision=highest,
        )
        cells = cells + jnp.exp(carried - top)[:, None] * carried_cells
        cell_list.append(rms_rows(cells, gain_local[h]).astype(jnp.bfloat16))
    cell_rows = jnp.concatenate(cell_list, axis=1)
    return jnp.dot(cell_rows, mixer_out_weight, preferred_element_type=jnp.float32).astype(
        jnp.bfloat16
    )


def shards(
    mixer_in,
    mixer_gain,
    query_weight,
    key_weight,
    value_weight,
    input_gate,
    forget_gate,
    head_gain,
    mixer_out_weight,
    expert_in,
    expert_gain,
    group_router,
    expert_router,
    routes,
    gate_experts,
    up_experts,
    down_experts,
):
    ranks = lax.axis_size("ep")
    share = expert_in.shape[0] // expert_router.shape[1]
    fused = lax.axis_size("tp") == 4 and ranks >= 4 and is_power(ranks) and share % 16 == 0
    fused = fused and mixer_in.shape[0] % 512 == 0 and input_gate.shape[0] == 2
    fused = fused and gate_experts.shape[0] == 1
    if fused:
        expert_out, mixer_out = all_fused(
            mixer_in, mixer_gain, query_weight, key_weight, value_weight, input_gate, forget_gate,
            head_gain, mixer_out_weight, expert_in, expert_gain, group_router, expert_router,
            routes, gate_experts[0], up_experts[0], down_experts[0],
        )
        return (mixer_out, expert_out)
    normed_b = rms_rows(expert_in, expert_gain).astype(jnp.bfloat16)
    tokens = normed_b.shape[0]
    expert_total = expert_router.shape[1]
    members = expert_total // group_router.shape[1]
    capacity = 4 * tokens // expert_total
    share = capacity // lax.axis_size("tp")
    group_logits = jnp.dot(normed_b, group_router, preferred_element_type=jnp.float32)
    expert_logits = jnp.dot(normed_b, expert_router, preferred_element_type=jnp.float32)
    expert_ids = jnp.arange(expert_total, dtype=jnp.int32)
    group_ids = jnp.arange(group_router.shape[1], dtype=jnp.int32)
    named = [routes[:, k : k + 1] == expert_ids[None, :] for k in range(2)]
    chosen = [jnp.sum(jnp.where(m, expert_logits, 0.0), axis=1, keepdims=True) for m in named]
    combine = jnp.zeros((tokens, expert_total), jnp.float32)
    for k in range(2):
        in_group = routes[:, k : k + 1] // members == group_ids[None, :]
        group_pick = jnp.sum(jnp.where(in_group, group_logits, 0.0), axis=1, keepdims=True)
        weight = jax.nn.sigmoid(group_pick) * jax.nn.sigmoid(chosen[k] - chosen[1 - k])
        combine = combine + jnp.where(named[k], weight, 0.0)
    matches = named[0] | named[1]
    earlier = jnp.tril(jnp.ones((tokens, tokens), jnp.bfloat16), -1)
    rank = jnp.dot(
        earlier, matches.astype(jnp.bfloat16), preferred_element_type=jnp.float32
    ).astype(jnp.int32)
    rank = jnp.where(matches, rank, -1)
    slots = jnp.arange(capacity, dtype=jnp.int32)
    mix = jnp.where(
        rank[:, :, None] == slots[None, None, :], combine[:, :, None], 0.0
    ).reshape(tokens, expert_total * capacity)
    own_slots = lax.axis_index("tp") * share + jnp.arange(share, dtype=jnp.int32)
    select = (rank.T[:, None, :] == own_slots[None, :, None]).astype(jnp.bfloat16)
    own_share = (
        jnp.dot(
            select.reshape(expert_total * share, tokens),
            normed_b,
            preferred_element_type=jnp.float32,
        )
        .astype(jnp.bfloat16)
        .reshape(expert_total, share, normed_b.shape[1])
    )
    normed_a = rms_rows(mixer_in, mixer_gain).astype(jnp.bfloat16)
    prepared = mixer_prepare(
        normed_a, query_weight, key_weight, value_weight, input_gate, forget_gate
    )
    width_local = query_weight.shape[1]
    gain_local = lax.dynamic_slice_in_dim(
        head_gain, lax.axis_index("tp") * width_local, width_local
    ).reshape(input_gate.shape[0], -1)
    experts = (own_share, gate_experts[0], up_experts[0], down_experts[0], mix)
    partial = mixer_partial(prepared, gain_local, mixer_out_weight)
    mixer_out = lax.psum_scatter(partial, "tp", scatter_dimension=0, tiled=True)
    expert_out = experts_plain(*experts)
    return (mixer_out, expert_out)


def solution(mesh):
    in_specs = (
        P("ep", None),
        P(),
        P(None, "tp"),
        P(None, "tp"),
        P(None, "tp"),
        P("tp", "ep"),
        P("tp", "ep"),
        P(),
        P("tp", None),
        P("ep", None),
        P(),
        P(),
        P(),
        P("ep", None),
        P("ep", None, "tp"),
        P("ep", None, "tp"),
        P("ep", "tp", None),
    )
    out_specs = (P(("ep", "tp"), None), P("ep", "tp"))
    return jax.shard_map(shards, mesh=mesh, in_specs=in_specs, out_specs=out_specs, check_vma=False)
```

```python
import functools

import jax
import jax.numpy as jnp
from jax import lax
from jax.experimental import pallas as pl
from jax.experimental.pallas import tpu as pltpu
from jax.sharding import PartitionSpec as P

MESH = pl.DeviceIdType.MESH


epsilon = 1e-06
highest = lax.Precision.HIGHEST
floor_log = -1e30


def is_power(count):
    return count & (count - 1) == 0


def rms_rows(matrix, gain):
    widened = matrix.astype(jnp.float32)
    scaled = widened * lax.rsqrt(jnp.mean(widened * widened, axis=-1, keepdims=True) + epsilon)
    return scaled * gain


def merged(earlier_memory, earlier_peak, later_memory, later_peak, later_total):
    moved = later_total + earlier_peak
    peak = jnp.maximum(moved, later_peak)
    return jnp.exp(moved - peak) * earlier_memory + jnp.exp(later_peak - peak) * later_memory, peak


def three_parts(matrix):
    parts = []
    for _ in range(3):
        top_part = matrix.astype(jnp.bfloat16)
        parts.append(top_part)
        matrix = matrix - top_part.astype(jnp.float32)
    return parts


nn = (((1,), (0,)), ((), ()))
nt = (((1,), (1,)), ((), ()))
tn = (((0,), (0,)), ((), ()))


def product(left, right, numbers):
    return lax.dot_general(left, right, numbers, preferred_element_type=jnp.float32)


def normalize(source, gain_ref, target):
    block = 64

    def body(b, carry):
        place = pl.ds(pl.multiple_of(b * block, block), block)
        widened = source[place, :].astype(jnp.float32)
        mean = jnp.mean(widened * widened, axis=-1, keepdims=True)
        factor = lax.rsqrt(mean + epsilon)
        target[place, :] = (source[place, :].astype(jnp.float32) * factor * gain_ref[...]).astype(
            target.dtype
        )
        return carry

    lax.fori_loop(0, source.shape[0] // block, body, 0)


def whole_kernel(
    sizes, mixer_hbm, expert_hbm, query_hbm, key_hbm, value_hbm, project_hbm, gate_hbm, up_hbm, down_hbm,
    mixer_gain_ref, expert_gain_ref, head_gain_ref, in_ref, forget_ref,
    group_router_ref, expert_router_ref, routes_ref,
    out_ref, mixed_ref,
    mixer_in, expert_in, query_w, key_w, value_w, project_ref, gate_ref, up_ref, down_ref,
    normed_a, normed_b, rank, combine, near_rows, far_rows,
    query_ref, key_ref, value_ref, cum_ref, cum_col_ref, packed_ref, acc,
    rows, part, pin, csum, xin, fin, ret,
    peer, plane, mem, pre, pre_in, state, state_peak, state_parts, mpart, mpin, msum, mxin,
    own_sem, send_a, recv_a, send_x, recv_x, send_p, recv_p,
    send_q, recv_q, send_c, recv_c, send_r, recv_r,
    send_m, recv_m, send_k, recv_k, send_h, recv_h, send_y, recv_y,
):
    n, share, cap, width, quarter, heads, size = sizes
    near = n // 2
    planes = n // 2
    me, tp = lax.axis_index("ep"), lax.axis_index("tp")
    core, column = lax.rem(tp, 2), lax.div(tp, 2)
    pair = tp + 1 - 2 * core
    cross = lax.rem(tp + 2, 4)
    pair_cross = lax.rem(pair + 2, 4)
    side, level = lax.rem(me, 2), lax.div(me, 2)
    mate = me + 1 - 2 * side
    tokens = expert_in.shape[0]
    length = mixer_in.shape[0]
    chunk = length // 4
    scale = size ** (-0.5)

    def other(i):
        total, bit = 0, 1
        while bit < n:
            total = total + bit * lax.rem(lax.div(me, bit) + lax.div(i, bit), 2)
            bit *= 2
        return total

    high = lax.rem(lax.div(me, near), 2)
    inner = lax.rem(high + lax.div(lax.rem(me, near), near // 2), 2)

    def far_turn(k):
        half = near // 2
        return near + half * lax.rem(lax.rem(k, 2) + 1 - inner, 2) + lax.div(k, 2)

    order = [(False, 0), (False, 1), (True, 0), (True, 1)]
    order += [(False, k) for k in range(2, near - 1)] + [(True, k) for k in range(2, near)]
    order += [(False, near - 1)] * (near > 2)

    def turn(t):
        total = 0
        for place, (far, k) in enumerate(order):
            total = total + jnp.where(t == place, far_turn(k) if far else k, 0)
        return total

    def is_far(t):
        total = t < 0
        for place, (far, k) in enumerate(order):
            total = total | (t == place) if far else total
        return total

    def remote(src, dst, send, recv, to):
        return pltpu.make_async_remote_copy(
            src_ref=src, dst_ref=dst, send_sem=send, recv_sem=recv, device_id=to, device_id_type=MESH
        )

    barrier = pltpu.get_barrier_semaphore()
    for i in range(1, n):
        pl.semaphore_signal(
            barrier, inc=1, device_id=(lax.rem(me + i, n), tp), device_id_type=MESH
        )
    pl.semaphore_signal(barrier, inc=1, device_id=(me, pair), device_id_type=MESH)
    pl.semaphore_signal(barrier, inc=1, device_id=(me, cross), device_id_type=MESH)

    loads = [
        pltpu.make_async_copy(src, dst, own_sem.at[k])
        for k, (src, dst) in enumerate(
            [
                (expert_hbm, expert_in), (gate_hbm, gate_ref), (up_hbm, up_ref),
                (down_hbm, down_ref), (mixer_hbm, mixer_in), (key_hbm, key_w),
                (value_hbm, value_w), (query_hbm, query_w), (project_hbm, project_ref),
            ]
        )
    ]
    for load in loads:
        load.start()

    def scatter_near(i, place):
        slot = jnp.maximum(i - 1, 0)
        return remote(
            near_rows.at[slot], rows.at[place, core], send_a.at[i], recv_a.at[i], (other(i), tp)
        )

    def scatter_far(i, place):
        slot = jnp.maximum(i - near, 0)
        mine = pl.ds(pl.multiple_of(column * share, share), share)
        return remote(
            far_rows.at[slot], rows.at[place, core, mine], send_a.at[i], recv_a.at[i], (other(i), tp)
        )

    def across(s, which):
        mine = pl.ds(pl.multiple_of(which * share, share), share)
        return remote(
            rows.at[s, core, mine], rows.at[s, core, mine], send_x.at[s], recv_x.at[s], (me, cross)
        )

    def beside(s, which):
        return remote(
            rows.at[s, which], rows.at[s, which], send_p.at[s], recv_p.at[s], (me, pair)
        )

    def halves(s, k, who):
        return remote(part.at[s, who], pin.at[s, k], send_q.at[s, k], recv_q.at[s, k], (me, pair))

    def summed(s):
        return remote(csum.at[s], xin.at[s], send_c.at[s], recv_c.at[s], (me, cross))

    def back(i):
        to = other(i)
        return remote(fin.at[to], ret.at[me], send_r.at[i], recv_r.at[i], (to, tp))

    def to_mate():
        return remote(
            packed_ref.at[1 - side], peer.at[1 - side], send_k.at[0], recv_k.at[0], (mate, tp)
        )

    def from_mate():
        return remote(packed_ref.at[side], peer.at[side], send_k.at[0], recv_k.at[0], (mate, tp))

    def rest_to_mate():
        return remote(packed_ref.at[0], peer.at[0], send_k.at[2], recv_k.at[2], (mate, tp))

    def to_level(d):
        return remote(
            plane, mem.at[level], send_m.at[d], recv_m.at[d], (lax.rem(me + 2 * d, n), tp)
        )

    def from_level(d):
        return remote(
            plane, mem.at[level - d], send_m.at[d], recv_m.at[d], (lax.rem(me + 2 * d, n), tp)
        )

    def prefix_mate():
        return remote(pre, pre_in, send_k.at[1], recv_k.at[1], (mate, tp))

    def mixed_half(k, who):
        return remote(mpart.at[who], mpin.at[k], send_h.at[k], recv_h.at[k], (me, pair))

    def mixed_sum(q):
        return remote(msum.at[q], mxin.at[q], send_y.at[q], recv_y.at[q], (me, cross))

    body, top_row, sum_row = slice(0, size), slice(size, size + 1), slice(size + 1, size + 2)

    def picks(e, first, count):
        slots = lax.broadcasted_iota(jnp.int32, (count, tokens), 0) + first
        return rank[pl.ds(e, 1), :] == slots.astype(jnp.float32)

    def gathered(parts):
        select = jnp.concatenate([jnp.where(p, 1.0, 0.0).astype(jnp.bfloat16) for p in parts], axis=0)
        return product(select, normed_b[...], nn).astype(jnp.bfloat16)

    def prepare_rank():
        experts = lax.broadcasted_iota(jnp.int32, (n, tokens), 0)
        matches = (routes_ref[0:1, :] == experts) | (routes_ref[1:2, :] == experts)
        earlier = lax.broadcasted_iota(jnp.int32, (tokens, tokens), 0)
        earlier = earlier < lax.broadcasted_iota(jnp.int32, (tokens, tokens), 1)
        count = product(
            jnp.where(matches, 1.0, 0.0).astype(jnp.bfloat16),
            jnp.where(earlier, 1.0, 0.0).astype(jnp.bfloat16),
            nn,
        )
        rank[...] = jnp.where(matches, count, -1.0)

    def prepare_combine():
        experts = lax.broadcasted_iota(jnp.int32, (n, tokens), 0)
        groups = group_router_ref.shape[0]
        expert_logits = product(expert_router_ref[...], normed_b[...], nt)
        group_logits = product(group_router_ref[...], normed_b[...], nt)
        group_full = jnp.zeros((n, tokens), jnp.float32)
        for g in range(groups):
            inside = (experts >= g * (n // groups)) & (experts < (g + 1) * (n // groups))
            group_full = group_full + jnp.where(inside, group_logits[g : g + 1, :], 0.0)
        named = [routes_ref[k : k + 1, :] == experts for k in range(2)]
        chosen = [jnp.sum(jnp.where(m, expert_logits, 0.0), axis=0, keepdims=True) for m in named]
        total = jnp.zeros((n, tokens), jnp.float32)
        for k in range(2):
            group_pick = jnp.sum(jnp.where(named[k], group_full, 0.0), axis=0, keepdims=True)
            weight = jax.nn.sigmoid(group_pick) * jax.nn.sigmoid(chosen[k] - chosen[1 - k])
            total = total + jnp.where(named[k], weight, 0.0)
        combine[...] = total

    def prepare_near():
        step_rows = 2 * share
        moved = gathered([picks(other(i), core * step_rows, step_rows) for i in range(1, near)])
        for i in range(1, near):
            near_rows[i - 1] = moved[(i - 1) * step_rows : i * step_rows]

    def prepare_far():
        first = core * (2 * share) + column * share
        moved = gathered([picks(other(i), first, share) for i in range(near, n)])
        for i in range(near, n):
            far_rows[i - near] = moved[(i - near) * share : (i - near + 1) * share]

    def prepare_own():
        rows[me] = gathered([picks(me, 0, cap)]).reshape(2, 2 * share, width)

    def ffn(s):
        x = rows[s].reshape(cap, width)
        gate_act = jnp.dot(x, gate_ref[...], preferred_element_type=jnp.float32)
        up_act = jnp.dot(x, up_ref[...], preferred_element_type=jnp.float32)
        hidden = (gate_act * jax.nn.sigmoid(gate_act) * up_act).astype(jnp.bfloat16)
        for q in range(4):
            part[s, q] = jnp.dot(
                hidden,
                down_ref[:, q * quarter : (q + 1) * quarter],
                preferred_element_type=jnp.float32,
            ).astype(jnp.bfloat16)

    def prepare_gates():
        log_forget = jnp.minimum(forget_ref[...], 0.0) - jnp.log1p(jnp.exp(-jnp.abs(forget_ref[...])))
        pieces = jnp.concatenate(
            [p.astype(jnp.float32) for p in three_parts(log_forget)]
            + [jnp.zeros((16 - 3 * heads, length), jnp.float32)],
            axis=0,
        ).astype(jnp.bfloat16)
        first = lax.broadcasted_iota(jnp.int32, (length, length), 0)
        upto = first <= lax.broadcasted_iota(jnp.int32, (length, length), 1)
        sums = product(pieces, jnp.where(upto, 1.0, 0.0).astype(jnp.bfloat16), nn)
        cum_ref[...] = sums[2 * heads : 3 * heads] + sums[heads : 2 * heads] + sums[0:heads]
        back_to = first >= lax.broadcasted_iota(jnp.int32, (length, length), 1)
        sums = product(jnp.where(back_to, 1.0, 0.0).astype(jnp.bfloat16), pieces, nt)
        cum_col_ref[...] = (
            sums[:, 2 * heads : 3 * heads] + sums[:, heads : 2 * heads] + sums[:, 0:heads]
        )

    def prepare_memory():
        key_ref[...] = jnp.dot(
            normed_a[...], key_w[...], preferred_element_type=jnp.float32
        ).astype(jnp.bfloat16)
        value_ref[...] = jnp.dot(
            normed_a[...], value_w[...], preferred_element_type=jnp.float32
        ).astype(jnp.bfloat16)
        for h in range(heads):
            cols = slice(h * size, (h + 1) * size)
            cum = cum_ref[h : h + 1, :]
            total = cum_ref[h : h + 1, length - 1 : length]
            log_weight = total - cum + in_ref[h : h + 1, :]
            peak = jnp.max(log_weight, axis=1, keepdims=True)
            weighted = value_ref[:, cols].astype(jnp.float32).T * jnp.exp(log_weight - peak)
            memory = jnp.zeros((size, size), jnp.float32)
            for piece in three_parts(weighted)[::-1]:
                memory = memory + product(piece, key_ref[:, cols], nn)
            packed_ref[h, body] = memory * scale
            packed_ref[h, size : size + 8] = jnp.zeros((8, size), jnp.float32)
            packed_ref[h, top_row] = jnp.broadcast_to(peak, (1, size))
            packed_ref[h, sum_row] = jnp.broadcast_to(total, (1, size))

    def prepare_query():
        query_ref[...] = jnp.dot(
            normed_a[...], query_w[...], preferred_element_type=jnp.float32
        ).astype(jnp.bfloat16)

    def combine_plane():
        from_mate().wait_recv()

        def joined(first, second):
            memory, peak = merged(
                first[side, body], first[side, top_row],
                second[side, body], second[side, top_row], second[side, sum_row],
            )
            plane[size : size + 8] = jnp.zeros((8, size), jnp.float32)
            plane[body] = memory
            plane[top_row] = peak
            plane[sum_row] = first[side, sum_row] + second[side, sum_row]

        @pl.when(side == 0)
        def _():
            joined(packed_ref, peer)

        @pl.when(side == 1)
        def _():
            joined(peer, packed_ref)

        for d in range(1, planes):
            @pl.when(level + d < planes)
            def _():
                to_level(d).start()

    def combine_levels():
        pre[...] = jnp.zeros_like(pre)
        pre[top_row] = jnp.full((1, size), floor_log, jnp.float32)
        for k in range(planes - 1):
            d = planes - 1 - k

            @pl.when(d <= level)
            def _():
                from_level(d).wait_recv()
                z = level - d
                memory, peak = merged(
                    pre[body], pre[top_row], mem[z, body], mem[z, top_row], mem[z, sum_row]
                )
                pre[body] = memory
                pre[top_row] = peak

        prefix_mate().start()

    def combine_last():
        prefix_mate().wait_recv()
        state[side] = pre[body]
        state_peak[side, 0:1, :] = pre[top_row]
        state[1 - side] = pre_in[body]
        state_peak[1 - side, 0:1, :] = pre_in[top_row]

        @pl.when(side == 1)
        def _():
            rest_to_mate().wait_recv()
            for h in range(heads):
                memory, peak = merged(
                    state[h], state_peak[h, 0:1, :],
                    peer[h, body], peer[h, top_row], peer[h, sum_row],
                )
                state[h] = memory
                state_peak[h, 0:1, :] = peak

        for h in range(heads):
            for piece, value in enumerate(three_parts(state[h])):
                state_parts[h, piece] = value

    def attend(j):
        start = pl.multiple_of(j * chunk, chunk)
        row = start + lax.broadcasted_iota(jnp.int32, (chunk, length), 0)
        causal = row >= lax.broadcasted_iota(jnp.int32, (chunk, length), 1)
        cell_list = []
        for h in range(heads):
            cols = slice(h * size, (h + 1) * size)
            q = query_ref[pl.ds(start, chunk), cols]
            c = cum_col_ref[pl.ds(start, chunk), h : h + 1]
            within = jnp.where(causal, c - cum_ref[h : h + 1, :] + in_ref[h : h + 1, :], -jnp.inf)
            carried = c + state_peak[h, 0:1, 0:1]
            top = jnp.maximum(jnp.max(within, axis=1, keepdims=True), carried)
            raw = product(q, key_ref[:, cols], nt)
            scores = (raw * scale * jnp.exp(within - top)).astype(jnp.bfloat16)
            cells = jnp.dot(scores, value_ref[:, cols], preferred_element_type=jnp.float32)
            held = jnp.zeros((chunk, size), jnp.float32)
            for piece in (2, 1, 0):
                held = held + product(q, state_parts[h, piece], nt)
            cells = cells + jnp.exp(carried - top) * held
            mean = jnp.mean(cells * cells, axis=1, keepdims=True)
            gain = head_gain_ref[pl.ds(tp * heads + h, 1), :]
            cell_list.append((cells * lax.rsqrt(mean + epsilon) * gain).astype(jnp.bfloat16))
        cell_rows = jnp.concatenate(cell_list, axis=1)
        for q in range(4):
            cols = slice(q * quarter, (q + 1) * quarter)
            mpart[j, q] = jnp.dot(
                cell_rows, project_ref[:, cols], preferred_element_type=jnp.float32
            ).astype(jnp.bfloat16)

    begin = n - 1

    def send_far(first):
        for k in range(first, first + 2):
            scatter_far(far_turn(k), me).start()

    def mixer_levels(t):
        @pl.when(t == begin - 2)
        def _():
            combine_levels()

    def mixer_first(t):
        @pl.when(t == n)
        def _():
            combine_last()

            def one(k, carry):
                attend(jnp.where(k == 0, pair_cross, cross))

                @pl.when(k == 0)
                def _():
                    mixed_half(1, pair_cross).start()

                return carry

            lax.fori_loop(0, 2, one, 0)

    def mixer_send(t):
        @pl.when(t == n + 1)
        def _():
            mixed_half(1, pair_cross).wait_recv()
            for q in range(4):
                msum[q] = (
                    mpart[cross, q].astype(jnp.float32) + mpin[1, q].astype(jnp.float32)
                ).astype(jnp.bfloat16)
                mixed_sum(q).start()

            def one(k, carry):
                attend(jnp.where(k == 0, pair, tp))

                @pl.when(k == 0)
                def _():
                    mixed_half(0, pair).start()

                return carry

            lax.fori_loop(0, 2, one, 0)

    def collect(s):
        halves(s, 1, pair_cross).wait_recv()
        csum[s] = (
            part[s, cross].astype(jnp.float32) + pin[s, 1].astype(jnp.float32)
        ).astype(jnp.bfloat16)
        summed(s).start()

    def send_halves(s):
        halves(s, 1, pair_cross).start()
        halves(s, 0, pair).start()

    prepare_rank()
    loads[0].wait()
    normalize(expert_in, expert_gain_ref, normed_b)
    prepare_near()
    prepare_far()
    pl.semaphore_wait(barrier, n + 1)
    scatter_near(1, me).start()

    @pl.when(inner == 0)
    def _():
        send_far(0)

    @pl.when(inner == 1)
    def _():
        for i in range(2, near - 1):
            scatter_near(i, me).start()

    prepare_own()
    for k in (1, 2, 3):
        loads[k].wait()
    ffn(me)
    send_halves(me)
    loads[4].wait()
    normalize(mixer_in, mixer_gain_ref, normed_a)
    collect(me)
    prepare_gates()
    loads[5].wait()
    loads[6].wait()
    prepare_memory()
    to_mate().start()

    @pl.when(inner == 0)
    def _():
        for i in range(2, near - 1):
            scatter_near(i, me).start()

    @pl.when(inner == 1)
    def _():
        send_far(0)
        if near > 2:
            scatter_near(near - 1, me).start()

    loads[7].wait()
    prepare_query()
    prepare_combine()
    loads[8].wait()

    def finish(t, carry):
        i = turn(t)
        s = other(i)

        @pl.when(t > 0)
        def _():
            back(i).wait_recv()

        chosen = picks(s, 0, cap)
        weight = combine[pl.ds(s, 1), :]
        high_weight = weight.astype(jnp.bfloat16).astype(jnp.float32)
        table = ret[s]
        acc[...] += product(
            jnp.where(chosen, high_weight, 0.0).astype(jnp.bfloat16), table, tn
        ) + product(jnp.where(chosen, weight - high_weight, 0.0).astype(jnp.bfloat16), table, tn)
        return carry

    acc[...] = jnp.zeros_like(acc)

    def step(t, carry):
        @pl.when((t >= 3) & (t < n + 2))
        def _():
            @pl.when(is_far(t - 2))
            def _():
                s = other(turn(t - 2))
                across(s, 1 - column).wait_recv()
                beside(s, core).start()

        @pl.when((t >= 3) & (t < n + 2))
        def _():
            s = other(turn(t - 2))
            beside(s, 1 - core).wait_recv()
            ffn(s)
            send_halves(s)

        @pl.when((t >= 3) & (t < n + 2))
        def _():
            collect(other(turn(t - 2)))

        mixer_send(t)

        @pl.when(t < n)
        def _():
            i = turn(t)
            s = other(i)

            @pl.when(is_far(t))
            def _():
                scatter_far(i, s).wait_recv()
                across(s, column).start()

            @pl.when(jnp.logical_not(is_far(t)))
            def _():
                scatter_near(i, s).wait_recv()
                beside(s, core).start()

        @pl.when(t == 1)
        def _():
            combine_plane()
            for first in range(2, near, 2):
                send_far(first)

            @pl.when(inner == 0)
            def _():
                if near > 2:
                    scatter_near(near - 1, me).start()

            @pl.when(side == 0)
            def _():
                rest_to_mate().start()

        mixer_first(t)

        @pl.when(t == n + 2)
        def _():
            lax.fori_loop(0, n - 3, finish, 0)

        @pl.when(t >= 3)
        def _():
            i = turn(t - 3)
            s = other(i)
            halves(s, 0, pair).wait_recv()
            summed(s).wait_recv()
            total = (
                part[s, tp].astype(jnp.float32)
                + pin[s, 0].astype(jnp.float32)
                + xin[s].astype(jnp.float32)
            ).astype(jnp.bfloat16)

            @pl.when(i > 0)
            def _():
                fin[s] = total
                back(i).start()

            @pl.when(i == 0)
            def _():
                ret[s] = total

        mixer_levels(t)
        return carry

    lax.fori_loop(1, n + 3, step, 0)

    lax.fori_loop(n - 3, n, finish, 0)
    out_ref[...] = acc[...].astype(out_ref.dtype)
    mixed_half(0, pair).wait_recv()
    for q in range(4):
        mixed_sum(q).wait_recv()
        cols = slice(q * quarter, (q + 1) * quarter)
        mixed_ref[:, cols] = (
            mpart[tp, q].astype(jnp.float32)
            + mpin[0, q].astype(jnp.float32)
            + mxin[q].astype(jnp.float32)
        ).astype(mixed_ref.dtype)

    def drain(i, carry):
        s = other(i)
        halves(s, 0, pair).wait_send()
        halves(s, 1, pair_cross).wait_send()
        summed(s).wait_send()

        @pl.when(i > 0)
        def _():
            beside(s, core).wait_send()
            back(i).wait_send()

        @pl.when((i > 0) & (i < near))
        def _():
            scatter_near(i, me).wait_send()

        @pl.when(i >= near)
        def _():
            scatter_far(i, me).wait_send()
            across(s, column).wait_send()

        return carry

    lax.fori_loop(0, n, drain, 0)
    to_mate().wait_send()

    @pl.when(side == 0)
    def _():
        rest_to_mate().wait_send()

    prefix_mate().wait_send()
    for d in range(1, planes):
        @pl.when(level + d < planes)
        def _():
            to_level(d).wait_send()
    mixed_half(0, pair).wait_send()
    mixed_half(1, pair_cross).wait_send()
    for q in range(4):
        mixed_sum(q).wait_send()


def hand_over(first_ref, second_ref, first_out, second_out):
    first_out[...] = first_ref[...]
    second_out[...] = second_ref[...]


def all_fused(
    mixer_in, mixer_gain, query_weight, key_weight, value_weight, input_gate, forget_gate,
    head_gain, mixer_out_weight, expert_in, expert_gain, group_router, expert_router, routes,
    gate_weight, up_weight, down_weight,
):
    n = expert_router.shape[1]
    tokens, width = expert_in.shape
    cap = 4 * tokens // n
    share = cap // 4
    quarter = width // 4
    length = mixer_in.shape[0]
    heads = input_gate.shape[0]
    inner_width = query_weight.shape[1]
    size = inner_width // heads
    hidden = gate_weight.shape[1]
    chunk = length // 4
    vmem = pl.BlockSpec(memory_space=pltpu.VMEM)
    whole = pl.BlockSpec(memory_space=pl.ANY)
    dma = pltpu.SemaphoreType.DMA
    bf = jnp.bfloat16
    f32 = jnp.float32
    results = pl.pallas_call(
        functools.partial(whole_kernel, (n, share, cap, width, quarter, heads, size)),
        out_shape=(
            jax.ShapeDtypeStruct((tokens, quarter), bf),
            jax.ShapeDtypeStruct((chunk, width), bf),
        ),
        in_specs=[whole] * 9 + [vmem] * 8,
        out_specs=(vmem, vmem),
        scratch_shapes=[
            pltpu.VMEM((length, width), bf),
            pltpu.VMEM((tokens, width), bf),
            pltpu.VMEM((width, inner_width), bf),
            pltpu.VMEM((width, inner_width), bf),
            pltpu.VMEM((width, inner_width), bf),
            pltpu.VMEM((inner_width, width), bf),
            pltpu.VMEM((width, hidden), bf),
            pltpu.VMEM((width, hidden), bf),
            pltpu.VMEM((hidden, width), bf),
            pltpu.VMEM((length, width), bf),
            pltpu.VMEM((tokens, width), bf),
            pltpu.VMEM((n, tokens), f32),
            pltpu.VMEM((n, tokens), f32),
            pltpu.VMEM((n // 2 - 1, 2 * share, width), bf),
            pltpu.VMEM((n // 2, share, width), bf),
            pltpu.VMEM((length, inner_width), bf),
            pltpu.VMEM((length, inner_width), bf),
            pltpu.VMEM((length, inner_width), bf),
            pltpu.VMEM((heads, length), f32),
            pltpu.VMEM((length, heads), f32),
            pltpu.VMEM((heads, size + 8, size), f32),
            pltpu.VMEM((tokens, quarter), f32),
            pltpu.VMEM((n, 2, 2 * share, width), bf),
            pltpu.VMEM((n, 4, cap, quarter), bf),
            pltpu.VMEM((n, 2, cap, quarter), bf),
            pltpu.VMEM((n, cap, quarter), bf),
            pltpu.VMEM((n, cap, quarter), bf),
            pltpu.VMEM((n, cap, quarter), bf),
            pltpu.VMEM((n, cap, quarter), bf),
            pltpu.VMEM((heads, size + 8, size), f32),
            pltpu.VMEM((size + 8, size), f32),
            pltpu.VMEM((n // 2, size + 8, size), f32),
            pltpu.VMEM((size + 8, size), f32),
            pltpu.VMEM((size + 8, size), f32),
            pltpu.VMEM((heads, size, size), f32),
            pltpu.VMEM((heads, 8, size), f32),
            pltpu.VMEM((heads, 3, size, size), bf),
            pltpu.VMEM((4, 4, chunk, quarter), bf),
            pltpu.VMEM((2, 4, chunk, quarter), bf),
            pltpu.VMEM((4, chunk, quarter), bf),
            pltpu.VMEM((4, chunk, quarter), bf),
            dma((9,)),
            dma((n,)), dma((n,)), dma((n,)), dma((n,)), dma((n,)), dma((n,)),
            dma((n, 2)), dma((n, 2)), dma((n,)), dma((n,)), dma((n,)), dma((n,)),
            dma((n // 2,)), dma((n // 2,)), dma((3,)), dma((3,)), dma((2,)), dma((2,)),
            dma((4,)), dma((4,)),
        ],
        compiler_params=pltpu.CompilerParams(
            collective_id=0, has_side_effects=True, vmem_limit_bytes=60 * 1024 * 1024
        ),
        cost_estimate=pl.CostEstimate(
            flops=60_000_000_000, bytes_accessed=8_000_000, transcendentals=0
        ),
    )(
        mixer_in, expert_in, query_weight, key_weight, value_weight, mixer_out_weight,
        gate_weight, up_weight, down_weight,
        mixer_gain.reshape(1, width), expert_gain.reshape(1, width),
        head_gain.reshape(-1, size), input_gate, forget_gate,
        group_router.T, expert_router.T, routes.T,
    )
    return pl.pallas_call(
        hand_over,
        out_shape=tuple(jax.ShapeDtypeStruct(r.shape, r.dtype) for r in results),
        in_specs=[vmem, vmem],
        out_specs=(vmem, vmem),
        compiler_params=pltpu.CompilerParams(vmem_limit_bytes=60 * 1024 * 1024),
    )(*results)


def experts_plain(own_share, gate_weight, up_weight, down_weight, mix):
    arrived = lax.all_to_all(own_share, "ep", split_axis=0, concat_axis=0, tiled=True)
    piece_rows = lax.all_gather(arrived, "tp", axis=1, tiled=True)
    gate_act = jnp.einsum(
        "scd,df->scf", piece_rows, gate_weight, preferred_element_type=jnp.float32
    )
    up_act = jnp.einsum("scd,df->scf", piece_rows, up_weight, preferred_element_type=jnp.float32)
    hidden = (jax.nn.silu(gate_act) * up_act).astype(jnp.bfloat16)
    partial_rows = jnp.einsum(
        "scf,fo->sco", hidden, down_weight, preferred_element_type=jnp.float32
    )
    summed = lax.psum_scatter(
        partial_rows.astype(jnp.bfloat16), "tp", scatter_dimension=2, tiled=True
    )
    returned = lax.all_to_all(summed, "ep", split_axis=0, concat_axis=0, tiled=True)
    return jnp.dot(
        mix, returned.reshape(-1, returned.shape[2]).astype(jnp.float32), precision=highest
    ).astype(jnp.bfloat16)


def mixer_prepare(normed_a, query_weight, key_weight, value_weight, input_gate, forget_gate):
    def project(weight):
        return jnp.dot(normed_a, weight, preferred_element_type=jnp.float32).astype(jnp.bfloat16)

    rows = normed_a.shape[0]
    heads = input_gate.shape[0]
    width_local = query_weight.shape[1]
    head_size = width_local // heads
    scale = head_size ** (-0.5)
    causal = jnp.tril(jnp.ones((rows, rows), dtype=bool))
    log_forget = jax.nn.log_sigmoid(forget_gate)
    cumulative = jnp.einsum(
        "hs,ts->ht", log_forget, causal.astype(jnp.float32), precision=highest
    )
    total = cumulative[:, -1]
    log_weight = total[:, None] - cumulative + input_gate
    peak = jnp.max(log_weight, axis=-1)
    weights = jnp.exp(log_weight - peak[:, None])
    keys = project(key_weight)
    values = project(value_weight)

    def by_head(matrix):
        return [matrix[:, h * head_size : (h + 1) * head_size] for h in range(heads)]

    key_heads, value_heads = by_head(keys), by_head(values)
    memory = jnp.stack(
        [
            lax.dot_general(
                value_heads[h].astype(jnp.float32) * weights[h][:, None],
                key_heads[h].astype(jnp.float32) * scale,
                (((0,), (0,)), ((), ())),
                precision=highest,
            )
            for h in range(heads)
        ]
    )
    stats = jnp.stack([peak, total], axis=1)
    stats = jnp.concatenate([stats, jnp.zeros((heads, 6), jnp.float32)], axis=1)
    packed = jnp.concatenate(
        [memory, jnp.broadcast_to(stats[:, :, None], (heads, 8, head_size))], axis=1
    )
    return (packed, project(query_weight), keys, values, cumulative, input_gate)


def mixer_partial(prepared, gain_local, mixer_out_weight):
    packed, queries, keys, values, cumulative, input_gate = prepared
    rows = queries.shape[0]
    heads, head_size = gain_local.shape
    scale = head_size ** (-0.5)
    causal = jnp.tril(jnp.ones((rows, rows), dtype=bool))

    def by_head(matrix):
        return [matrix[:, h * head_size : (h + 1) * head_size] for h in range(heads)]

    query_heads, key_heads, value_heads = by_head(queries), by_head(keys), by_head(values)
    everything = lax.all_gather(packed, "ep")
    n, place = lax.axis_size("ep"), lax.axis_index("ep")
    peaks = everything[:, :, head_size, 0]
    totals = everything[:, :, head_size + 1, 0]
    order = jnp.arange(n)
    later = (order[None, :] > order[:, None]) & (order[None, :] < place)
    suffix = jnp.sum(jnp.where(later[:, :, None], totals[None], 0.0), axis=1)
    before = (order < place)[:, None]
    candidate = jnp.where(before, peaks + suffix, floor_log)
    state_peak = jnp.max(candidate, axis=0)
    fade = jnp.where(before, jnp.exp(candidate - state_peak[None]), 0.0)
    state = jnp.sum(everything[:, :, :head_size] * fade[:, :, None, None], axis=0)
    cell_list = []
    for h in range(heads):
        c, gate = cumulative[h], input_gate[h]
        within = jnp.where(causal, c[:, None] - c[None, :] + gate[None, :], -jnp.inf)
        carried = c + state_peak[h]
        top = jnp.maximum(jnp.max(within, axis=-1), carried)
        raw = lax.dot_general(
            query_heads[h], key_heads[h], (((1,), (1,)), ((), ())), preferred_element_type=jnp.float32
        )
        scores = raw * scale * jnp.exp(within - top[:, None])
        cells = jnp.dot(
            scores.astype(jnp.bfloat16), value_heads[h], preferred_element_type=jnp.float32
        )
        carried_cells = lax.dot_general(
            query_heads[h].astype(jnp.float32),
            state[h],
            (((1,), (1,)), ((), ())),
            precision=highest,
        )
        cells = cells + jnp.exp(carried - top)[:, None] * carried_cells
        cell_list.append(rms_rows(cells, gain_local[h]).astype(jnp.bfloat16))
    cell_rows = jnp.concatenate(cell_list, axis=1)
    return jnp.dot(cell_rows, mixer_out_weight, preferred_element_type=jnp.float32).astype(
        jnp.bfloat16
    )


def shards(
    mixer_in,
    mixer_gain,
    query_weight,
    key_weight,
    value_weight,
    input_gate,
    forget_gate,
    head_gain,
    mixer_out_weight,
    expert_in,
    expert_gain,
    group_router,
    expert_router,
    routes,
    gate_experts,
    up_experts,
    down_experts,
):
    ranks = lax.axis_size("ep")
    share = expert_in.shape[0] // expert_router.shape[1]
    fused = lax.axis_size("tp") == 4 and ranks >= 4 and is_power(ranks) and share % 16 == 0
    fused = fused and mixer_in.shape[0] % 512 == 0 and input_gate.shape[0] == 2
    fused = fused and gate_experts.shape[0] == 1
    if fused:
        expert_out, mixer_out = all_fused(
            mixer_in, mixer_gain, query_weight, key_weight, value_weight, input_gate, forget_gate,
            head_gain, mixer_out_weight, expert_in, expert_gain, group_router, expert_router,
            routes, gate_experts[0], up_experts[0], down_experts[0],
        )
        return (mixer_out, expert_out)
    normed_b = rms_rows(expert_in, expert_gain).astype(jnp.bfloat16)
    tokens = normed_b.shape[0]
    expert_total = expert_router.shape[1]
    members = expert_total // group_router.shape[1]
    capacity = 4 * tokens // expert_total
    share = capacity // lax.axis_size("tp")
    group_logits = jnp.dot(normed_b, group_router, preferred_element_type=jnp.float32)
    expert_logits = jnp.dot(normed_b, expert_router, preferred_element_type=jnp.float32)
    expert_ids = jnp.arange(expert_total, dtype=jnp.int32)
    group_ids = jnp.arange(group_router.shape[1], dtype=jnp.int32)
    named = [routes[:, k : k + 1] == expert_ids[None, :] for k in range(2)]
    chosen = [jnp.sum(jnp.where(m, expert_logits, 0.0), axis=1, keepdims=True) for m in named]
    combine = jnp.zeros((tokens, expert_total), jnp.float32)
    for k in range(2):
        in_group = routes[:, k : k + 1] // members == group_ids[None, :]
        group_pick = jnp.sum(jnp.where(in_group, group_logits, 0.0), axis=1, keepdims=True)
        weight = jax.nn.sigmoid(group_pick) * jax.nn.sigmoid(chosen[k] - chosen[1 - k])
        combine = combine + jnp.where(named[k], weight, 0.0)
    matches = named[0] | named[1]
    earlier = jnp.tril(jnp.ones((tokens, tokens), jnp.bfloat16), -1)
    rank = jnp.dot(
        earlier, matches.astype(jnp.bfloat16), preferred_element_type=jnp.float32
    ).astype(jnp.int32)
    rank = jnp.where(matches, rank, -1)
    slots = jnp.arange(capacity, dtype=jnp.int32)
    mix = jnp.where(
        rank[:, :, None] == slots[None, None, :], combine[:, :, None], 0.0
    ).reshape(tokens, expert_total * capacity)
    own_slots = lax.axis_index("tp") * share + jnp.arange(share, dtype=jnp.int32)
    select = (rank.T[:, None, :] == own_slots[None, :, None]).astype(jnp.bfloat16)
    own_share = (
        jnp.dot(
            select.reshape(expert_total * share, tokens),
            normed_b,
            preferred_element_type=jnp.float32,
        )
        .astype(jnp.bfloat16)
        .reshape(expert_total, share, normed_b.shape[1])
    )
    normed_a = rms_rows(mixer_in, mixer_gain).astype(jnp.bfloat16)
    prepared = mixer_prepare(
        normed_a, query_weight, key_weight, value_weight, input_gate, forget_gate
    )
    width_local = query_weight.shape[1]
    gain_local = lax.dynamic_slice_in_dim(
        head_gain, lax.axis_index("tp") * width_local, width_local
    ).reshape(input_gate.shape[0], -1)
    experts = (own_share, gate_experts[0], up_experts[0], down_experts[0], mix)
    partial = mixer_partial(prepared, gain_local, mixer_out_weight)
    mixer_out = lax.psum_scatter(partial, "tp", scatter_dimension=0, tiled=True)
    expert_out = experts_plain(*experts)
    return (mixer_out, expert_out)


def solution(mesh):
    in_specs = (
        P("ep", None),
        P(),
        P(None, "tp"),
        P(None, "tp"),
        P(None, "tp"),
        P("tp", "ep"),
        P("tp", "ep"),
        P(),
        P("tp", None),
        P("ep", None),
        P(),
        P(),
        P(),
        P("ep", None),
        P("ep", None, "tp"),
        P("ep", None, "tp"),
        P("ep", "tp", None),
    )
    out_specs = (P(("ep", "tp"), None), P("ep", "tp"))
    return jax.shard_map(shards, mesh=mesh, in_specs=in_specs, out_specs=out_specs, check_vma=False)
```

```python
import functools

import jax
import jax.numpy as jnp
from jax import lax
from jax.experimental import pallas as pl
from jax.experimental.pallas import tpu as pltpu
from jax.sharding import PartitionSpec as P

MESH = pl.DeviceIdType.MESH


epsilon = 1e-06
highest = lax.Precision.HIGHEST
floor_log = -1e30


def is_power(count):
    return count & (count - 1) == 0


def rms_rows(matrix, gain):
    widened = matrix.astype(jnp.float32)
    scaled = widened * lax.rsqrt(jnp.mean(widened * widened, axis=-1, keepdims=True) + epsilon)
    return scaled * gain


def merged(earlier_memory, earlier_peak, later_memory, later_peak, later_total):
    moved = later_total + earlier_peak
    peak = jnp.maximum(moved, later_peak)
    return jnp.exp(moved - peak) * earlier_memory + jnp.exp(later_peak - peak) * later_memory, peak


def three_parts(matrix):
    parts = []
    for _ in range(3):
        top_part = matrix.astype(jnp.bfloat16)
        parts.append(top_part)
        matrix = matrix - top_part.astype(jnp.float32)
    return parts


nn = (((1,), (0,)), ((), ()))
nt = (((1,), (1,)), ((), ()))
tn = (((0,), (0,)), ((), ()))


def product(left, right, numbers):
    return lax.dot_general(left, right, numbers, preferred_element_type=jnp.float32)


def normalize(source, gain_ref, target):
    block = 64

    def body(b, carry):
        place = pl.ds(pl.multiple_of(b * block, block), block)
        widened = source[place, :].astype(jnp.float32)
        mean = jnp.mean(widened * widened, axis=-1, keepdims=True)
        factor = lax.rsqrt(mean + epsilon)
        target[place, :] = (source[place, :].astype(jnp.float32) * factor * gain_ref[...]).astype(
            target.dtype
        )
        return carry

    lax.fori_loop(0, source.shape[0] // block, body, 0)


def whole_kernel(
    sizes, mixer_hbm, expert_hbm, query_hbm, key_hbm, value_hbm, project_hbm, gate_hbm, up_hbm, down_hbm,
    mixer_gain_ref, expert_gain_ref, head_gain_ref, in_ref, forget_ref,
    group_router_ref, expert_router_ref, routes_ref,
    out_ref, mixed_ref,
    mixer_in, expert_in, query_w, key_w, value_w, project_ref, gate_ref, up_ref, down_ref,
    normed_a, normed_b, rank, rank_in, combine, near_rows, fwd, mine_b, entry_in,
    query_ref, key_ref, value_ref, cum_ref, cum_col_ref, packed_ref, acc,
    rows, part, pin, csum, xin, fin, ret,
    peer, plane, mem, pre, pre_in, state, state_peak, state_parts, mpart, mpin, msum, mxin,
    own_sem, send_a, recv_a, send_x, recv_x, send_p, recv_p,
    send_q, recv_q, send_c, recv_c, send_r, recv_r,
    send_m, recv_m, send_k, recv_k, send_h, recv_h, send_y, recv_y,
):
    n, share, cap, width, quarter, heads, size = sizes
    near = n // 2
    planes = n // 2
    me, tp = lax.axis_index("ep"), lax.axis_index("tp")
    core, column = lax.rem(tp, 2), lax.div(tp, 2)
    pair = tp + 1 - 2 * core
    cross = lax.rem(tp + 2, 4)
    pair_cross = lax.rem(pair + 2, 4)
    side, level = lax.rem(me, 2), lax.div(me, 2)
    mate = me + 1 - 2 * side
    tokens = expert_in.shape[0]
    length = mixer_in.shape[0]
    chunk = length // 4
    scale = size ** (-0.5)

    def other(i):
        total, bit = 0, 1
        while bit < n:
            total = total + bit * lax.rem(lax.div(me, bit) + lax.div(i, bit), 2)
            bit *= 2
        return total

    def far_turn(k):
        return near + (near // 2) * lax.rem(k, 2) + lax.div(k, 2)

    order = [(False, 0), (False, 1)] + [(False, k) for k in range(2, near - 1)]
    order += [(True, k) for k in range(near)]
    order += [(False, near - 1)] * (near > 2)

    def turn(t):
        total = 0
        for place, (far, k) in enumerate(order):
            total = total + jnp.where(t == place, far_turn(k) if far else k, 0)
        return total

    def is_far(t):
        total = t < 0
        for place, (far, k) in enumerate(order):
            total = total | (t == place) if far else total
        return total

    def remote(src, dst, send, recv, to):
        return pltpu.make_async_remote_copy(
            src_ref=src, dst_ref=dst, send_sem=send, recv_sem=recv, device_id=to, device_id_type=MESH
        )

    barrier = pltpu.get_barrier_semaphore()
    for i in range(1, n):
        pl.semaphore_signal(
            barrier, inc=1, device_id=(lax.rem(me + i, n), tp), device_id_type=MESH
        )
    pl.semaphore_signal(barrier, inc=1, device_id=(me, pair), device_id_type=MESH)
    pl.semaphore_signal(barrier, inc=1, device_id=(me, cross), device_id_type=MESH)

    loads = [
        pltpu.make_async_copy(src, dst, own_sem.at[k])
        for k, (src, dst) in enumerate(
            [
                (expert_hbm, expert_in), (gate_hbm, gate_ref), (up_hbm, up_ref),
                (down_hbm, down_ref), (mixer_hbm, mixer_in), (key_hbm, key_w),
                (value_hbm, value_w), (query_hbm, query_w), (project_hbm, project_ref),
            ]
        )
    ]
    for load in loads:
        load.start()

    def scatter_near(i, place):
        slot = jnp.maximum(i - 1, 0)
        return remote(
            near_rows.at[slot], rows.at[place, core], send_a.at[i], recv_a.at[i], (other(i), tp)
        )

    def entry():
        return remote(mine_b, entry_in, send_a.at[0], recv_a.at[0], (other(near), tp))

    def entry_rank():
        return remote(rank, rank_in, send_a.at[near], recv_a.at[near], (other(near), tp))

    def forward(j):
        return remote(
            fwd.at[j], rows.at[other(near), core, column],
            send_a.at[near + j], recv_a.at[near + j], (other(j), tp),
        )

    def arrival(i, s):
        return remote(
            fwd.at[i - near], rows.at[s, core, column], send_a.at[i], recv_a.at[i],
            (other(i - near), tp),
        )

    def across(s, which):
        return remote(
            rows.at[s, core, which], rows.at[s, core, which],
            send_x.at[s], recv_x.at[s], (me, cross),
        )

    def beside(s, which):
        return remote(
            rows.at[s, which], rows.at[s, which], send_p.at[s], recv_p.at[s], (me, pair)
        )

    def halves(s, k, who):
        return remote(part.at[s, who], pin.at[s, k], send_q.at[s, k], recv_q.at[s, k], (me, pair))

    def summed(s):
        return remote(csum.at[s], xin.at[s], send_c.at[s], recv_c.at[s], (me, cross))

    def back(i):
        to = other(i)
        return remote(fin.at[to], ret.at[me], send_r.at[i], recv_r.at[i], (to, tp))

    def to_mate():
        return remote(
            packed_ref.at[1 - side], peer.at[1 - side], send_k.at[0], recv_k.at[0], (mate, tp)
        )

    def from_mate():
        return remote(packed_ref.at[side], peer.at[side], send_k.at[0], recv_k.at[0], (mate, tp))

    def rest_to_mate():
        return remote(packed_ref.at[0], peer.at[0], send_k.at[2], recv_k.at[2], (mate, tp))

    def to_level(d):
        return remote(
            plane, mem.at[level], send_m.at[d], recv_m.at[d], (lax.rem(me + 2 * d, n), tp)
        )

    def from_level(d):
        return remote(
            plane, mem.at[level - d], send_m.at[d], recv_m.at[d], (lax.rem(me + 2 * d, n), tp)
        )

    def prefix_mate():
        return remote(pre, pre_in, send_k.at[1], recv_k.at[1], (mate, tp))

    def mixed_half(k, who):
        return remote(mpart.at[who], mpin.at[k], send_h.at[k], recv_h.at[k], (me, pair))

    def mixed_sum(q):
        return remote(msum.at[q], mxin.at[q], send_y.at[q], recv_y.at[q], (me, cross))

    body, top_row, sum_row = slice(0, size), slice(size, size + 1), slice(size + 1, size + 2)

    def picks(table, e):
        slots = lax.broadcasted_iota(jnp.int32, (cap, tokens), 0)
        return table[pl.ds(e, 1), :] == slots.astype(jnp.float32)

    def selection(table, experts):
        return jnp.concatenate(
            [jnp.where(picks(table, e), 1.0, 0.0).astype(jnp.bfloat16) for e in experts], axis=0
        )

    def features(q):
        return pl.ds(pl.multiple_of(q * quarter, quarter), quarter)

    def prepare_rank():
        experts = lax.broadcasted_iota(jnp.int32, (n, tokens), 0)
        matches = (routes_ref[0:1, :] == experts) | (routes_ref[1:2, :] == experts)
        earlier = lax.broadcasted_iota(jnp.int32, (tokens, tokens), 0)
        earlier = earlier < lax.broadcasted_iota(jnp.int32, (tokens, tokens), 1)
        count = product(
            jnp.where(matches, 1.0, 0.0).astype(jnp.bfloat16),
            jnp.where(earlier, 1.0, 0.0).astype(jnp.bfloat16),
            nn,
        )
        rank[...] = jnp.where(matches, count, -1.0)

    def prepare_combine():
        experts = lax.broadcasted_iota(jnp.int32, (n, tokens), 0)
        groups = group_router_ref.shape[0]
        expert_logits = product(expert_router_ref[...], normed_b[...], nt)
        group_logits = product(group_router_ref[...], normed_b[...], nt)
        group_full = jnp.zeros((n, tokens), jnp.float32)
        for g in range(groups):
            inside = (experts >= g * (n // groups)) & (experts < (g + 1) * (n // groups))
            group_full = group_full + jnp.where(inside, group_logits[g : g + 1, :], 0.0)
        named = [routes_ref[k : k + 1, :] == experts for k in range(2)]
        chosen = [jnp.sum(jnp.where(m, expert_logits, 0.0), axis=0, keepdims=True) for m in named]
        total = jnp.zeros((n, tokens), jnp.float32)
        for k in range(2):
            group_pick = jnp.sum(jnp.where(named[k], group_full, 0.0), axis=0, keepdims=True)
            weight = jax.nn.sigmoid(group_pick) * jax.nn.sigmoid(chosen[k] - chosen[1 - k])
            total = total + jnp.where(named[k], weight, 0.0)
        combine[...] = total

    def prepare_near():
        select = selection(rank, [other(i) for i in range(1, near)])
        for c in range(2):
            moved = product(select, normed_b[:, features(2 * c + core)], nn).astype(jnp.bfloat16)
            for i in range(1, near):
                near_rows[i - 1, c] = moved[(i - 1) * cap : i * cap]

    def prepare_own():
        moved = product(selection(rank, [me]), normed_b[...], nn).astype(jnp.bfloat16)
        for q in range(4):
            rows[me, q % 2, q // 2] = moved[:, q * quarter : (q + 1) * quarter]

    def redistribute():
        entry_rank().wait_recv()
        entry().wait_recv()
        select = selection(rank_in, [other(j) for j in range(near)])
        moved = product(select, entry_in[...], nn).astype(jnp.bfloat16)
        for j in range(1, near):
            fwd[j] = moved[j * cap : (j + 1) * cap]
        rows[other(near), core, column] = moved[0:cap]
        for j in range(1, near):
            forward(j).start()

    def ffn(s):
        x = jnp.concatenate([rows[s, q % 2, q // 2] for q in range(4)], axis=1)
        gate_act = jnp.dot(x, gate_ref[...], preferred_element_type=jnp.float32)
        up_act = jnp.dot(x, up_ref[...], preferred_element_type=jnp.float32)
        hidden = (gate_act * jax.nn.sigmoid(gate_act) * up_act).astype(jnp.bfloat16)
        for q in range(4):
            part[s, q] = jnp.dot(
                hidden,
                down_ref[:, q * quarter : (q + 1) * quarter],
                preferred_element_type=jnp.float32,
            ).astype(jnp.bfloat16)

    def prepare_gates():
        log_forget = jnp.minimum(forget_ref[...], 0.0) - jnp.log1p(jnp.exp(-jnp.abs(forget_ref[...])))
        pieces = jnp.concatenate(
            [p.astype(jnp.float32) for p in three_parts(log_forget)]
            + [jnp.zeros((16 - 3 * heads, length), jnp.float32)],
            axis=0,
        ).astype(jnp.bfloat16)
        first = lax.broadcasted_iota(jnp.int32, (length, length), 0)
        upto = first <= lax.broadcasted_iota(jnp.int32, (length, length), 1)
        sums = product(pieces, jnp.where(upto, 1.0, 0.0).astype(jnp.bfloat16), nn)
        cum_ref[...] = sums[2 * heads : 3 * heads] + sums[heads : 2 * heads] + sums[0:heads]
        back_to = first >= lax.broadcasted_iota(jnp.int32, (length, length), 1)
        sums = product(jnp.where(back_to, 1.0, 0.0).astype(jnp.bfloat16), pieces, nt)
        cum_col_ref[...] = (
            sums[:, 2 * heads : 3 * heads] + sums[:, heads : 2 * heads] + sums[:, 0:heads]
        )

    def prepare_memory():
        key_ref[...] = jnp.dot(
            normed_a[...], key_w[...], preferred_element_type=jnp.float32
        ).astype(jnp.bfloat16)
        value_ref[...] = jnp.dot(
            normed_a[...], value_w[...], preferred_element_type=jnp.float32
        ).astype(jnp.bfloat16)
        for h in range(heads):
            cols = slice(h * size, (h + 1) * size)
            cum = cum_ref[h : h + 1, :]
            total = cum_ref[h : h + 1, length - 1 : length]
            log_weight = total - cum + in_ref[h : h + 1, :]
            peak = jnp.max(log_weight, axis=1, keepdims=True)
            weighted = value_ref[:, cols].astype(jnp.float32).T * jnp.exp(log_weight - peak)
            memory = jnp.zeros((size, size), jnp.float32)
            for piece in three_parts(weighted)[::-1]:
                memory = memory + product(piece, key_ref[:, cols], nn)
            packed_ref[h, body] = memory * scale
            packed_ref[h, size : size + 8] = jnp.zeros((8, size), jnp.float32)
            packed_ref[h, top_row] = jnp.broadcast_to(peak, (1, size))
            packed_ref[h, sum_row] = jnp.broadcast_to(total, (1, size))

    def prepare_query():
        query_ref[...] = jnp.dot(
            normed_a[...], query_w[...], preferred_element_type=jnp.float32
        ).astype(jnp.bfloat16)

    def combine_plane():
        from_mate().wait_recv()

        def joined(first, second):
            memory, peak = merged(
                first[side, body], first[side, top_row],
                second[side, body], second[side, top_row], second[side, sum_row],
            )
            plane[size : size + 8] = jnp.zeros((8, size), jnp.float32)
            plane[body] = memory
            plane[top_row] = peak
            plane[sum_row] = first[side, sum_row] + second[side, sum_row]

        @pl.when(side == 0)
        def _():
            joined(packed_ref, peer)

        @pl.when(side == 1)
        def _():
            joined(peer, packed_ref)

        for d in range(1, planes):
            @pl.when(level + d < planes)
            def _():
                to_level(d).start()

    def combine_levels():
        pre[...] = jnp.zeros_like(pre)
        pre[top_row] = jnp.full((1, size), floor_log, jnp.float32)
        for k in range(planes - 1):
            d = planes - 1 - k

            @pl.when(d <= level)
            def _():
                from_level(d).wait_recv()
                z = level - d
                memory, peak = merged(
                    pre[body], pre[top_row], mem[z, body], mem[z, top_row], mem[z, sum_row]
                )
                pre[body] = memory
                pre[top_row] = peak

        prefix_mate().start()

    def combine_last():
        prefix_mate().wait_recv()
        state[side] = pre[body]
        state_peak[side, 0:1, :] = pre[top_row]
        state[1 - side] = pre_in[body]
        state_peak[1 - side, 0:1, :] = pre_in[top_row]

        @pl.when(side == 1)
        def _():
            rest_to_mate().wait_recv()
            for h in range(heads):
                memory, peak = merged(
                    state[h], state_peak[h, 0:1, :],
                    peer[h, body], peer[h, top_row], peer[h, sum_row],
                )
                state[h] = memory
                state_peak[h, 0:1, :] = peak

        for h in range(heads):
            for piece, value in enumerate(three_parts(state[h])):
                state_parts[h, piece] = value

    def attend(j):
        start = pl.multiple_of(j * chunk, chunk)
        row = start + lax.broadcasted_iota(jnp.int32, (chunk, length), 0)
        causal = row >= lax.broadcasted_iota(jnp.int32, (chunk, length), 1)
        cell_list = []
        for h in range(heads):
            cols = slice(h * size, (h + 1) * size)
            q = query_ref[pl.ds(start, chunk), cols]
            c = cum_col_ref[pl.ds(start, chunk), h : h + 1]
            within = jnp.where(causal, c - cum_ref[h : h + 1, :] + in_ref[h : h + 1, :], -jnp.inf)
            carried = c + state_peak[h, 0:1, 0:1]
            top = jnp.maximum(jnp.max(within, axis=1, keepdims=True), carried)
            raw = product(q, key_ref[:, cols], nt)
            scores = (raw * scale * jnp.exp(within - top)).astype(jnp.bfloat16)
            cells = jnp.dot(scores, value_ref[:, cols], preferred_element_type=jnp.float32)
            held = jnp.zeros((chunk, size), jnp.float32)
            for piece in (2, 1, 0):
                held = held + product(q, state_parts[h, piece], nt)
            cells = cells + jnp.exp(carried - top) * held
            mean = jnp.mean(cells * cells, axis=1, keepdims=True)
            gain = head_gain_ref[pl.ds(tp * heads + h, 1), :]
            cell_list.append((cells * lax.rsqrt(mean + epsilon) * gain).astype(jnp.bfloat16))
        cell_rows = jnp.concatenate(cell_list, axis=1)
        for q in range(4):
            cols = slice(q * quarter, (q + 1) * quarter)
            mpart[j, q] = jnp.dot(
                cell_rows, project_ref[:, cols], preferred_element_type=jnp.float32
            ).astype(jnp.bfloat16)

    begin = n - 1

    def mixer_levels(t):
        @pl.when(t == 4)
        def _():
            combine_levels()

    def mixer_first(t):
        @pl.when(t == n)
        def _():
            combine_last()

            def one(k, carry):
                attend(jnp.where(k == 0, pair_cross, cross))

                @pl.when(k == 0)
                def _():
                    mixed_half(1, pair_cross).start()

                return carry

            lax.fori_loop(0, 2, one, 0)

    def mixer_send(t):
        @pl.when(t == n + 1)
        def _():
            mixed_half(1, pair_cross).wait_recv()
            for q in range(4):
                msum[q] = (
                    mpart[cross, q].astype(jnp.float32) + mpin[1, q].astype(jnp.float32)
                ).astype(jnp.bfloat16)
            for q in range(0):
                mixed_sum(q).start()

        @pl.when(t == n + 1)
        def _():
            for q in range(0, 4):
                mixed_sum(q).start()

            def one(k, carry):
                attend(jnp.where(k == 0, pair, tp))

                @pl.when(k == 0)
                def _():
                    mixed_half(0, pair).start()

                return carry

            lax.fori_loop(0, 2, one, 0)

    def collect(s):
        halves(s, 1, pair_cross).wait_recv()
        csum[s] = (
            part[s, cross].astype(jnp.float32) + pin[s, 1].astype(jnp.float32)
        ).astype(jnp.bfloat16)
        summed(s).start()

    def send_halves(s):
        halves(s, 1, pair_cross).start()
        halves(s, 0, pair).start()

    prepare_rank()
    loads[0].wait()
    normalize(expert_in, expert_gain_ref, normed_b)
    mine_b[...] = normed_b[:, features(tp)]
    prepare_near()
    pl.semaphore_wait(barrier, n + 1)
    entry_rank().start()
    entry().start()
    scatter_near(1, me).start()
    prepare_own()
    for k in (1, 2, 3):
        loads[k].wait()
    ffn(me)
    send_halves(me)
    for i in range(2, near - 1):
        scatter_near(i, me).start()
    loads[4].wait()
    normalize(mixer_in, mixer_gain_ref, normed_a)
    collect(me)
    prepare_gates()
    loads[5].wait()
    loads[6].wait()
    prepare_memory()
    to_mate().start()
    loads[7].wait()
    prepare_query()
    prepare_combine()
    loads[8].wait()

    def finish(t, carry):
        i = turn(t)
        s = other(i)

        @pl.when(t > 0)
        def _():
            back(i).wait_recv()

        chosen = picks(rank, s)
        weight = combine[pl.ds(s, 1), :]
        high_weight = weight.astype(jnp.bfloat16).astype(jnp.float32)
        table = ret[s]
        acc[...] += product(
            jnp.where(chosen, high_weight, 0.0).astype(jnp.bfloat16), table, tn
        ) + product(jnp.where(chosen, weight - high_weight, 0.0).astype(jnp.bfloat16), table, tn)
        return carry

    acc[...] = jnp.zeros_like(acc)

    def step(t, carry):
        working = (t == 2) | ((t > 3) & (t < n + 2))
        now = jnp.where(t == 2, 1, t - 2)

        @pl.when(working)
        def _():
            @pl.when(is_far(now))
            def _():
                s = other(turn(now))
                across(s, 1 - column).wait_recv()
                beside(s, core).start()

        @pl.when(working)
        def _():
            s = other(turn(now))
            beside(s, 1 - core).wait_recv()
            ffn(s)
            send_halves(s)

        @pl.when(working)
        def _():
            collect(other(turn(now)))

        mixer_send(t)

        @pl.when(t == 2)
        def _():
            redistribute()

        @pl.when(t == 4)
        def _():
            if near > 2:
                scatter_near(near - 1, me).start()

        def arrive(place, carry):
            i = turn(place)
            s = other(i)

            @pl.when(is_far(place))
            def _():
                @pl.when(i > near)
                def _():
                    arrival(i, s).wait_recv()

                across(s, column).start()

            @pl.when(jnp.logical_not(is_far(place)))
            def _():
                scatter_near(i, s).wait_recv()
                beside(s, core).start()

            return carry

        begins = jnp.where(t > near + 1, jnp.where(t == n - 1, n - 1, n), t)
        ends = jnp.where(t == near + 1, t + 2, t + 1)
        lax.fori_loop(jnp.minimum(begins, n), jnp.minimum(ends, n), arrive, 0)

        @pl.when(t == 1)
        def _():
            combine_plane()

            @pl.when(side == 0)
            def _():
                rest_to_mate().start()

        mixer_first(t)

        @pl.when(t == n + 2)
        def _():
            lax.fori_loop(0, n - 3, finish, 0)

        @pl.when(t >= 3)
        def _():
            i = turn(t - 3)
            s = other(i)
            halves(s, 0, pair).wait_recv()
            summed(s).wait_recv()
            total = (
                part[s, tp].astype(jnp.float32)
                + pin[s, 0].astype(jnp.float32)
                + xin[s].astype(jnp.float32)
            ).astype(jnp.bfloat16)

            @pl.when(i > 0)
            def _():
                fin[s] = total
                back(i).start()

            @pl.when(i == 0)
            def _():
                ret[s] = total

        mixer_levels(t)
        return carry

    lax.fori_loop(1, n + 3, step, 0)

    lax.fori_loop(n - 3, n, finish, 0)
    out_ref[...] = acc[...].astype(out_ref.dtype)
    mixed_half(0, pair).wait_recv()
    for q in range(4):
        mixed_sum(q).wait_recv()
        cols = slice(q * quarter, (q + 1) * quarter)
        mixed_ref[:, cols] = (
            mpart[tp, q].astype(jnp.float32)
            + mpin[0, q].astype(jnp.float32)
            + mxin[q].astype(jnp.float32)
        ).astype(mixed_ref.dtype)

    def drain(i, carry):
        s = other(i)
        halves(s, 0, pair).wait_send()
        halves(s, 1, pair_cross).wait_send()
        summed(s).wait_send()

        @pl.when(i > 0)
        def _():
            beside(s, core).wait_send()
            back(i).wait_send()

        @pl.when((i > 0) & (i < near))
        def _():
            scatter_near(i, me).wait_send()

        @pl.when(i >= near)
        def _():
            across(s, column).wait_send()
            @pl.when(i > near)
            def _():
                forward(i - near).wait_send()

        return carry

    lax.fori_loop(0, n, drain, 0)
    entry().wait_send()
    entry_rank().wait_send()
    to_mate().wait_send()

    @pl.when(side == 0)
    def _():
        rest_to_mate().wait_send()

    prefix_mate().wait_send()
    for d in range(1, planes):
        @pl.when(level + d < planes)
        def _():
            to_level(d).wait_send()
    mixed_half(0, pair).wait_send()
    mixed_half(1, pair_cross).wait_send()
    for q in range(4):
        mixed_sum(q).wait_send()


def hand_over(first_ref, second_ref, first_out, second_out):
    first_out[...] = first_ref[...]
    second_out[...] = second_ref[...]


def all_fused(
    mixer_in, mixer_gain, query_weight, key_weight, value_weight, input_gate, forget_gate,
    head_gain, mixer_out_weight, expert_in, expert_gain, group_router, expert_router, routes,
    gate_weight, up_weight, down_weight,
):
    n = expert_router.shape[1]
    tokens, width = expert_in.shape
    cap = 4 * tokens // n
    share = cap // 4
    quarter = width // 4
    length = mixer_in.shape[0]
    heads = input_gate.shape[0]
    inner_width = query_weight.shape[1]
    size = inner_width // heads
    hidden = gate_weight.shape[1]
    chunk = length // 4
    vmem = pl.BlockSpec(memory_space=pltpu.VMEM)
    whole = pl.BlockSpec(memory_space=pl.ANY)
    dma = pltpu.SemaphoreType.DMA
    bf = jnp.bfloat16
    f32 = jnp.float32
    results = pl.pallas_call(
        functools.partial(whole_kernel, (n, share, cap, width, quarter, heads, size)),
        out_shape=(
            jax.ShapeDtypeStruct((tokens, quarter), bf),
            jax.ShapeDtypeStruct((chunk, width), bf),
        ),
        in_specs=[whole] * 9 + [vmem] * 8,
        out_specs=(vmem, vmem),
        scratch_shapes=[
            pltpu.VMEM((length, width), bf),
            pltpu.VMEM((tokens, width), bf),
            pltpu.VMEM((width, inner_width), bf),
            pltpu.VMEM((width, inner_width), bf),
            pltpu.VMEM((width, inner_width), bf),
            pltpu.VMEM((inner_width, width), bf),
            pltpu.VMEM((width, hidden), bf),
            pltpu.VMEM((width, hidden), bf),
            pltpu.VMEM((hidden, width), bf),
            pltpu.VMEM((length, width), bf),
            pltpu.VMEM((tokens, width), bf),
            pltpu.VMEM((n, tokens), f32),
            pltpu.VMEM((n, tokens), f32),
            pltpu.VMEM((n, tokens), f32),
            pltpu.VMEM((n // 2 - 1, 2, cap, quarter), bf),
            pltpu.VMEM((n // 2, cap, quarter), bf),
            pltpu.VMEM((tokens, quarter), bf),
            pltpu.VMEM((tokens, quarter), bf),
            pltpu.VMEM((length, inner_width), bf),
            pltpu.VMEM((length, inner_width), bf),
            pltpu.VMEM((length, inner_width), bf),
            pltpu.VMEM((heads, length), f32),
            pltpu.VMEM((length, heads), f32),
            pltpu.VMEM((heads, size + 8, size), f32),
            pltpu.VMEM((tokens, quarter), f32),
            pltpu.VMEM((n, 2, 2, cap, quarter), bf),
            pltpu.VMEM((n, 4, cap, quarter), bf),
            pltpu.VMEM((n, 2, cap, quarter), bf),
            pltpu.VMEM((n, cap, quarter), bf),
            pltpu.VMEM((n, cap, quarter), bf),
            pltpu.VMEM((n, cap, quarter), bf),
            pltpu.VMEM((n, cap, quarter), bf),
            pltpu.VMEM((heads, size + 8, size), f32),
            pltpu.VMEM((size + 8, size), f32),
            pltpu.VMEM((n // 2, size + 8, size), f32),
            pltpu.VMEM((size + 8, size), f32),
            pltpu.VMEM((size + 8, size), f32),
            pltpu.VMEM((heads, size, size), f32),
            pltpu.VMEM((heads, 8, size), f32),
            pltpu.VMEM((heads, 3, size, size), bf),
            pltpu.VMEM((4, 4, chunk, quarter), bf),
            pltpu.VMEM((2, 4, chunk, quarter), bf),
            pltpu.VMEM((4, chunk, quarter), bf),
            pltpu.VMEM((4, chunk, quarter), bf),
            dma((9,)),
            dma((n,)), dma((n,)), dma((n,)), dma((n,)), dma((n,)), dma((n,)),
            dma((n, 2)), dma((n, 2)), dma((n,)), dma((n,)), dma((n,)), dma((n,)),
            dma((n // 2,)), dma((n // 2,)), dma((3,)), dma((3,)), dma((2,)), dma((2,)),
            dma((4,)), dma((4,)),
        ],
        compiler_params=pltpu.CompilerParams(
            collective_id=0, has_side_effects=True, vmem_limit_bytes=60 * 1024 * 1024
        ),
        cost_estimate=pl.CostEstimate(
            flops=60_000_000_000, bytes_accessed=8_000_000, transcendentals=0
        ),
    )(
        mixer_in, expert_in, query_weight, key_weight, value_weight, mixer_out_weight,
        gate_weight, up_weight, down_weight,
        mixer_gain.reshape(1, width), expert_gain.reshape(1, width),
        head_gain.reshape(-1, size), input_gate, forget_gate,
        group_router.T, expert_router.T, routes.T,
    )
    return pl.pallas_call(
        hand_over,
        out_shape=tuple(jax.ShapeDtypeStruct(r.shape, r.dtype) for r in results),
        in_specs=[vmem, vmem],
        out_specs=(vmem, vmem),
        compiler_params=pltpu.CompilerParams(vmem_limit_bytes=60 * 1024 * 1024),
    )(*results)


def experts_plain(own_share, gate_weight, up_weight, down_weight, mix):
    arrived = lax.all_to_all(own_share, "ep", split_axis=0, concat_axis=0, tiled=True)
    piece_rows = lax.all_gather(arrived, "tp", axis=1, tiled=True)
    gate_act = jnp.einsum(
        "scd,df->scf", piece_rows, gate_weight, preferred_element_type=jnp.float32
    )
    up_act = jnp.einsum("scd,df->scf", piece_rows, up_weight, preferred_element_type=jnp.float32)
    hidden = (jax.nn.silu(gate_act) * up_act).astype(jnp.bfloat16)
    partial_rows = jnp.einsum(
        "scf,fo->sco", hidden, down_weight, preferred_element_type=jnp.float32
    )
    summed = lax.psum_scatter(
        partial_rows.astype(jnp.bfloat16), "tp", scatter_dimension=2, tiled=True
    )
    returned = lax.all_to_all(summed, "ep", split_axis=0, concat_axis=0, tiled=True)
    return jnp.dot(
        mix, returned.reshape(-1, returned.shape[2]).astype(jnp.float32), precision=highest
    ).astype(jnp.bfloat16)


def mixer_prepare(normed_a, query_weight, key_weight, value_weight, input_gate, forget_gate):
    def project(weight):
        return jnp.dot(normed_a, weight, preferred_element_type=jnp.float32).astype(jnp.bfloat16)

    rows = normed_a.shape[0]
    heads = input_gate.shape[0]
    width_local = query_weight.shape[1]
    head_size = width_local // heads
    scale = head_size ** (-0.5)
    causal = jnp.tril(jnp.ones((rows, rows), dtype=bool))
    log_forget = jax.nn.log_sigmoid(forget_gate)
    cumulative = jnp.einsum(
        "hs,ts->ht", log_forget, causal.astype(jnp.float32), precision=highest
    )
    total = cumulative[:, -1]
    log_weight = total[:, None] - cumulative + input_gate
    peak = jnp.max(log_weight, axis=-1)
    weights = jnp.exp(log_weight - peak[:, None])
    keys = project(key_weight)
    values = project(value_weight)

    def by_head(matrix):
        return [matrix[:, h * head_size : (h + 1) * head_size] for h in range(heads)]

    key_heads, value_heads = by_head(keys), by_head(values)
    memory = jnp.stack(
        [
            lax.dot_general(
                value_heads[h].astype(jnp.float32) * weights[h][:, None],
                key_heads[h].astype(jnp.float32) * scale,
                (((0,), (0,)), ((), ())),
                precision=highest,
            )
            for h in range(heads)
        ]
    )
    stats = jnp.stack([peak, total], axis=1)
    stats = jnp.concatenate([stats, jnp.zeros((heads, 6), jnp.float32)], axis=1)
    packed = jnp.concatenate(
        [memory, jnp.broadcast_to(stats[:, :, None], (heads, 8, head_size))], axis=1
    )
    return (packed, project(query_weight), keys, values, cumulative, input_gate)


def mixer_partial(prepared, gain_local, mixer_out_weight):
    packed, queries, keys, values, cumulative, input_gate = prepared
    rows = queries.shape[0]
    heads, head_size = gain_local.shape
    scale = head_size ** (-0.5)
    causal = jnp.tril(jnp.ones((rows, rows), dtype=bool))

    def by_head(matrix):
        return [matrix[:, h * head_size : (h + 1) * head_size] for h in range(heads)]

    query_heads, key_heads, value_heads = by_head(queries), by_head(keys), by_head(values)
    everything = lax.all_gather(packed, "ep")
    n, place = lax.axis_size("ep"), lax.axis_index("ep")
    peaks = everything[:, :, head_size, 0]
    totals = everything[:, :, head_size + 1, 0]
    order = jnp.arange(n)
    later = (order[None, :] > order[:, None]) & (order[None, :] < place)
    suffix = jnp.sum(jnp.where(later[:, :, None], totals[None], 0.0), axis=1)
    before = (order < place)[:, None]
    candidate = jnp.where(before, peaks + suffix, floor_log)
    state_peak = jnp.max(candidate, axis=0)
    fade = jnp.where(before, jnp.exp(candidate - state_peak[None]), 0.0)
    state = jnp.sum(everything[:, :, :head_size] * fade[:, :, None, None], axis=0)
    cell_list = []
    for h in range(heads):
        c, gate = cumulative[h], input_gate[h]
        within = jnp.where(causal, c[:, None] - c[None, :] + gate[None, :], -jnp.inf)
        carried = c + state_peak[h]
        top = jnp.maximum(jnp.max(within, axis=-1), carried)
        raw = lax.dot_general(
            query_heads[h], key_heads[h], (((1,), (1,)), ((), ())), preferred_element_type=jnp.float32
        )
        scores = raw * scale * jnp.exp(within - top[:, None])
        cells = jnp.dot(
            scores.astype(jnp.bfloat16), value_heads[h], preferred_element_type=jnp.float32
        )
        carried_cells = lax.dot_general(
            query_heads[h].astype(jnp.float32),
            state[h],
            (((1,), (1,)), ((), ())),
            precision=highest,
        )
        cells = cells + jnp.exp(carried - top)[:, None] * carried_cells
        cell_list.append(rms_rows(cells, gain_local[h]).astype(jnp.bfloat16))
    cell_rows = jnp.concatenate(cell_list, axis=1)
    return jnp.dot(cell_rows, mixer_out_weight, preferred_element_type=jnp.float32).astype(
        jnp.bfloat16
    )


def shards(
    mixer_in,
    mixer_gain,
    query_weight,
    key_weight,
    value_weight,
    input_gate,
    forget_gate,
    head_gain,
    mixer_out_weight,
    expert_in,
    expert_gain,
    group_router,
    expert_router,
    routes,
    gate_experts,
    up_experts,
    down_experts,
):
    ranks = lax.axis_size("ep")
    share = expert_in.shape[0] // expert_router.shape[1]
    fused = lax.axis_size("tp") == 4 and ranks >= 4 and is_power(ranks) and share % 16 == 0
    fused = fused and mixer_in.shape[0] % 512 == 0 and input_gate.shape[0] == 2
    fused = fused and gate_experts.shape[0] == 1
    if fused:
        expert_out, mixer_out = all_fused(
            mixer_in, mixer_gain, query_weight, key_weight, value_weight, input_gate, forget_gate,
            head_gain, mixer_out_weight, expert_in, expert_gain, group_router, expert_router,
            routes, gate_experts[0], up_experts[0], down_experts[0],
        )
        return (mixer_out, expert_out)
    normed_b = rms_rows(expert_in, expert_gain).astype(jnp.bfloat16)
    tokens = normed_b.shape[0]
    expert_total = expert_router.shape[1]
    members = expert_total // group_router.shape[1]
    capacity = 4 * tokens // expert_total
    share = capacity // lax.axis_size("tp")
    group_logits = jnp.dot(normed_b, group_router, preferred_element_type=jnp.float32)
    expert_logits = jnp.dot(normed_b, expert_router, preferred_element_type=jnp.float32)
    expert_ids = jnp.arange(expert_total, dtype=jnp.int32)
    group_ids = jnp.arange(group_router.shape[1], dtype=jnp.int32)
    named = [routes[:, k : k + 1] == expert_ids[None, :] for k in range(2)]
    chosen = [jnp.sum(jnp.where(m, expert_logits, 0.0), axis=1, keepdims=True) for m in named]
    combine = jnp.zeros((tokens, expert_total), jnp.float32)
    for k in range(2):
        in_group = routes[:, k : k + 1] // members == group_ids[None, :]
        group_pick = jnp.sum(jnp.where(in_group, group_logits, 0.0), axis=1, keepdims=True)
        weight = jax.nn.sigmoid(group_pick) * jax.nn.sigmoid(chosen[k] - chosen[1 - k])
        combine = combine + jnp.where(named[k], weight, 0.0)
    matches = named[0] | named[1]
    earlier = jnp.tril(jnp.ones((tokens, tokens), jnp.bfloat16), -1)
    rank = jnp.dot(
        earlier, matches.astype(jnp.bfloat16), preferred_element_type=jnp.float32
    ).astype(jnp.int32)
    rank = jnp.where(matches, rank, -1)
    slots = jnp.arange(capacity, dtype=jnp.int32)
    mix = jnp.where(
        rank[:, :, None] == slots[None, None, :], combine[:, :, None], 0.0
    ).reshape(tokens, expert_total * capacity)
    own_slots = lax.axis_index("tp") * share + jnp.arange(share, dtype=jnp.int32)
    select = (rank.T[:, None, :] == own_slots[None, :, None]).astype(jnp.bfloat16)
    own_share = (
        jnp.dot(
            select.reshape(expert_total * share, tokens),
            normed_b,
            preferred_element_type=jnp.float32,
        )
        .astype(jnp.bfloat16)
        .reshape(expert_total, share, normed_b.shape[1])
    )
    normed_a = rms_rows(mixer_in, mixer_gain).astype(jnp.bfloat16)
    prepared = mixer_prepare(
        normed_a, query_weight, key_weight, value_weight, input_gate, forget_gate
    )
    width_local = query_weight.shape[1]
    gain_local = lax.dynamic_slice_in_dim(
        head_gain, lax.axis_index("tp") * width_local, width_local
    ).reshape(input_gate.shape[0], -1)
    experts = (own_share, gate_experts[0], up_experts[0], down_experts[0], mix)
    partial = mixer_partial(prepared, gain_local, mixer_out_weight)
    mixer_out = lax.psum_scatter(partial, "tp", scatter_dimension=0, tiled=True)
    expert_out = experts_plain(*experts)
    return (mixer_out, expert_out)


def solution(mesh):
    in_specs = (
        P("ep", None),
        P(),
        P(None, "tp"),
        P(None, "tp"),
        P(None, "tp"),
        P("tp", "ep"),
        P("tp", "ep"),
        P(),
        P("tp", None),
        P("ep", None),
        P(),
        P(),
        P(),
        P("ep", None),
        P("ep", None, "tp"),
        P("ep", None, "tp"),
        P("ep", "tp", None),
    )
    out_specs = (P(("ep", "tp"), None), P("ep", "tp"))
    return jax.shard_map(shards, mesh=mesh, in_specs=in_specs, out_specs=out_specs, check_vma=False)
```

```python
import functools

import jax
import jax.numpy as jnp
from jax import lax
from jax.experimental import pallas as pl
from jax.experimental.pallas import tpu as pltpu
from jax.sharding import PartitionSpec as P

MESH = pl.DeviceIdType.MESH


epsilon = 1e-06
highest = lax.Precision.HIGHEST
floor_log = -1e30


def is_power(count):
    return count & (count - 1) == 0


def rms_rows(matrix, gain):
    widened = matrix.astype(jnp.float32)
    scaled = widened * lax.rsqrt(jnp.mean(widened * widened, axis=-1, keepdims=True) + epsilon)
    return scaled * gain


def merged(earlier_memory, earlier_peak, later_memory, later_peak, later_total):
    moved = later_total + earlier_peak
    peak = jnp.maximum(moved, later_peak)
    return jnp.exp(moved - peak) * earlier_memory + jnp.exp(later_peak - peak) * later_memory, peak


def three_parts(matrix):
    parts = []
    for _ in range(3):
        top_part = matrix.astype(jnp.bfloat16)
        parts.append(top_part)
        matrix = matrix - top_part.astype(jnp.float32)
    return parts


nn = (((1,), (0,)), ((), ()))
nt = (((1,), (1,)), ((), ()))
tn = (((0,), (0,)), ((), ()))


def product(left, right, numbers):
    return lax.dot_general(left, right, numbers, preferred_element_type=jnp.float32)


def normalize(source, gain_ref, target):
    block = 64

    def body(b, carry):
        place = pl.ds(pl.multiple_of(b * block, block), block)
        widened = source[place, :].astype(jnp.float32)
        mean = jnp.mean(widened * widened, axis=-1, keepdims=True)
        factor = lax.rsqrt(mean + epsilon)
        target[place, :] = (source[place, :].astype(jnp.float32) * factor * gain_ref[...]).astype(
            target.dtype
        )
        return carry

    lax.fori_loop(0, source.shape[0] // block, body, 0)


def whole_kernel(
    sizes, mixer_hbm, expert_hbm, query_hbm, key_hbm, value_hbm, project_hbm, gate_hbm, up_hbm, down_hbm,
    mixer_gain_ref, expert_gain_ref, head_gain_ref, in_ref, forget_ref,
    group_router_ref, expert_router_ref, routes_ref,
    out_ref, mixed_ref,
    mixer_in, expert_in, query_w, key_w, value_w, project_ref, gate_ref, up_ref, down_ref,
    normed_a, normed_b, rank, rank_in, combine, near_rows, fwd, mine_b, entry_in,
    query_ref, key_ref, value_ref, cum_ref, cum_col_ref, packed_ref, acc,
    rows, part, pin, csum, xin, fin, ret,
    peer, plane, mem, pre, pre_in, state, state_peak, state_parts, mpart, mpin, msum, mxin,
    own_sem, send_a, recv_a, send_x, recv_x, send_p, recv_p,
    send_q, recv_q, send_c, recv_c, send_r, recv_r,
    send_m, recv_m, send_k, recv_k, send_h, recv_h, send_y, recv_y,
):
    n, share, cap, width, quarter, heads, size = sizes
    near = n // 2
    planes = n // 2
    me, tp = lax.axis_index("ep"), lax.axis_index("tp")
    core, column = lax.rem(tp, 2), lax.div(tp, 2)
    pair = tp + 1 - 2 * core
    cross = lax.rem(tp + 2, 4)
    pair_cross = lax.rem(pair + 2, 4)
    side, level = lax.rem(me, 2), lax.div(me, 2)
    mate = me + 1 - 2 * side
    tokens = expert_in.shape[0]
    length = mixer_in.shape[0]
    chunk = length // 4
    scale = size ** (-0.5)

    def other(i):
        total, bit = 0, 1
        while bit < n:
            total = total + bit * lax.rem(lax.div(me, bit) + lax.div(i, bit), 2)
            bit *= 2
        return total

    def far_turn(k):
        return near + (near // 2) * lax.rem(k, 2) + lax.div(k, 2)

    order = [(False, 0), (False, 1)] + [(False, k) for k in range(2, near - 1)]
    order += [(True, k) for k in range(near)]
    order += [(False, near - 1)] * (near > 2)

    def turn(t):
        total = 0
        for place, (far, k) in enumerate(order):
            total = total + jnp.where(t == place, far_turn(k) if far else k, 0)
        return total

    def is_far(t):
        total = t < 0
        for place, (far, k) in enumerate(order):
            total = total | (t == place) if far else total
        return total

    def remote(src, dst, send, recv, to):
        return pltpu.make_async_remote_copy(
            src_ref=src, dst_ref=dst, send_sem=send, recv_sem=recv, device_id=to, device_id_type=MESH
        )

    barrier = pltpu.get_barrier_semaphore()
    for i in range(1, n):
        pl.semaphore_signal(
            barrier, inc=1, device_id=(lax.rem(me + i, n), tp), device_id_type=MESH
        )
    pl.semaphore_signal(barrier, inc=1, device_id=(me, pair), device_id_type=MESH)
    pl.semaphore_signal(barrier, inc=1, device_id=(me, cross), device_id_type=MESH)

    loads = [
        pltpu.make_async_copy(src, dst, own_sem.at[k])
        for k, (src, dst) in enumerate(
            [
                (expert_hbm, expert_in), (gate_hbm, gate_ref), (up_hbm, up_ref),
                (down_hbm, down_ref), (mixer_hbm, mixer_in), (key_hbm, key_w),
                (value_hbm, value_w), (query_hbm, query_w), (project_hbm, project_ref),
            ]
        )
    ]
    for load in loads:
        load.start()

    def scatter_near(i, place):
        slot = jnp.maximum(i - 1, 0)
        return remote(
            near_rows.at[slot], rows.at[place, core], send_a.at[i], recv_a.at[i], (other(i), tp)
        )

    def entry():
        return remote(mine_b, entry_in, send_a.at[0], recv_a.at[0], (other(near), tp))

    def entry_rank():
        return remote(rank, rank_in, send_a.at[near], recv_a.at[near], (other(near), tp))

    def forward(j):
        return remote(
            fwd.at[j], rows.at[other(near), core, column],
            send_a.at[near + j], recv_a.at[near + j], (other(j), tp),
        )

    def arrival(i, s):
        return remote(
            fwd.at[i - near], rows.at[s, core, column], send_a.at[i], recv_a.at[i],
            (other(i - near), tp),
        )

    def across(s, which):
        return remote(
            rows.at[s, core, which], rows.at[s, core, which],
            send_x.at[s], recv_x.at[s], (me, cross),
        )

    def beside(s, which):
        return remote(
            rows.at[s, which], rows.at[s, which], send_p.at[s], recv_p.at[s], (me, pair)
        )

    def halves(s, k, who):
        return remote(part.at[s, who], pin.at[s, k], send_q.at[s, k], recv_q.at[s, k], (me, pair))

    def summed(s):
        return remote(csum.at[s], xin.at[s], send_c.at[s], recv_c.at[s], (me, cross))

    def back(i):
        to = other(i)
        return remote(fin.at[to], ret.at[me], send_r.at[i], recv_r.at[i], (to, tp))

    def to_mate():
        return remote(
            packed_ref.at[1 - side], peer.at[1 - side], send_k.at[0], recv_k.at[0], (mate, tp)
        )

    def from_mate():
        return remote(packed_ref.at[side], peer.at[side], send_k.at[0], recv_k.at[0], (mate, tp))

    def rest_to_mate():
        return remote(packed_ref.at[0], peer.at[0], send_k.at[2], recv_k.at[2], (mate, tp))

    def to_level(d):
        return remote(
            plane, mem.at[level], send_m.at[d], recv_m.at[d], (lax.rem(me + 2 * d, n), tp)
        )

    def from_level(d):
        return remote(
            plane, mem.at[level - d], send_m.at[d], recv_m.at[d], (lax.rem(me + 2 * d, n), tp)
        )

    def prefix_mate():
        return remote(pre, pre_in, send_k.at[1], recv_k.at[1], (mate, tp))

    def mixed_half(k, who):
        return remote(mpart.at[who], mpin.at[k], send_h.at[k], recv_h.at[k], (me, pair))

    def mixed_sum(q):
        return remote(msum.at[q], mxin.at[q], send_y.at[q], recv_y.at[q], (me, cross))

    body, top_row, sum_row = slice(0, size), slice(size, size + 1), slice(size + 1, size + 2)

    def picks(table, e):
        slots = lax.broadcasted_iota(jnp.int32, (cap, tokens), 0)
        return table[pl.ds(e, 1), :] == slots.astype(jnp.float32)

    def selection(table, experts):
        return jnp.concatenate(
            [jnp.where(picks(table, e), 1.0, 0.0).astype(jnp.bfloat16) for e in experts], axis=0
        )

    def features(q):
        return pl.ds(pl.multiple_of(q * quarter, quarter), quarter)

    def prepare_rank():
        experts = lax.broadcasted_iota(jnp.int32, (n, tokens), 0)
        matches = (routes_ref[0:1, :] == experts) | (routes_ref[1:2, :] == experts)
        earlier = lax.broadcasted_iota(jnp.int32, (tokens, tokens), 0)
        earlier = earlier < lax.broadcasted_iota(jnp.int32, (tokens, tokens), 1)
        count = product(
            jnp.where(matches, 1.0, 0.0).astype(jnp.bfloat16),
            jnp.where(earlier, 1.0, 0.0).astype(jnp.bfloat16),
            nn,
        )
        rank[...] = jnp.where(matches, count, -1.0)

    def prepare_combine():
        experts = lax.broadcasted_iota(jnp.int32, (n, tokens), 0)
        groups = group_router_ref.shape[0]
        expert_logits = product(expert_router_ref[...], normed_b[...], nt)
        group_logits = product(group_router_ref[...], normed_b[...], nt)
        group_full = jnp.zeros((n, tokens), jnp.float32)
        for g in range(groups):
            inside = (experts >= g * (n // groups)) & (experts < (g + 1) * (n // groups))
            group_full = group_full + jnp.where(inside, group_logits[g : g + 1, :], 0.0)
        named = [routes_ref[k : k + 1, :] == experts for k in range(2)]
        chosen = [jnp.sum(jnp.where(m, expert_logits, 0.0), axis=0, keepdims=True) for m in named]
        total = jnp.zeros((n, tokens), jnp.float32)
        for k in range(2):
            group_pick = jnp.sum(jnp.where(named[k], group_full, 0.0), axis=0, keepdims=True)
            weight = jax.nn.sigmoid(group_pick) * jax.nn.sigmoid(chosen[k] - chosen[1 - k])
            total = total + jnp.where(named[k], weight, 0.0)
        combine[...] = total

    def prepare_near():
        select = selection(rank, [other(i) for i in range(1, near)])
        for c in range(2):
            moved = product(select, normed_b[:, features(2 * c + core)], nn).astype(jnp.bfloat16)
            for i in range(1, near):
                near_rows[i - 1, c] = moved[(i - 1) * cap : i * cap]

    def prepare_own():
        moved = product(selection(rank, [me]), normed_b[...], nn).astype(jnp.bfloat16)
        for q in range(4):
            rows[me, q % 2, q // 2] = moved[:, q * quarter : (q + 1) * quarter]

    def redistribute():
        entry_rank().wait_recv()
        entry().wait_recv()
        select = selection(rank_in, [other(j) for j in range(near)])
        moved = product(select, entry_in[...], nn).astype(jnp.bfloat16)
        for j in range(1, near):
            fwd[j] = moved[j * cap : (j + 1) * cap]
        rows[other(near), core, column] = moved[0:cap]
        for j in range(1, near):
            forward(j).start()

    def ffn(s):
        x = jnp.concatenate([rows[s, q % 2, q // 2] for q in range(4)], axis=1)
        gate_act = jnp.dot(x, gate_ref[...], preferred_element_type=jnp.float32)
        up_act = jnp.dot(x, up_ref[...], preferred_element_type=jnp.float32)
        hidden = (gate_act * jax.nn.sigmoid(gate_act) * up_act).astype(jnp.bfloat16)
        for q in range(4):
            part[s, q] = jnp.dot(
                hidden,
                down_ref[:, q * quarter : (q + 1) * quarter],
                preferred_element_type=jnp.float32,
            ).astype(jnp.bfloat16)

    def prepare_gates():
        log_forget = jnp.minimum(forget_ref[...], 0.0) - jnp.log1p(jnp.exp(-jnp.abs(forget_ref[...])))
        pieces = jnp.concatenate(
            [p.astype(jnp.float32) for p in three_parts(log_forget)]
            + [jnp.zeros((16 - 3 * heads, length), jnp.float32)],
            axis=0,
        ).astype(jnp.bfloat16)
        first = lax.broadcasted_iota(jnp.int32, (length, length), 0)
        upto = first <= lax.broadcasted_iota(jnp.int32, (length, length), 1)
        sums = product(pieces, jnp.where(upto, 1.0, 0.0).astype(jnp.bfloat16), nn)
        cum_ref[...] = sums[2 * heads : 3 * heads] + sums[heads : 2 * heads] + sums[0:heads]
        back_to = first >= lax.broadcasted_iota(jnp.int32, (length, length), 1)
        sums = product(jnp.where(back_to, 1.0, 0.0).astype(jnp.bfloat16), pieces, nt)
        cum_col_ref[...] = (
            sums[:, 2 * heads : 3 * heads] + sums[:, heads : 2 * heads] + sums[:, 0:heads]
        )

    def prepare_memory():
        key_ref[...] = jnp.dot(
            normed_a[...], key_w[...], preferred_element_type=jnp.float32
        ).astype(jnp.bfloat16)
        value_ref[...] = jnp.dot(
            normed_a[...], value_w[...], preferred_element_type=jnp.float32
        ).astype(jnp.bfloat16)
        for h in range(heads):
            cols = slice(h * size, (h + 1) * size)
            cum = cum_ref[h : h + 1, :]
            total = cum_ref[h : h + 1, length - 1 : length]
            log_weight = total - cum + in_ref[h : h + 1, :]
            peak = jnp.max(log_weight, axis=1, keepdims=True)
            weighted = value_ref[:, cols].astype(jnp.float32).T * jnp.exp(log_weight - peak)
            memory = jnp.zeros((size, size), jnp.float32)
            for piece in three_parts(weighted)[::-1]:
                memory = memory + product(piece, key_ref[:, cols], nn)
            packed_ref[h, body] = memory * scale
            packed_ref[h, size : size + 8] = jnp.zeros((8, size), jnp.float32)
            packed_ref[h, top_row] = jnp.broadcast_to(peak, (1, size))
            packed_ref[h, sum_row] = jnp.broadcast_to(total, (1, size))

    def prepare_query():
        query_ref[...] = jnp.dot(
            normed_a[...], query_w[...], preferred_element_type=jnp.float32
        ).astype(jnp.bfloat16)

    def combine_plane():
        from_mate().wait_recv()

        def joined(first, second):
            memory, peak = merged(
                first[side, body], first[side, top_row],
                second[side, body], second[side, top_row], second[side, sum_row],
            )
            plane[size : size + 8] = jnp.zeros((8, size), jnp.float32)
            plane[body] = memory
            plane[top_row] = peak
            plane[sum_row] = first[side, sum_row] + second[side, sum_row]

        @pl.when(side == 0)
        def _():
            joined(packed_ref, peer)

        @pl.when(side == 1)
        def _():
            joined(peer, packed_ref)

        for d in range(1, planes):
            @pl.when(level + d < planes)
            def _():
                to_level(d).start()

    def combine_levels():
        pre[...] = jnp.zeros_like(pre)
        pre[top_row] = jnp.full((1, size), floor_log, jnp.float32)
        for k in range(planes - 1):
            d = planes - 1 - k

            @pl.when(d <= level)
            def _():
                from_level(d).wait_recv()
                z = level - d
                memory, peak = merged(
                    pre[body], pre[top_row], mem[z, body], mem[z, top_row], mem[z, sum_row]
                )
                pre[body] = memory
                pre[top_row] = peak

        prefix_mate().start()

    def combine_last():
        prefix_mate().wait_recv()
        state[side] = pre[body]
        state_peak[side, 0:1, :] = pre[top_row]
        state[1 - side] = pre_in[body]
        state_peak[1 - side, 0:1, :] = pre_in[top_row]

        @pl.when(side == 1)
        def _():
            rest_to_mate().wait_recv()
            for h in range(heads):
                memory, peak = merged(
                    state[h], state_peak[h, 0:1, :],
                    peer[h, body], peer[h, top_row], peer[h, sum_row],
                )
                state[h] = memory
                state_peak[h, 0:1, :] = peak

        for h in range(heads):
            for piece, value in enumerate(three_parts(state[h])):
                state_parts[h, piece] = value

    def attend(j):
        start = pl.multiple_of(j * chunk, chunk)
        row = start + lax.broadcasted_iota(jnp.int32, (chunk, length), 0)
        causal = row >= lax.broadcasted_iota(jnp.int32, (chunk, length), 1)
        cell_list = []
        for h in range(heads):
            cols = slice(h * size, (h + 1) * size)
            q = query_ref[pl.ds(start, chunk), cols]
            c = cum_col_ref[pl.ds(start, chunk), h : h + 1]
            within = jnp.where(causal, c - cum_ref[h : h + 1, :] + in_ref[h : h + 1, :], -jnp.inf)
            carried = c + state_peak[h, 0:1, 0:1]
            top = jnp.maximum(jnp.max(within, axis=1, keepdims=True), carried)
            raw = product(q, key_ref[:, cols], nt)
            scores = (raw * scale * jnp.exp(within - top)).astype(jnp.bfloat16)
            cells = jnp.dot(scores, value_ref[:, cols], preferred_element_type=jnp.float32)
            held = jnp.zeros((chunk, size), jnp.float32)
            for piece in (2, 1, 0):
                held = held + product(q, state_parts[h, piece], nt)
            cells = cells + jnp.exp(carried - top) * held
            mean = jnp.mean(cells * cells, axis=1, keepdims=True)
            gain = head_gain_ref[pl.ds(tp * heads + h, 1), :]
            cell_list.append((cells * lax.rsqrt(mean + epsilon) * gain).astype(jnp.bfloat16))
        cell_rows = jnp.concatenate(cell_list, axis=1)
        for q in range(4):
            cols = slice(q * quarter, (q + 1) * quarter)
            mpart[j, q] = jnp.dot(
                cell_rows, project_ref[:, cols], preferred_element_type=jnp.float32
            ).astype(jnp.bfloat16)

    begin = n - 1

    def mixer_levels(t):
        @pl.when(t == 4)
        def _():
            combine_levels()

    def mixer_first(t):
        @pl.when(t == n + 1)
        def _():
            combine_last()

            def one(k, carry):
                attend(jnp.where(k == 0, pair_cross, cross))

                @pl.when(k == 0)
                def _():
                    mixed_half(1, pair_cross).start()

                return carry

            lax.fori_loop(0, 2, one, 0)
            mixed_half(1, pair_cross).wait_recv()
            for q in range(4):
                msum[q] = (
                    mpart[cross, q].astype(jnp.float32) + mpin[1, q].astype(jnp.float32)
                ).astype(jnp.bfloat16)
            for q in range(4):
                mixed_sum(q).start()

    def mixer_late(t):
        @pl.when(t == n + 2)
        def _():
            def one(k, carry):
                attend(jnp.where(k == 0, pair, tp))

                @pl.when(k == 0)
                def _():
                    mixed_half(0, pair).start()

                return carry

            lax.fori_loop(0, 2, one, 0)

    def collect(s):
        halves(s, 1, pair_cross).wait_recv()
        csum[s] = (
            part[s, cross].astype(jnp.float32) + pin[s, 1].astype(jnp.float32)
        ).astype(jnp.bfloat16)
        summed(s).start()

    def send_halves(s):
        halves(s, 1, pair_cross).start()
        halves(s, 0, pair).start()

    prepare_rank()
    loads[0].wait()
    normalize(expert_in, expert_gain_ref, normed_b)
    mine_b[...] = normed_b[:, features(tp)]
    prepare_near()
    pl.semaphore_wait(barrier, n + 1)
    entry_rank().start()
    entry().start()
    scatter_near(1, me).start()
    prepare_own()
    for k in (1, 2, 3):
        loads[k].wait()
    ffn(me)
    send_halves(me)
    for i in range(2, near - 1):
        scatter_near(i, me).start()
    loads[4].wait()
    normalize(mixer_in, mixer_gain_ref, normed_a)
    collect(me)
    prepare_gates()
    loads[5].wait()
    loads[6].wait()
    prepare_memory()
    to_mate().start()
    loads[7].wait()
    prepare_query()
    prepare_combine()
    loads[8].wait()

    def finish(t, carry):
        i = turn(t)
        s = other(i)

        @pl.when(t > 0)
        def _():
            back(i).wait_recv()

        chosen = picks(rank, s)
        weight = combine[pl.ds(s, 1), :]
        high_weight = weight.astype(jnp.bfloat16).astype(jnp.float32)
        table = ret[s]
        acc[...] += product(
            jnp.where(chosen, high_weight, 0.0).astype(jnp.bfloat16), table, tn
        ) + product(jnp.where(chosen, weight - high_weight, 0.0).astype(jnp.bfloat16), table, tn)
        return carry

    acc[...] = jnp.zeros_like(acc)

    collects = {2: (1, 2), n + 1: (n - 2, n)}
    late_collects = {n - 1: (n - 3, n - 2)}
    collects.update({t: (t - 2, t - 1) for t in range(4, n - 1)})
    delivers = {n + 1: (n - 3, n - 2), n + 2: (n - 2, n - 1), n + 3: (n - 1, n)}
    delivers.update({t: (t - 3, t - 2) for t in range(3, n)})

    def span(table, t):
        low = sum(jnp.where(t == k, v[0], 0) for k, v in sorted(table.items()))
        return low, sum(jnp.where(t == k, v[1], 0) for k, v in sorted(table.items()))

    def step(t, carry):
        working = (t == 2) | ((t > 3) & (t < n + 2))
        now = jnp.where(t == 2, 1, t - 2)

        @pl.when(working)
        def _():
            s = other(turn(now))
            beside(s, 1 - core).wait_recv()
            ffn(s)
            send_halves(s)

        def gather(place, carry):
            collect(other(turn(place)))
            return carry

        lax.fori_loop(*span(collects, t), gather, 0)

        @pl.when(t == 2)
        def _():
            redistribute()

        @pl.when(t == 4)
        def _():
            if near > 2:
                scatter_near(near - 1, me).start()

        def arrive(place, carry):
            i = turn(place)
            s = other(i)

            @pl.when(is_far(place))
            def _():
                @pl.when(i > near)
                def _():
                    arrival(i, s).wait_recv()

                across(s, column).start()

            @pl.when(jnp.logical_not(is_far(place)))
            def _():
                scatter_near(i, s).wait_recv()
                beside(s, core).start()

            return carry

        begins = jnp.where(t > near + 1, jnp.where(t == n - 1, n - 1, n), t)
        ends = jnp.where(t == near + 1, t + 2, t + 1)
        lax.fori_loop(jnp.minimum(begins, n), jnp.minimum(ends, n), arrive, 0)

        @pl.when(t == 1)
        def _():
            combine_plane()

            @pl.when(side == 0)
            def _():
                rest_to_mate().start()

        @pl.when(is_far(t - 1))
        def _():
            s = other(turn(t - 1))
            across(s, 1 - column).wait_recv()
            beside(s, core).start()

        lax.fori_loop(*span(late_collects, t), gather, 0)
        mixer_first(t)

        @pl.when(t == n + 3)
        def _():
            lax.fori_loop(0, n - 3, finish, 0)

        def deliver(place, carry):
            i = turn(place)
            s = other(i)
            halves(s, 0, pair).wait_recv()
            summed(s).wait_recv()
            total = (
                part[s, tp].astype(jnp.float32)
                + pin[s, 0].astype(jnp.float32)
                + xin[s].astype(jnp.float32)
            ).astype(jnp.bfloat16)

            @pl.when(i > 0)
            def _():
                fin[s] = total
                back(i).start()

            @pl.when(i == 0)
            def _():
                ret[s] = total

            return carry

        lax.fori_loop(*span(delivers, t), deliver, 0)
        mixer_levels(t)
        mixer_late(t)
        return carry

    lax.fori_loop(1, n + 4, step, 0)

    lax.fori_loop(n - 3, n, finish, 0)
    out_ref[...] = acc[...].astype(out_ref.dtype)
    mixed_half(0, pair).wait_recv()
    for q in range(4):
        mixed_sum(q).wait_recv()
        cols = slice(q * quarter, (q + 1) * quarter)
        mixed_ref[:, cols] = (
            mpart[tp, q].astype(jnp.float32)
            + mpin[0, q].astype(jnp.float32)
            + mxin[q].astype(jnp.float32)
        ).astype(mixed_ref.dtype)

    def drain(i, carry):
        s = other(i)
        halves(s, 0, pair).wait_send()
        halves(s, 1, pair_cross).wait_send()
        summed(s).wait_send()

        @pl.when(i > 0)
        def _():
            beside(s, core).wait_send()
            back(i).wait_send()

        @pl.when((i > 0) & (i < near))
        def _():
            scatter_near(i, me).wait_send()

        @pl.when(i >= near)
        def _():
            across(s, column).wait_send()
            @pl.when(i > near)
            def _():
                forward(i - near).wait_send()

        return carry

    lax.fori_loop(0, n, drain, 0)
    entry().wait_send()
    entry_rank().wait_send()
    to_mate().wait_send()

    @pl.when(side == 0)
    def _():
        rest_to_mate().wait_send()

    prefix_mate().wait_send()
    for d in range(1, planes):
        @pl.when(level + d < planes)
        def _():
            to_level(d).wait_send()
    mixed_half(0, pair).wait_send()
    mixed_half(1, pair_cross).wait_send()
    for q in range(4):
        mixed_sum(q).wait_send()


def hand_over(first_ref, second_ref, first_out, second_out):
    first_out[...] = first_ref[...]
    second_out[...] = second_ref[...]


def all_fused(
    mixer_in, mixer_gain, query_weight, key_weight, value_weight, input_gate, forget_gate,
    head_gain, mixer_out_weight, expert_in, expert_gain, group_router, expert_router, routes,
    gate_weight, up_weight, down_weight,
):
    n = expert_router.shape[1]
    tokens, width = expert_in.shape
    cap = 4 * tokens // n
    share = cap // 4
    quarter = width // 4
    length = mixer_in.shape[0]
    heads = input_gate.shape[0]
    inner_width = query_weight.shape[1]
    size = inner_width // heads
    hidden = gate_weight.shape[1]
    chunk = length // 4
    vmem = pl.BlockSpec(memory_space=pltpu.VMEM)
    whole = pl.BlockSpec(memory_space=pl.ANY)
    dma = pltpu.SemaphoreType.DMA
    bf = jnp.bfloat16
    f32 = jnp.float32
    results = pl.pallas_call(
        functools.partial(whole_kernel, (n, share, cap, width, quarter, heads, size)),
        out_shape=(
            jax.ShapeDtypeStruct((tokens, quarter), bf),
            jax.ShapeDtypeStruct((chunk, width), bf),
        ),
        in_specs=[whole] * 9 + [vmem] * 8,
        out_specs=(vmem, vmem),
        scratch_shapes=[
            pltpu.VMEM((length, width), bf),
            pltpu.VMEM((tokens, width), bf),
            pltpu.VMEM((width, inner_width), bf),
            pltpu.VMEM((width, inner_width), bf),
            pltpu.VMEM((width, inner_width), bf),
            pltpu.VMEM((inner_width, width), bf),
            pltpu.VMEM((width, hidden), bf),
            pltpu.VMEM((width, hidden), bf),
            pltpu.VMEM((hidden, width), bf),
            pltpu.VMEM((length, width), bf),
            pltpu.VMEM((tokens, width), bf),
            pltpu.VMEM((n, tokens), f32),
            pltpu.VMEM((n, tokens), f32),
            pltpu.VMEM((n, tokens), f32),
            pltpu.VMEM((n // 2 - 1, 2, cap, quarter), bf),
            pltpu.VMEM((n // 2, cap, quarter), bf),
            pltpu.VMEM((tokens, quarter), bf),
            pltpu.VMEM((tokens, quarter), bf),
            pltpu.VMEM((length, inner_width), bf),
            pltpu.VMEM((length, inner_width), bf),
            pltpu.VMEM((length, inner_width), bf),
            pltpu.VMEM((heads, length), f32),
            pltpu.VMEM((length, heads), f32),
            pltpu.VMEM((heads, size + 8, size), f32),
            pltpu.VMEM((tokens, quarter), f32),
            pltpu.VMEM((n, 2, 2, cap, quarter), bf),
            pltpu.VMEM((n, 4, cap, quarter), bf),
            pltpu.VMEM((n, 2, cap, quarter), bf),
            pltpu.VMEM((n, cap, quarter), bf),
            pltpu.VMEM((n, cap, quarter), bf),
            pltpu.VMEM((n, cap, quarter), bf),
            pltpu.VMEM((n, cap, quarter), bf),
            pltpu.VMEM((heads, size + 8, size), f32),
            pltpu.VMEM((size + 8, size), f32),
            pltpu.VMEM((n // 2, size + 8, size), f32),
            pltpu.VMEM((size + 8, size), f32),
            pltpu.VMEM((size + 8, size), f32),
            pltpu.VMEM((heads, size, size), f32),
            pltpu.VMEM((heads, 8, size), f32),
            pltpu.VMEM((heads, 3, size, size), bf),
            pltpu.VMEM((4, 4, chunk, quarter), bf),
            pltpu.VMEM((2, 4, chunk, quarter), bf),
            pltpu.VMEM((4, chunk, quarter), bf),
            pltpu.VMEM((4, chunk, quarter), bf),
            dma((9,)),
            dma((n,)), dma((n,)), dma((n,)), dma((n,)), dma((n,)), dma((n,)),
            dma((n, 2)), dma((n, 2)), dma((n,)), dma((n,)), dma((n,)), dma((n,)),
            dma((n // 2,)), dma((n // 2,)), dma((3,)), dma((3,)), dma((2,)), dma((2,)),
            dma((4,)), dma((4,)),
        ],
        compiler_params=pltpu.CompilerParams(
            collective_id=0, has_side_effects=True, vmem_limit_bytes=60 * 1024 * 1024
        ),
        cost_estimate=pl.CostEstimate(
            flops=60_000_000_000, bytes_accessed=8_000_000, transcendentals=0
        ),
    )(
        mixer_in, expert_in, query_weight, key_weight, value_weight, mixer_out_weight,
        gate_weight, up_weight, down_weight,
        mixer_gain.reshape(1, width), expert_gain.reshape(1, width),
        head_gain.reshape(-1, size), input_gate, forget_gate,
        group_router.T, expert_router.T, routes.T,
    )
    return pl.pallas_call(
        hand_over,
        out_shape=tuple(jax.ShapeDtypeStruct(r.shape, r.dtype) for r in results),
        in_specs=[vmem, vmem],
        out_specs=(vmem, vmem),
        compiler_params=pltpu.CompilerParams(vmem_limit_bytes=60 * 1024 * 1024),
    )(*results)


def experts_plain(own_share, gate_weight, up_weight, down_weight, mix):
    arrived = lax.all_to_all(own_share, "ep", split_axis=0, concat_axis=0, tiled=True)
    piece_rows = lax.all_gather(arrived, "tp", axis=1, tiled=True)
    gate_act = jnp.einsum(
        "scd,df->scf", piece_rows, gate_weight, preferred_element_type=jnp.float32
    )
    up_act = jnp.einsum("scd,df->scf", piece_rows, up_weight, preferred_element_type=jnp.float32)
    hidden = (jax.nn.silu(gate_act) * up_act).astype(jnp.bfloat16)
    partial_rows = jnp.einsum(
        "scf,fo->sco", hidden, down_weight, preferred_element_type=jnp.float32
    )
    summed = lax.psum_scatter(
        partial_rows.astype(jnp.bfloat16), "tp", scatter_dimension=2, tiled=True
    )
    returned = lax.all_to_all(summed, "ep", split_axis=0, concat_axis=0, tiled=True)
    return jnp.dot(
        mix, returned.reshape(-1, returned.shape[2]).astype(jnp.float32), precision=highest
    ).astype(jnp.bfloat16)


def mixer_prepare(normed_a, query_weight, key_weight, value_weight, input_gate, forget_gate):
    def project(weight):
        return jnp.dot(normed_a, weight, preferred_element_type=jnp.float32).astype(jnp.bfloat16)

    rows = normed_a.shape[0]
    heads = input_gate.shape[0]
    width_local = query_weight.shape[1]
    head_size = width_local // heads
    scale = head_size ** (-0.5)
    causal = jnp.tril(jnp.ones((rows, rows), dtype=bool))
    log_forget = jax.nn.log_sigmoid(forget_gate)
    cumulative = jnp.einsum(
        "hs,ts->ht", log_forget, causal.astype(jnp.float32), precision=highest
    )
    total = cumulative[:, -1]
    log_weight = total[:, None] - cumulative + input_gate
    peak = jnp.max(log_weight, axis=-1)
    weights = jnp.exp(log_weight - peak[:, None])
    keys = project(key_weight)
    values = project(value_weight)

    def by_head(matrix):
        return [matrix[:, h * head_size : (h + 1) * head_size] for h in range(heads)]

    key_heads, value_heads = by_head(keys), by_head(values)
    memory = jnp.stack(
        [
            lax.dot_general(
                value_heads[h].astype(jnp.float32) * weights[h][:, None],
                key_heads[h].astype(jnp.float32) * scale,
                (((0,), (0,)), ((), ())),
                precision=highest,
            )
            for h in range(heads)
        ]
    )
    stats = jnp.stack([peak, total], axis=1)
    stats = jnp.concatenate([stats, jnp.zeros((heads, 6), jnp.float32)], axis=1)
    packed = jnp.concatenate(
        [memory, jnp.broadcast_to(stats[:, :, None], (heads, 8, head_size))], axis=1
    )
    return (packed, project(query_weight), keys, values, cumulative, input_gate)


def mixer_partial(prepared, gain_local, mixer_out_weight):
    packed, queries, keys, values, cumulative, input_gate = prepared
    rows = queries.shape[0]
    heads, head_size = gain_local.shape
    scale = head_size ** (-0.5)
    causal = jnp.tril(jnp.ones((rows, rows), dtype=bool))

    def by_head(matrix):
        return [matrix[:, h * head_size : (h + 1) * head_size] for h in range(heads)]

    query_heads, key_heads, value_heads = by_head(queries), by_head(keys), by_head(values)
    everything = lax.all_gather(packed, "ep")
    n, place = lax.axis_size("ep"), lax.axis_index("ep")
    peaks = everything[:, :, head_size, 0]
    totals = everything[:, :, head_size + 1, 0]
    order = jnp.arange(n)
    later = (order[None, :] > order[:, None]) & (order[None, :] < place)
    suffix = jnp.sum(jnp.where(later[:, :, None], totals[None], 0.0), axis=1)
    before = (order < place)[:, None]
    candidate = jnp.where(before, peaks + suffix, floor_log)
    state_peak = jnp.max(candidate, axis=0)
    fade = jnp.where(before, jnp.exp(candidate - state_peak[None]), 0.0)
    state = jnp.sum(everything[:, :, :head_size] * fade[:, :, None, None], axis=0)
    cell_list = []
    for h in range(heads):
        c, gate = cumulative[h], input_gate[h]
        within = jnp.where(causal, c[:, None] - c[None, :] + gate[None, :], -jnp.inf)
        carried = c + state_peak[h]
        top = jnp.maximum(jnp.max(within, axis=-1), carried)
        raw = lax.dot_general(
            query_heads[h], key_heads[h], (((1,), (1,)), ((), ())), preferred_element_type=jnp.float32
        )
        scores = raw * scale * jnp.exp(within - top[:, None])
        cells = jnp.dot(
            scores.astype(jnp.bfloat16), value_heads[h], preferred_element_type=jnp.float32
        )
        carried_cells = lax.dot_general(
            query_heads[h].astype(jnp.float32),
            state[h],
            (((1,), (1,)), ((), ())),
            precision=highest,
        )
        cells = cells + jnp.exp(carried - top)[:, None] * carried_cells
        cell_list.append(rms_rows(cells, gain_local[h]).astype(jnp.bfloat16))
    cell_rows = jnp.concatenate(cell_list, axis=1)
    return jnp.dot(cell_rows, mixer_out_weight, preferred_element_type=jnp.float32).astype(
        jnp.bfloat16
    )


def shards(
    mixer_in,
    mixer_gain,
    query_weight,
    key_weight,
    value_weight,
    input_gate,
    forget_gate,
    head_gain,
    mixer_out_weight,
    expert_in,
    expert_gain,
    group_router,
    expert_router,
    routes,
    gate_experts,
    up_experts,
    down_experts,
):
    ranks = lax.axis_size("ep")
    share = expert_in.shape[0] // expert_router.shape[1]
    fused = lax.axis_size("tp") == 4 and ranks >= 4 and is_power(ranks) and share % 16 == 0
    fused = fused and mixer_in.shape[0] % 512 == 0 and input_gate.shape[0] == 2
    fused = fused and gate_experts.shape[0] == 1
    if fused:
        expert_out, mixer_out = all_fused(
            mixer_in, mixer_gain, query_weight, key_weight, value_weight, input_gate, forget_gate,
            head_gain, mixer_out_weight, expert_in, expert_gain, group_router, expert_router,
            routes, gate_experts[0], up_experts[0], down_experts[0],
        )
        return (mixer_out, expert_out)
    normed_b = rms_rows(expert_in, expert_gain).astype(jnp.bfloat16)
    tokens = normed_b.shape[0]
    expert_total = expert_router.shape[1]
    members = expert_total // group_router.shape[1]
    capacity = 4 * tokens // expert_total
    share = capacity // lax.axis_size("tp")
    group_logits = jnp.dot(normed_b, group_router, preferred_element_type=jnp.float32)
    expert_logits = jnp.dot(normed_b, expert_router, preferred_element_type=jnp.float32)
    expert_ids = jnp.arange(expert_total, dtype=jnp.int32)
    group_ids = jnp.arange(group_router.shape[1], dtype=jnp.int32)
    named = [routes[:, k : k + 1] == expert_ids[None, :] for k in range(2)]
    chosen = [jnp.sum(jnp.where(m, expert_logits, 0.0), axis=1, keepdims=True) for m in named]
    combine = jnp.zeros((tokens, expert_total), jnp.float32)
    for k in range(2):
        in_group = routes[:, k : k + 1] // members == group_ids[None, :]
        group_pick = jnp.sum(jnp.where(in_group, group_logits, 0.0), axis=1, keepdims=True)
        weight = jax.nn.sigmoid(group_pick) * jax.nn.sigmoid(chosen[k] - chosen[1 - k])
        combine = combine + jnp.where(named[k], weight, 0.0)
    matches = named[0] | named[1]
    earlier = jnp.tril(jnp.ones((tokens, tokens), jnp.bfloat16), -1)
    rank = jnp.dot(
        earlier, matches.astype(jnp.bfloat16), preferred_element_type=jnp.float32
    ).astype(jnp.int32)
    rank = jnp.where(matches, rank, -1)
    slots = jnp.arange(capacity, dtype=jnp.int32)
    mix = jnp.where(
        rank[:, :, None] == slots[None, None, :], combine[:, :, None], 0.0
    ).reshape(tokens, expert_total * capacity)
    own_slots = lax.axis_index("tp") * share + jnp.arange(share, dtype=jnp.int32)
    select = (rank.T[:, None, :] == own_slots[None, :, None]).astype(jnp.bfloat16)
    own_share = (
        jnp.dot(
            select.reshape(expert_total * share, tokens),
            normed_b,
            preferred_element_type=jnp.float32,
        )
        .astype(jnp.bfloat16)
        .reshape(expert_total, share, normed_b.shape[1])
    )
    normed_a = rms_rows(mixer_in, mixer_gain).astype(jnp.bfloat16)
    prepared = mixer_prepare(
        normed_a, query_weight, key_weight, value_weight, input_gate, forget_gate
    )
    width_local = query_weight.shape[1]
    gain_local = lax.dynamic_slice_in_dim(
        head_gain, lax.axis_index("tp") * width_local, width_local
    ).reshape(input_gate.shape[0], -1)
    experts = (own_share, gate_experts[0], up_experts[0], down_experts[0], mix)
    partial = mixer_partial(prepared, gain_local, mixer_out_weight)
    mixer_out = lax.psum_scatter(partial, "tp", scatter_dimension=0, tiled=True)
    expert_out = experts_plain(*experts)
    return (mixer_out, expert_out)


def solution(mesh):
    in_specs = (
        P("ep", None),
        P(),
        P(None, "tp"),
        P(None, "tp"),
        P(None, "tp"),
        P("tp", "ep"),
        P("tp", "ep"),
        P(),
        P("tp", None),
        P("ep", None),
        P(),
        P(),
        P(),
        P("ep", None),
        P("ep", None, "tp"),
        P("ep", None, "tp"),
        P("ep", "tp", None),
    )
    out_specs = (P(("ep", "tp"), None), P("ep", "tp"))
    return jax.shard_map(shards, mesh=mesh, in_specs=in_specs, out_specs=out_specs, check_vma=False)
```

```python
import functools

import jax
import jax.numpy as jnp
from jax import lax
from jax.experimental import pallas as pl
from jax.experimental.pallas import tpu as pltpu
from jax.sharding import PartitionSpec as P

MESH = pl.DeviceIdType.MESH


epsilon = 1e-06
highest = lax.Precision.HIGHEST
floor_log = -1e30


def is_power(count):
    return count & (count - 1) == 0


def rms_rows(matrix, gain):
    widened = matrix.astype(jnp.float32)
    scaled = widened * lax.rsqrt(jnp.mean(widened * widened, axis=-1, keepdims=True) + epsilon)
    return scaled * gain


def merged(earlier_memory, earlier_peak, later_memory, later_peak, later_total):
    moved = later_total + earlier_peak
    peak = jnp.maximum(moved, later_peak)
    return jnp.exp(moved - peak) * earlier_memory + jnp.exp(later_peak - peak) * later_memory, peak


def three_parts(matrix):
    parts = []
    for _ in range(3):
        top_part = matrix.astype(jnp.bfloat16)
        parts.append(top_part)
        matrix = matrix - top_part.astype(jnp.float32)
    return parts


nn = (((1,), (0,)), ((), ()))
nt = (((1,), (1,)), ((), ()))
tn = (((0,), (0,)), ((), ()))


def product(left, right, numbers):
    return lax.dot_general(left, right, numbers, preferred_element_type=jnp.float32)


def normalize(source, gain_ref, target):
    block = 64

    def body(b, carry):
        place = pl.ds(pl.multiple_of(b * block, block), block)
        widened = source[place, :].astype(jnp.float32)
        mean = jnp.mean(widened * widened, axis=-1, keepdims=True)
        factor = lax.rsqrt(mean + epsilon)
        target[place, :] = (source[place, :].astype(jnp.float32) * factor * gain_ref[...]).astype(
            target.dtype
        )
        return carry

    lax.fori_loop(0, source.shape[0] // block, body, 0)


def whole_kernel(
    sizes, mixer_hbm, expert_hbm, query_hbm, key_hbm, value_hbm, project_hbm, gate_hbm, up_hbm, down_hbm,
    mixer_gain_ref, expert_gain_ref, head_gain_ref, in_ref, forget_ref,
    group_router_ref, expert_router_ref, routes_ref,
    out_ref, mixed_ref,
    mixer_in, expert_in, query_w, key_w, value_w, project_ref, gate_ref, up_ref, down_ref,
    normed_a, normed_b, rank, rank_in, combine, near_rows, fwd, mine_b, entry_in,
    query_ref, key_ref, value_ref, cum_ref, cum_col_ref, packed_ref, acc,
    rows, part, pin, csum, xin, fin, ret,
    peer, plane, mem, pre, pre_in, state, state_peak, state_parts, mpart, mpin, msum, mxin,
    own_sem, send_a, recv_a, send_x, recv_x, send_p, recv_p,
    send_q, recv_q, send_c, recv_c, send_r, recv_r,
    send_m, recv_m, send_k, recv_k, send_h, recv_h, send_y, recv_y,
):
    n, share, cap, width, quarter, heads, size = sizes
    near = n // 2
    planes = n // 2
    me, tp = lax.axis_index("ep"), lax.axis_index("tp")
    core, column = lax.rem(tp, 2), lax.div(tp, 2)
    pair = tp + 1 - 2 * core
    cross = lax.rem(tp + 2, 4)
    pair_cross = lax.rem(pair + 2, 4)
    side, level = lax.rem(me, 2), lax.div(me, 2)
    mate = me + 1 - 2 * side
    tokens = expert_in.shape[0]
    length = mixer_in.shape[0]
    chunk = length // 4
    scale = size ** (-0.5)

    def other(i):
        total, bit = 0, 1
        while bit < n:
            total = total + bit * lax.rem(lax.div(me, bit) + lax.div(i, bit), 2)
            bit *= 2
        return total

    def far_turn(k):
        return near + (near // 2) * lax.rem(k, 2) + lax.div(k, 2)

    order = [(False, 0), (False, 1)] + [(False, k) for k in range(2, near - 1)]
    order += [(True, k) for k in range(near)]
    order += [(False, near - 1)] * (near > 2)

    def turn(t):
        total = 0
        for place, (far, k) in enumerate(order):
            total = total + jnp.where(t == place, far_turn(k) if far else k, 0)
        return total

    def is_far(t):
        total = t < 0
        for place, (far, k) in enumerate(order):
            total = total | (t == place) if far else total
        return total

    def remote(src, dst, send, recv, to):
        return pltpu.make_async_remote_copy(
            src_ref=src, dst_ref=dst, send_sem=send, recv_sem=recv, device_id=to, device_id_type=MESH
        )

    barrier = pltpu.get_barrier_semaphore()
    for i in range(1, n):
        pl.semaphore_signal(
            barrier, inc=1, device_id=(lax.rem(me + i, n), tp), device_id_type=MESH
        )
    pl.semaphore_signal(barrier, inc=1, device_id=(me, pair), device_id_type=MESH)
    pl.semaphore_signal(barrier, inc=1, device_id=(me, cross), device_id_type=MESH)

    loads = [
        pltpu.make_async_copy(src, dst, own_sem.at[k])
        for k, (src, dst) in enumerate(
            [
                (expert_hbm, expert_in), (gate_hbm, gate_ref), (up_hbm, up_ref),
                (down_hbm, down_ref), (mixer_hbm, mixer_in), (key_hbm, key_w),
                (value_hbm, value_w), (query_hbm, query_w), (project_hbm, project_ref),
            ]
        )
    ]
    loads[0].start()

    def scatter_near(i, place):
        slot = jnp.maximum(i - 1, 0)
        return remote(
            near_rows.at[slot], rows.at[place, core], send_a.at[i], recv_a.at[i], (other(i), tp)
        )

    def entry():
        return remote(mine_b, entry_in, send_a.at[0], recv_a.at[0], (other(near), tp))

    def entry_rank():
        return remote(rank, rank_in, send_a.at[near], recv_a.at[near], (other(near), tp))

    def forward(j):
        return remote(
            fwd.at[j], rows.at[other(near), core, column],
            send_a.at[near + j], recv_a.at[near + j], (other(j), tp),
        )

    def arrival(i, s):
        return remote(
            fwd.at[i - near], rows.at[s, core, column], send_a.at[i], recv_a.at[i],
            (other(i - near), tp),
        )

    def across(s, which):
        return remote(
            rows.at[s, core, which], rows.at[s, core, which],
            send_x.at[s], recv_x.at[s], (me, cross),
        )

    def beside(s, which):
        return remote(
            rows.at[s, which], rows.at[s, which], send_p.at[s], recv_p.at[s], (me, pair)
        )

    def halves(s, k, who):
        return remote(part.at[s, who], pin.at[s, k], send_q.at[s, k], recv_q.at[s, k], (me, pair))

    def summed(s):
        return remote(csum.at[s], xin.at[s], send_c.at[s], recv_c.at[s], (me, cross))

    def back(i):
        to = other(i)
        return remote(fin.at[to], ret.at[me], send_r.at[i], recv_r.at[i], (to, tp))

    def to_mate():
        return remote(
            packed_ref.at[1 - side], peer.at[1 - side], send_k.at[0], recv_k.at[0], (mate, tp)
        )

    def from_mate():
        return remote(packed_ref.at[side], peer.at[side], send_k.at[0], recv_k.at[0], (mate, tp))

    def rest_to_mate():
        return remote(packed_ref.at[0], peer.at[0], send_k.at[2], recv_k.at[2], (mate, tp))

    def to_level(d):
        return remote(
            plane, mem.at[level], send_m.at[d], recv_m.at[d], (lax.rem(me + 2 * d, n), tp)
        )

    def from_level(d):
        return remote(
            plane, mem.at[level - d], send_m.at[d], recv_m.at[d], (lax.rem(me + 2 * d, n), tp)
        )

    def prefix_mate():
        return remote(pre, pre_in, send_k.at[1], recv_k.at[1], (mate, tp))

    def mixed_half(k, who):
        return remote(mpart.at[who], mpin.at[k], send_h.at[k], recv_h.at[k], (me, pair))

    def mixed_sum(q):
        return remote(msum.at[q], mxin.at[q], send_y.at[q], recv_y.at[q], (me, cross))

    body, top_row, sum_row = slice(0, size), slice(size, size + 1), slice(size + 1, size + 2)

    def picks(table, e):
        slots = lax.broadcasted_iota(jnp.int32, (cap, tokens), 0)
        return table[pl.ds(e, 1), :] == slots.astype(jnp.float32)

    def selection(table, experts):
        return jnp.concatenate(
            [jnp.where(picks(table, e), 1.0, 0.0).astype(jnp.bfloat16) for e in experts], axis=0
        )

    def features(q):
        return pl.ds(pl.multiple_of(q * quarter, quarter), quarter)

    def prepare_rank():
        experts = lax.broadcasted_iota(jnp.int32, (n, tokens), 0)
        matches = (routes_ref[0:1, :] == experts) | (routes_ref[1:2, :] == experts)
        earlier = lax.broadcasted_iota(jnp.int32, (tokens, tokens), 0)
        earlier = earlier < lax.broadcasted_iota(jnp.int32, (tokens, tokens), 1)
        count = product(
            jnp.where(matches, 1.0, 0.0).astype(jnp.bfloat16),
            jnp.where(earlier, 1.0, 0.0).astype(jnp.bfloat16),
            nn,
        )
        rank[...] = jnp.where(matches, count, -1.0)

    def prepare_combine():
        experts = lax.broadcasted_iota(jnp.int32, (n, tokens), 0)
        groups = group_router_ref.shape[0]
        expert_logits = product(expert_router_ref[...], normed_b[...], nt)
        group_logits = product(group_router_ref[...], normed_b[...], nt)
        group_full = jnp.zeros((n, tokens), jnp.float32)
        for g in range(groups):
            inside = (experts >= g * (n // groups)) & (experts < (g + 1) * (n // groups))
            group_full = group_full + jnp.where(inside, group_logits[g : g + 1, :], 0.0)
        named = [routes_ref[k : k + 1, :] == experts for k in range(2)]
        chosen = [jnp.sum(jnp.where(m, expert_logits, 0.0), axis=0, keepdims=True) for m in named]
        total = jnp.zeros((n, tokens), jnp.float32)
        for k in range(2):
            group_pick = jnp.sum(jnp.where(named[k], group_full, 0.0), axis=0, keepdims=True)
            weight = jax.nn.sigmoid(group_pick) * jax.nn.sigmoid(chosen[k] - chosen[1 - k])
            total = total + jnp.where(named[k], weight, 0.0)
        combine[...] = total

    def prepare_near():
        select = selection(rank, [other(i) for i in range(1, near)])
        for c in range(2):
            moved = product(select, normed_b[:, features(2 * c + core)], nn).astype(jnp.bfloat16)
            for i in range(1, near):
                near_rows[i - 1, c] = moved[(i - 1) * cap : i * cap]

    def prepare_own():
        moved = product(selection(rank, [me]), normed_b[...], nn).astype(jnp.bfloat16)
        for q in range(4):
            rows[me, q % 2, q // 2] = moved[:, q * quarter : (q + 1) * quarter]

    def redistribute():
        entry_rank().wait_recv()
        entry().wait_recv()
        select = selection(rank_in, [other(j) for j in range(near)])
        moved = product(select, entry_in[...], nn).astype(jnp.bfloat16)
        for j in range(1, near):
            fwd[j] = moved[j * cap : (j + 1) * cap]
        rows[other(near), core, column] = moved[0:cap]
        for j in range(1, near):
            forward(j).start()

    def ffn(s):
        x = jnp.concatenate([rows[s, q % 2, q // 2] for q in range(4)], axis=1)
        gate_act = jnp.dot(x, gate_ref[...], preferred_element_type=jnp.float32)
        up_act = jnp.dot(x, up_ref[...], preferred_element_type=jnp.float32)
        hidden = (gate_act * jax.nn.sigmoid(gate_act) * up_act).astype(jnp.bfloat16)
        for q in range(4):
            part[s, q] = jnp.dot(
                hidden,
                down_ref[:, q * quarter : (q + 1) * quarter],
                preferred_element_type=jnp.float32,
            ).astype(jnp.bfloat16)

    def prepare_gates():
        log_forget = jnp.minimum(forget_ref[...], 0.0) - jnp.log1p(jnp.exp(-jnp.abs(forget_ref[...])))
        pieces = jnp.concatenate(
            [p.astype(jnp.float32) for p in three_parts(log_forget)]
            + [jnp.zeros((16 - 3 * heads, length), jnp.float32)],
            axis=0,
        ).astype(jnp.bfloat16)
        first = lax.broadcasted_iota(jnp.int32, (length, length), 0)
        upto = first <= lax.broadcasted_iota(jnp.int32, (length, length), 1)
        sums = product(pieces, jnp.where(upto, 1.0, 0.0).astype(jnp.bfloat16), nn)
        cum_ref[...] = sums[2 * heads : 3 * heads] + sums[heads : 2 * heads] + sums[0:heads]
        back_to = first >= lax.broadcasted_iota(jnp.int32, (length, length), 1)
        sums = product(jnp.where(back_to, 1.0, 0.0).astype(jnp.bfloat16), pieces, nt)
        cum_col_ref[...] = (
            sums[:, 2 * heads : 3 * heads] + sums[:, heads : 2 * heads] + sums[:, 0:heads]
        )

    def prepare_memory():
        key_ref[...] = jnp.dot(
            normed_a[...], key_w[...], preferred_element_type=jnp.float32
        ).astype(jnp.bfloat16)
        value_ref[...] = jnp.dot(
            normed_a[...], value_w[...], preferred_element_type=jnp.float32
        ).astype(jnp.bfloat16)
        for h in range(heads):
            cols = slice(h * size, (h + 1) * size)
            cum = cum_ref[h : h + 1, :]
            total = cum_ref[h : h + 1, length - 1 : length]
            log_weight = total - cum + in_ref[h : h + 1, :]
            peak = jnp.max(log_weight, axis=1, keepdims=True)
            weighted = value_ref[:, cols].astype(jnp.float32).T * jnp.exp(log_weight - peak)
            memory = jnp.zeros((size, size), jnp.float32)
            for piece in three_parts(weighted)[::-1]:
                memory = memory + product(piece, key_ref[:, cols], nn)
            packed_ref[h, body] = memory * scale
            packed_ref[h, size : size + 8] = jnp.zeros((8, size), jnp.float32)
            packed_ref[h, top_row] = jnp.broadcast_to(peak, (1, size))
            packed_ref[h, sum_row] = jnp.broadcast_to(total, (1, size))

    def prepare_query():
        query_ref[...] = jnp.dot(
            normed_a[...], query_w[...], preferred_element_type=jnp.float32
        ).astype(jnp.bfloat16)

    def combine_plane():
        from_mate().wait_recv()

        def joined(first, second):
            memory, peak = merged(
                first[side, body], first[side, top_row],
                second[side, body], second[side, top_row], second[side, sum_row],
            )
            plane[size : size + 8] = jnp.zeros((8, size), jnp.float32)
            plane[body] = memory
            plane[top_row] = peak
            plane[sum_row] = first[side, sum_row] + second[side, sum_row]

        @pl.when(side == 0)
        def _():
            joined(packed_ref, peer)

        @pl.when(side == 1)
        def _():
            joined(peer, packed_ref)

        for d in range(1, planes):
            @pl.when(level + d < planes)
            def _():
                to_level(d).start()

    def combine_levels():
        pre[...] = jnp.zeros_like(pre)
        pre[top_row] = jnp.full((1, size), floor_log, jnp.float32)
        for k in range(planes - 1):
            d = planes - 1 - k

            @pl.when(d <= level)
            def _():
                from_level(d).wait_recv()
                z = level - d
                memory, peak = merged(
                    pre[body], pre[top_row], mem[z, body], mem[z, top_row], mem[z, sum_row]
                )
                pre[body] = memory
                pre[top_row] = peak

        prefix_mate().start()

    def combine_last():
        prefix_mate().wait_recv()
        state[side] = pre[body]
        state_peak[side, 0:1, :] = pre[top_row]
        state[1 - side] = pre_in[body]
        state_peak[1 - side, 0:1, :] = pre_in[top_row]

        @pl.when(side == 1)
        def _():
            rest_to_mate().wait_recv()
            for h in range(heads):
                memory, peak = merged(
                    state[h], state_peak[h, 0:1, :],
                    peer[h, body], peer[h, top_row], peer[h, sum_row],
                )
                state[h] = memory
                state_peak[h, 0:1, :] = peak

        for h in range(heads):
            for piece, value in enumerate(three_parts(state[h])):
                state_parts[h, piece] = value

    def attend(j):
        start = pl.multiple_of(j * chunk, chunk)
        row = start + lax.broadcasted_iota(jnp.int32, (chunk, length), 0)
        causal = row >= lax.broadcasted_iota(jnp.int32, (chunk, length), 1)
        cell_list = []
        for h in range(heads):
            cols = slice(h * size, (h + 1) * size)
            q = query_ref[pl.ds(start, chunk), cols]
            c = cum_col_ref[pl.ds(start, chunk), h : h + 1]
            within = jnp.where(causal, c - cum_ref[h : h + 1, :] + in_ref[h : h + 1, :], -jnp.inf)
            carried = c + state_peak[h, 0:1, 0:1]
            top = jnp.maximum(jnp.max(within, axis=1, keepdims=True), carried)
            raw = product(q, key_ref[:, cols], nt)
            scores = (raw * scale * jnp.exp(within - top)).astype(jnp.bfloat16)
            cells = jnp.dot(scores, value_ref[:, cols], preferred_element_type=jnp.float32)
            held = jnp.zeros((chunk, size), jnp.float32)
            for piece in (2, 1, 0):
                held = held + product(q, state_parts[h, piece], nt)
            cells = cells + jnp.exp(carried - top) * held
            mean = jnp.mean(cells * cells, axis=1, keepdims=True)
            gain = head_gain_ref[pl.ds(tp * heads + h, 1), :]
            cell_list.append((cells * lax.rsqrt(mean + epsilon) * gain).astype(jnp.bfloat16))
        cell_rows = jnp.concatenate(cell_list, axis=1)
        for q in range(4):
            cols = slice(q * quarter, (q + 1) * quarter)
            mpart[j, q] = jnp.dot(
                cell_rows, project_ref[:, cols], preferred_element_type=jnp.float32
            ).astype(jnp.bfloat16)

    begin = n - 1

    def mixer_levels(t):
        @pl.when(t == 4)
        def _():
            combine_levels()

    def mixer_first(t):
        @pl.when(t == n + 1)
        def _():
            combine_last()

            def one(k, carry):
                attend(jnp.where(k == 0, pair_cross, cross))

                @pl.when(k == 0)
                def _():
                    mixed_half(1, pair_cross).start()

                return carry

            lax.fori_loop(0, 2, one, 0)
            mixed_half(1, pair_cross).wait_recv()
            for q in range(4):
                msum[q] = (
                    mpart[cross, q].astype(jnp.float32) + mpin[1, q].astype(jnp.float32)
                ).astype(jnp.bfloat16)
            for q in range(4):
                mixed_sum(q).start()

    def mixer_late(t):
        @pl.when(t == n + 2)
        def _():
            def one(k, carry):
                attend(jnp.where(k == 0, pair, tp))

                @pl.when(k == 0)
                def _():
                    mixed_half(0, pair).start()

                return carry

            lax.fori_loop(0, 2, one, 0)

    def collect(s):
        halves(s, 1, pair_cross).wait_recv()
        csum[s] = (
            part[s, cross].astype(jnp.float32) + pin[s, 1].astype(jnp.float32)
        ).astype(jnp.bfloat16)
        summed(s).start()

    def send_halves(s):
        halves(s, 1, pair_cross).start()
        halves(s, 0, pair).start()

    prepare_rank()
    loads[0].wait()
    for load in loads[1:]:
        load.start()
    normalize(expert_in, expert_gain_ref, normed_b)
    mine_b[...] = normed_b[:, features(tp)]
    prepare_near()
    pl.semaphore_wait(barrier, n + 1)
    entry_rank().start()
    entry().start()
    scatter_near(1, me).start()
    prepare_own()
    for k in (1, 2, 3):
        loads[k].wait()
    ffn(me)
    send_halves(me)
    for i in range(2, near - 1):
        scatter_near(i, me).start()
    loads[4].wait()
    normalize(mixer_in, mixer_gain_ref, normed_a)
    collect(me)
    prepare_gates()
    loads[5].wait()
    loads[6].wait()
    prepare_memory()
    to_mate().start()
    loads[7].wait()
    prepare_query()
    prepare_combine()
    loads[8].wait()

    def finish(t, carry):
        i = turn(t)
        s = other(i)

        @pl.when(t > 0)
        def _():
            back(i).wait_recv()

        chosen = picks(rank, s)
        weight = combine[pl.ds(s, 1), :]
        high_weight = weight.astype(jnp.bfloat16).astype(jnp.float32)
        table = ret[s]
        acc[...] += product(
            jnp.where(chosen, high_weight, 0.0).astype(jnp.bfloat16), table, tn
        ) + product(jnp.where(chosen, weight - high_weight, 0.0).astype(jnp.bfloat16), table, tn)
        return carry

    acc[...] = jnp.zeros_like(acc)

    collects = {2: (1, 2), n + 1: (n - 2, n)}
    late_collects = {n - 1: (n - 3, n - 2)}
    collects.update({t: (t - 2, t - 1) for t in range(4, n - 1)})
    delivers = {n + 1: (n - 3, n - 2), n + 2: (n - 2, n - 1), n + 3: (n - 1, n)}
    delivers.update({t: (t - 3, t - 2) for t in range(3, n)})

    def span(table, t):
        low = sum(jnp.where(t == k, v[0], 0) for k, v in sorted(table.items()))
        return low, sum(jnp.where(t == k, v[1], 0) for k, v in sorted(table.items()))

    def step(t, carry):
        working = (t == 2) | ((t > 3) & (t < n + 2))
        now = jnp.where(t == 2, 1, t - 2)

        @pl.when(working)
        def _():
            s = other(turn(now))
            beside(s, 1 - core).wait_recv()
            ffn(s)
            send_halves(s)

        def gather(place, carry):
            collect(other(turn(place)))
            return carry

        lax.fori_loop(*span(collects, t), gather, 0)

        @pl.when(t == 2)
        def _():
            redistribute()

        @pl.when(t == 4)
        def _():
            if near > 2:
                scatter_near(near - 1, me).start()

        def arrive(place, carry):
            i = turn(place)
            s = other(i)

            @pl.when(is_far(place))
            def _():
                @pl.when(i > near)
                def _():
                    arrival(i, s).wait_recv()

                across(s, column).start()

            @pl.when(jnp.logical_not(is_far(place)))
            def _():
                scatter_near(i, s).wait_recv()
                beside(s, core).start()

            return carry

        begins = jnp.where(t > near + 1, jnp.where(t == n - 1, n - 1, n), t)
        ends = jnp.where(t == near + 1, t + 2, t + 1)
        lax.fori_loop(jnp.minimum(begins, n), jnp.minimum(ends, n), arrive, 0)

        @pl.when(t == 1)
        def _():
            combine_plane()

            @pl.when(side == 0)
            def _():
                rest_to_mate().start()

        @pl.when(is_far(t - 1))
        def _():
            s = other(turn(t - 1))
            across(s, 1 - column).wait_recv()
            beside(s, core).start()

        lax.fori_loop(*span(late_collects, t), gather, 0)
        mixer_first(t)

        @pl.when(t == n + 3)
        def _():
            lax.fori_loop(0, n - 3, finish, 0)

        def deliver(place, carry):
            i = turn(place)
            s = other(i)
            halves(s, 0, pair).wait_recv()
            summed(s).wait_recv()
            total = (
                part[s, tp].astype(jnp.float32)
                + pin[s, 0].astype(jnp.float32)
                + xin[s].astype(jnp.float32)
            ).astype(jnp.bfloat16)

            @pl.when(i > 0)
            def _():
                fin[s] = total
                back(i).start()

            @pl.when(i == 0)
            def _():
                ret[s] = total

            return carry

        lax.fori_loop(*span(delivers, t), deliver, 0)
        mixer_levels(t)
        mixer_late(t)
        return carry

    lax.fori_loop(1, n + 4, step, 0)

    lax.fori_loop(n - 3, n, finish, 0)
    out_ref[...] = acc[...].astype(out_ref.dtype)
    mixed_half(0, pair).wait_recv()
    for q in range(4):
        mixed_sum(q).wait_recv()
        cols = slice(q * quarter, (q + 1) * quarter)
        mixed_ref[:, cols] = (
            mpart[tp, q].astype(jnp.float32)
            + mpin[0, q].astype(jnp.float32)
            + mxin[q].astype(jnp.float32)
        ).astype(mixed_ref.dtype)

    def drain(i, carry):
        s = other(i)
        halves(s, 0, pair).wait_send()
        halves(s, 1, pair_cross).wait_send()
        summed(s).wait_send()

        @pl.when(i > 0)
        def _():
            beside(s, core).wait_send()
            back(i).wait_send()

        @pl.when((i > 0) & (i < near))
        def _():
            scatter_near(i, me).wait_send()

        @pl.when(i >= near)
        def _():
            across(s, column).wait_send()
            @pl.when(i > near)
            def _():
                forward(i - near).wait_send()

        return carry

    lax.fori_loop(0, n, drain, 0)
    entry().wait_send()
    entry_rank().wait_send()
    to_mate().wait_send()

    @pl.when(side == 0)
    def _():
        rest_to_mate().wait_send()

    prefix_mate().wait_send()
    for d in range(1, planes):
        @pl.when(level + d < planes)
        def _():
            to_level(d).wait_send()
    mixed_half(0, pair).wait_send()
    mixed_half(1, pair_cross).wait_send()
    for q in range(4):
        mixed_sum(q).wait_send()


def hand_over(first_ref, second_ref, first_out, second_out, first_held, second_held, taken, given):
    moves = []
    for source, held, target in (
        (second_ref, second_held, second_out), (first_ref, first_held, first_out)
    ):
        half = source.shape[0] // 2
        for k in range(2):
            part, place = pl.ds(k * half, half), len(moves)
            moves.append(
                (
                    pltpu.make_async_copy(source.at[part], held.at[part], taken.at[place]),
                    pltpu.make_async_copy(held.at[part], target.at[part], given.at[place]),
                )
            )
    for take, _ in moves:
        take.start()
    for take, give in moves:
        take.wait()
        give.start()
    for _, give in moves:
        give.wait()


def all_fused(
    mixer_in, mixer_gain, query_weight, key_weight, value_weight, input_gate, forget_gate,
    head_gain, mixer_out_weight, expert_in, expert_gain, group_router, expert_router, routes,
    gate_weight, up_weight, down_weight,
):
    n = expert_router.shape[1]
    tokens, width = expert_in.shape
    cap = 4 * tokens // n
    share = cap // 4
    quarter = width // 4
    length = mixer_in.shape[0]
    heads = input_gate.shape[0]
    inner_width = query_weight.shape[1]
    size = inner_width // heads
    hidden = gate_weight.shape[1]
    chunk = length // 4
    vmem = pl.BlockSpec(memory_space=pltpu.VMEM)
    whole = pl.BlockSpec(memory_space=pl.ANY)
    dma = pltpu.SemaphoreType.DMA
    bf = jnp.bfloat16
    f32 = jnp.float32
    results = pl.pallas_call(
        functools.partial(whole_kernel, (n, share, cap, width, quarter, heads, size)),
        out_shape=(
            jax.ShapeDtypeStruct((tokens, quarter), bf),
            jax.ShapeDtypeStruct((chunk, width), bf),
        ),
        in_specs=[whole] * 9 + [vmem] * 8,
        out_specs=(vmem, vmem),
        scratch_shapes=[
            pltpu.VMEM((length, width), bf),
            pltpu.VMEM((tokens, width), bf),
            pltpu.VMEM((width, inner_width), bf),
            pltpu.VMEM((width, inner_width), bf),
            pltpu.VMEM((width, inner_width), bf),
            pltpu.VMEM((inner_width, width), bf),
            pltpu.VMEM((width, hidden), bf),
            pltpu.VMEM((width, hidden), bf),
            pltpu.VMEM((hidden, width), bf),
            pltpu.VMEM((length, width), bf),
            pltpu.VMEM((tokens, width), bf),
            pltpu.VMEM((n, tokens), f32),
            pltpu.VMEM((n, tokens), f32),
            pltpu.VMEM((n, tokens), f32),
            pltpu.VMEM((n // 2 - 1, 2, cap, quarter), bf),
            pltpu.VMEM((n // 2, cap, quarter), bf),
            pltpu.VMEM((tokens, quarter), bf),
            pltpu.VMEM((tokens, quarter), bf),
            pltpu.VMEM((length, inner_width), bf),
            pltpu.VMEM((length, inner_width), bf),
            pltpu.VMEM((length, inner_width), bf),
            pltpu.VMEM((heads, length), f32),
            pltpu.VMEM((length, heads), f32),
            pltpu.VMEM((heads, size + 8, size), f32),
            pltpu.VMEM((tokens, quarter), f32),
            pltpu.VMEM((n, 2, 2, cap, quarter), bf),
            pltpu.VMEM((n, 4, cap, quarter), bf),
            pltpu.VMEM((n, 2, cap, quarter), bf),
            pltpu.VMEM((n, cap, quarter), bf),
            pltpu.VMEM((n, cap, quarter), bf),
            pltpu.VMEM((n, cap, quarter), bf),
            pltpu.VMEM((n, cap, quarter), bf),
            pltpu.VMEM((heads, size + 8, size), f32),
            pltpu.VMEM((size + 8, size), f32),
            pltpu.VMEM((n // 2, size + 8, size), f32),
            pltpu.VMEM((size + 8, size), f32),
            pltpu.VMEM((size + 8, size), f32),
            pltpu.VMEM((heads, size, size), f32),
            pltpu.VMEM((heads, 8, size), f32),
            pltpu.VMEM((heads, 3, size, size), bf),
            pltpu.VMEM((4, 4, chunk, quarter), bf),
            pltpu.VMEM((2, 4, chunk, quarter), bf),
            pltpu.VMEM((4, chunk, quarter), bf),
            pltpu.VMEM((4, chunk, quarter), bf),
            dma((9,)),
            dma((n,)), dma((n,)), dma((n,)), dma((n,)), dma((n,)), dma((n,)),
            dma((n, 2)), dma((n, 2)), dma((n,)), dma((n,)), dma((n,)), dma((n,)),
            dma((n // 2,)), dma((n // 2,)), dma((3,)), dma((3,)), dma((2,)), dma((2,)),
            dma((4,)), dma((4,)),
        ],
        compiler_params=pltpu.CompilerParams(
            collective_id=0, has_side_effects=True, vmem_limit_bytes=60 * 1024 * 1024
        ),
        cost_estimate=pl.CostEstimate(
            flops=60_000_000_000, bytes_accessed=8_000_000, transcendentals=0
        ),
    )(
        mixer_in, expert_in, query_weight, key_weight, value_weight, mixer_out_weight,
        gate_weight, up_weight, down_weight,
        mixer_gain.reshape(1, width), expert_gain.reshape(1, width),
        head_gain.reshape(-1, size), input_gate, forget_gate,
        group_router.T, expert_router.T, routes.T,
    )
    return pl.pallas_call(
        hand_over,
        out_shape=tuple(jax.ShapeDtypeStruct(r.shape, r.dtype) for r in results),
        in_specs=[whole, whole],
        out_specs=(whole, whole),
        scratch_shapes=[pltpu.VMEM(r.shape, r.dtype) for r in results] + [dma((4,)), dma((4,))],
        compiler_params=pltpu.CompilerParams(vmem_limit_bytes=60 * 1024 * 1024),
    )(*results)


def experts_plain(own_share, gate_weight, up_weight, down_weight, mix):
    arrived = lax.all_to_all(own_share, "ep", split_axis=0, concat_axis=0, tiled=True)
    piece_rows = lax.all_gather(arrived, "tp", axis=1, tiled=True)
    gate_act = jnp.einsum(
        "scd,df->scf", piece_rows, gate_weight, preferred_element_type=jnp.float32
    )
    up_act = jnp.einsum("scd,df->scf", piece_rows, up_weight, preferred_element_type=jnp.float32)
    hidden = (jax.nn.silu(gate_act) * up_act).astype(jnp.bfloat16)
    partial_rows = jnp.einsum(
        "scf,fo->sco", hidden, down_weight, preferred_element_type=jnp.float32
    )
    summed = lax.psum_scatter(
        partial_rows.astype(jnp.bfloat16), "tp", scatter_dimension=2, tiled=True
    )
    returned = lax.all_to_all(summed, "ep", split_axis=0, concat_axis=0, tiled=True)
    return jnp.dot(
        mix, returned.reshape(-1, returned.shape[2]).astype(jnp.float32), precision=highest
    ).astype(jnp.bfloat16)


def mixer_prepare(normed_a, query_weight, key_weight, value_weight, input_gate, forget_gate):
    def project(weight):
        return jnp.dot(normed_a, weight, preferred_element_type=jnp.float32).astype(jnp.bfloat16)

    rows = normed_a.shape[0]
    heads = input_gate.shape[0]
    width_local = query_weight.shape[1]
    head_size = width_local // heads
    scale = head_size ** (-0.5)
    causal = jnp.tril(jnp.ones((rows, rows), dtype=bool))
    log_forget = jax.nn.log_sigmoid(forget_gate)
    cumulative = jnp.einsum(
        "hs,ts->ht", log_forget, causal.astype(jnp.float32), precision=highest
    )
    total = cumulative[:, -1]
    log_weight = total[:, None] - cumulative + input_gate
    peak = jnp.max(log_weight, axis=-1)
    weights = jnp.exp(log_weight - peak[:, None])
    keys = project(key_weight)
    values = project(value_weight)

    def by_head(matrix):
        return [matrix[:, h * head_size : (h + 1) * head_size] for h in range(heads)]

    key_heads, value_heads = by_head(keys), by_head(values)
    memory = jnp.stack(
        [
            lax.dot_general(
                value_heads[h].astype(jnp.float32) * weights[h][:, None],
                key_heads[h].astype(jnp.float32) * scale,
                (((0,), (0,)), ((), ())),
                precision=highest,
            )
            for h in range(heads)
        ]
    )
    stats = jnp.stack([peak, total], axis=1)
    stats = jnp.concatenate([stats, jnp.zeros((heads, 6), jnp.float32)], axis=1)
    packed = jnp.concatenate(
        [memory, jnp.broadcast_to(stats[:, :, None], (heads, 8, head_size))], axis=1
    )
    return (packed, project(query_weight), keys, values, cumulative, input_gate)


def mixer_partial(prepared, gain_local, mixer_out_weight):
    packed, queries, keys, values, cumulative, input_gate = prepared
    rows = queries.shape[0]
    heads, head_size = gain_local.shape
    scale = head_size ** (-0.5)
    causal = jnp.tril(jnp.ones((rows, rows), dtype=bool))

    def by_head(matrix):
        return [matrix[:, h * head_size : (h + 1) * head_size] for h in range(heads)]

    query_heads, key_heads, value_heads = by_head(queries), by_head(keys), by_head(values)
    everything = lax.all_gather(packed, "ep")
    n, place = lax.axis_size("ep"), lax.axis_index("ep")
    peaks = everything[:, :, head_size, 0]
    totals = everything[:, :, head_size + 1, 0]
    order = jnp.arange(n)
    later = (order[None, :] > order[:, None]) & (order[None, :] < place)
    suffix = jnp.sum(jnp.where(later[:, :, None], totals[None], 0.0), axis=1)
    before = (order < place)[:, None]
    candidate = jnp.where(before, peaks + suffix, floor_log)
    state_peak = jnp.max(candidate, axis=0)
    fade = jnp.where(before, jnp.exp(candidate - state_peak[None]), 0.0)
    state = jnp.sum(everything[:, :, :head_size] * fade[:, :, None, None], axis=0)
    cell_list = []
    for h in range(heads):
        c, gate = cumulative[h], input_gate[h]
        within = jnp.where(causal, c[:, None] - c[None, :] + gate[None, :], -jnp.inf)
        carried = c + state_peak[h]
        top = jnp.maximum(jnp.max(within, axis=-1), carried)
        raw = lax.dot_general(
            query_heads[h], key_heads[h], (((1,), (1,)), ((), ())), preferred_element_type=jnp.float32
        )
        scores = raw * scale * jnp.exp(within - top[:, None])
        cells = jnp.dot(
            scores.astype(jnp.bfloat16), value_heads[h], preferred_element_type=jnp.float32
        )
        carried_cells = lax.dot_general(
            query_heads[h].astype(jnp.float32),
            state[h],
            (((1,), (1,)), ((), ())),
            precision=highest,
        )
        cells = cells + jnp.exp(carried - top)[:, None] * carried_cells
        cell_list.append(rms_rows(cells, gain_local[h]).astype(jnp.bfloat16))
    cell_rows = jnp.concatenate(cell_list, axis=1)
    return jnp.dot(cell_rows, mixer_out_weight, preferred_element_type=jnp.float32).astype(
        jnp.bfloat16
    )


def shards(
    mixer_in,
    mixer_gain,
    query_weight,
    key_weight,
    value_weight,
    input_gate,
    forget_gate,
    head_gain,
    mixer_out_weight,
    expert_in,
    expert_gain,
    group_router,
    expert_router,
    routes,
    gate_experts,
    up_experts,
    down_experts,
):
    ranks = lax.axis_size("ep")
    share = expert_in.shape[0] // expert_router.shape[1]
    fused = lax.axis_size("tp") == 4 and ranks >= 4 and is_power(ranks) and share % 16 == 0
    fused = fused and mixer_in.shape[0] % 512 == 0 and input_gate.shape[0] == 2
    fused = fused and gate_experts.shape[0] == 1
    if fused:
        expert_out, mixer_out = all_fused(
            mixer_in, mixer_gain, query_weight, key_weight, value_weight, input_gate, forget_gate,
            head_gain, mixer_out_weight, expert_in, expert_gain, group_router, expert_router,
            routes, gate_experts[0], up_experts[0], down_experts[0],
        )
        return (mixer_out, expert_out)
    normed_b = rms_rows(expert_in, expert_gain).astype(jnp.bfloat16)
    tokens = normed_b.shape[0]
    expert_total = expert_router.shape[1]
    members = expert_total // group_router.shape[1]
    capacity = 4 * tokens // expert_total
    share = capacity // lax.axis_size("tp")
    group_logits = jnp.dot(normed_b, group_router, preferred_element_type=jnp.float32)
    expert_logits = jnp.dot(normed_b, expert_router, preferred_element_type=jnp.float32)
    expert_ids = jnp.arange(expert_total, dtype=jnp.int32)
    group_ids = jnp.arange(group_router.shape[1], dtype=jnp.int32)
    named = [routes[:, k : k + 1] == expert_ids[None, :] for k in range(2)]
    chosen = [jnp.sum(jnp.where(m, expert_logits, 0.0), axis=1, keepdims=True) for m in named]
    combine = jnp.zeros((tokens, expert_total), jnp.float32)
    for k in range(2):
        in_group = routes[:, k : k + 1] // members == group_ids[None, :]
        group_pick = jnp.sum(jnp.where(in_group, group_logits, 0.0), axis=1, keepdims=True)
        weight = jax.nn.sigmoid(group_pick) * jax.nn.sigmoid(chosen[k] - chosen[1 - k])
        combine = combine + jnp.where(named[k], weight, 0.0)
    matches = named[0] | named[1]
    earlier = jnp.tril(jnp.ones((tokens, tokens), jnp.bfloat16), -1)
    rank = jnp.dot(
        earlier, matches.astype(jnp.bfloat16), preferred_element_type=jnp.float32
    ).astype(jnp.int32)
    rank = jnp.where(matches, rank, -1)
    slots = jnp.arange(capacity, dtype=jnp.int32)
    mix = jnp.where(
        rank[:, :, None] == slots[None, None, :], combine[:, :, None], 0.0
    ).reshape(tokens, expert_total * capacity)
    own_slots = lax.axis_index("tp") * share + jnp.arange(share, dtype=jnp.int32)
    select = (rank.T[:, None, :] == own_slots[None, :, None]).astype(jnp.bfloat16)
    own_share = (
        jnp.dot(
            select.reshape(expert_total * share, tokens),
            normed_b,
            preferred_element_type=jnp.float32,
        )
        .astype(jnp.bfloat16)
        .reshape(expert_total, share, normed_b.shape[1])
    )
    normed_a = rms_rows(mixer_in, mixer_gain).astype(jnp.bfloat16)
    prepared = mixer_prepare(
        normed_a, query_weight, key_weight, value_weight, input_gate, forget_gate
    )
    width_local = query_weight.shape[1]
    gain_local = lax.dynamic_slice_in_dim(
        head_gain, lax.axis_index("tp") * width_local, width_local
    ).reshape(input_gate.shape[0], -1)
    experts = (own_share, gate_experts[0], up_experts[0], down_experts[0], mix)
    partial = mixer_partial(prepared, gain_local, mixer_out_weight)
    mixer_out = lax.psum_scatter(partial, "tp", scatter_dimension=0, tiled=True)
    expert_out = experts_plain(*experts)
    return (mixer_out, expert_out)


def solution(mesh):
    in_specs = (
        P("ep", None),
        P(),
        P(None, "tp"),
        P(None, "tp"),
        P(None, "tp"),
        P("tp", "ep"),
        P("tp", "ep"),
        P(),
        P("tp", None),
        P("ep", None),
        P(),
        P(),
        P(),
        P("ep", None),
        P("ep", None, "tp"),
        P("ep", None, "tp"),
        P("ep", "tp", None),
    )
    out_specs = (P(("ep", "tp"), None), P("ep", "tp"))
    return jax.shard_map(shards, mesh=mesh, in_specs=in_specs, out_specs=out_specs, check_vma=False)
```
